256 devices in a mesh: sp: 64 (over z, x, core), tp: 4 (over y).
Axes of the slice: x: 4, y: 4, z: 8, core: 2. Of those that a mesh axis runs over, the one named last changes fastest.
Arguments:
- moe_input: bfloat16 [8192, 2048], P('sp'), may hold values from -6 to 6
- out_cotangent: bfloat16 [8192, 2048], P('sp'), may hold values from -16 to 16
- routes: int32 [8192, 2], P('sp'), may hold values from 0 to 15, all different within a row; in each aligned block of 128 rows (0 to 127, 128 to 255, ...) at most 16 rows name the same one
- route_weight: float32 [8192, 2], P('sp'), may hold values from 0.2 to 1
- w_gate: bfloat16 [64, 2048, 896], P('sp', None, 'tp'), may hold values from -0.125 to 0.125
- w_up: bfloat16 [64, 2048, 896], P('sp', None, 'tp'), may hold values from -0.125 to 0.125
- w_down: bfloat16 [64, 896, 2048], P('sp', 'tp'), may hold values from -0.09375 to 0.09375
- out_proj: bfloat16 [2048, 1024], P(None, 'tp'), may hold values from -0.243067956 to 0.243067956
- conv_out: bfloat16 [8192, 1024], P('sp', 'tp'), may hold values from -17 to 17
- glu_value: bfloat16 [8192, 1024], P('sp', 'tp'), may hold values from -6 to 6
- glu_gate: bfloat16 [8192, 1024], P('sp', 'tp'), may hold values from -9 to 9
- taps: float32 [31, 1024], P(None, 'tp'), may hold values from -1 to 1
- norm_gain: float32 [1024], P('tp'), may hold values from 0.1 to 1.9
Outputs:
- grad_gate: bfloat16 [64, 2048, 896], P('sp', None, 'tp')
- grad_up: bfloat16 [64, 2048, 896], P('sp', None, 'tp')
- grad_down: bfloat16 [64, 896, 2048], P('sp', 'tp')
- grad_proj: float32 [2048, 1024], P('sp', 'tp')
- grad_glu_value: bfloat16 [8192, 1024], P('sp', 'tp')
- grad_glu_gate: bfloat16 [8192, 1024], P('sp', 'tp')
The draws below stay inside these ranges and needn't reach their ends.
Inputs may be any that keep to these rules, and one draw needn't show every extreme that they name: `routes`: each token names two different experts. Within the 128 tokens of one index of sp no expert is named more than 16 times, a bound that some block reaches.
All inputs are finite; a program needn't handle non-finite values.
Results may differ from the reference program's by a relative error of at most 0.014.
Values may be sent and summed in bfloat16 or wider, within the bound.
A program may use at most 128 MiB of HBM per device.

```python
import math
import jax
import jax.numpy as jnp
import numpy as np
from jax import lax

D = 2048
DB = 1024
FF = 3584
WIDTH = 31
SPAN = 4
TOK_DEV = 128
TOKENS = 8192
EXPERTS = 16
CAP = 16
N_SP = 64
N_TP = 4


def channel_profile(rough_key, lowest, highest):
    rising = jnp.exp(jnp.linspace(math.log(lowest), math.log(highest), DB)).astype(jnp.float32)
    rough = jnp.exp(jax.random.uniform(rough_key, (DB,), jnp.float32, -0.35, 0.35))
    return rising * rough


def draw_out_proj(key, part):
    base_key, rough_key = jax.random.split(jax.random.fold_in(key, 11), 2)
    profile = channel_profile(rough_key, 0.6, 1.8)
    values = jnp.clip(jax.random.normal(base_key, (D, DB), jnp.float32), -4.0, 4.0)
    return (values * profile[None, :] / math.sqrt(D)).astype(jnp.bfloat16)


def draw_conv_out(key, part):
    base_key, rough_key = jax.random.split(jax.random.fold_in(key, 23), 2)
    profile = channel_profile(rough_key, 0.5, 2.0)
    values = jnp.clip(jax.random.normal(base_key, (TOKENS, DB), jnp.float32), -4.0, 4.0)
    return (values * profile[None, :]).astype(jnp.bfloat16)


def raised(drawn, rng, source, target, shards_of, factor):
    def block_of(position):
        return (jnp.arange(drawn.shape[position]) // (drawn.shape[position] // shards_of)).reshape((-1,) + (1,) * (drawn.ndim - 1 - position))

    near = jax.random.permutation(rng, shards_of)[block_of(target)]
    other_side = (block_of(target) + shards_of // 2) % shards_of
    return jnp.where((block_of(source) == near) | (block_of(source) == other_side), factor * drawn, drawn)


def steps_of(key, shape, shards, low, top_value):
    gain, own = 1.0, jax.random.fold_in(key, 6)
    for position, parts in shards:
        draws = jnp.exp(jax.random.uniform(jax.random.fold_in(own, position), (parts,), jnp.float32, low / len(shards), top_value / len(shards)))
        gain = gain * jnp.repeat(draws, shape[position] // parts).reshape([-1 if axis == position else 1 for axis in range(len(shape))])
    return gain


def shared_out(key, own, number, rows, amount, top, reach, skew):
    sequence = jax.random.permutation(key, amount)
    heavy_load, common = portions_of(amount, rows * top, reach, skew, True), portions_of(amount, rows * top, reach, skew, False)
    places = jnp.arange(amount)

    def named(sizes, offset_by):
        used = int((sizes > 0).sum())
        fixed = max(1, used // 4)
        moved = fixed + (places - fixed + offset_by * (used - fixed)) % max(1, amount - fixed)
        return jnp.zeros((amount,), jnp.int32).at[sequence[jnp.where(places < fixed, places, moved)]].set(jnp.asarray(sizes, jnp.int32))

    sizes = jnp.where(number % 4 == 0, named(heavy_load, number // 4), named(common, number - number // 4 - 1))
    mixed = jax.random.permutation(jax.random.fold_in(own, 3), amount)
    donor, receiver = mixed[0:amount // 2 * 2:2], mixed[1:amount // 2 * 2:2]
    room = jnp.minimum(sizes[donor] - 1, reach - sizes[receiver]) // 2
    room = jnp.where((donor == sequence[0]) | (receiver == sequence[0]) | (sizes[receiver] == 0), 0, jnp.maximum(room, 0))
    moved = jax.random.randint(jax.random.fold_in(own, 4), (amount // 2,), 0, 1 << 20) % (room + 1)
    sizes = sizes.at[donor].add(-moved).at[receiver].add(moved)
    items = jnp.searchsorted(jnp.cumsum(sizes), jnp.arange(rows * top), side="right").astype(jnp.int32)
    listing = items.reshape(top, rows).T
    listing = listing[jax.random.permutation(jax.random.fold_in(own, 1), rows)]
    offset_by = jax.random.randint(jax.random.fold_in(own, 2), (rows, 1), 0, top)
    return jnp.take_along_axis(listing, (jnp.arange(top)[None, :] + offset_by) % top, axis=1)


def portions_of(count, total, most, slope, full):
    weights = [(1 << 20) // math.isqrt(standing ** slope) + 1 for standing in range(1, count + 1)]
    largest = most if full else min(most, max(-(-total // count), total * weights[0] // sum(weights)))
    least = 1 if total - largest >= count - 1 else 0
    holding, surplus = [largest] + [least] * (count - 1), total - largest - least * (count - 1)
    while surplus > 0:
        free = [i for i in range(1, count) if holding[i] < largest] or [i for i in range(1, count) if holding[i] < most]
        mass, remaining = sum([weights[i] for i in free]), surplus
        for i in free:
            extra = min(most - holding[i], max(1, remaining * weights[i] // mass), surplus)
            holding[i] = holding[i] + extra
            surplus = surplus - extra
    return np.array(holding)


def scatter_about(key, extent, scale, reach, shards=(), held_as=jnp.bfloat16):
    array = scale * jax.random.normal(key, extent, jnp.float32)
    if shards:
        array = array * steps_of(key, extent, shards, -0.22, 0.18)
    return jnp.clip(array, -reach, reach).astype(held_as)


def gaussian_with(own_key, extent, deviation, most, pieces, heavy, kind=jnp.bfloat16):
    result = deviation * jax.random.normal(own_key, extent, jnp.float32)
    if pieces:
        result = result * steps_of(own_key, extent, pieces, -0.22, 0.18)
    return jnp.clip(raised(result, jax.random.fold_in(own_key, 3), *heavy), -most, most).astype(kind)


def setup_inputs(seed: int = 0) -> dict:
    splits = jax.random.split(jax.random.key(seed), 14)
    moe_input = scatter_about(splits[0], (TOKENS, D), 1.0, 6.0, ((0, 64),))
    out_cotangent = gaussian_with(splits[1], (TOKENS, D), 1.0, 16.0, ((0, 64),), (0, 1, 64, 4.0))
    routes_keys = jax.random.split(jax.random.fold_in(splits[2], 1), TOKENS // TOK_DEV)
    routes_turns = jax.random.permutation(jax.random.fold_in(splits[2], 3), TOKENS // TOK_DEV)
    routes = jax.vmap(lambda own, number: shared_out(jax.random.fold_in(splits[2], 2), own, number, TOK_DEV, EXPERTS, 2, CAP, 0))(routes_keys, routes_turns).reshape((TOKENS, 2))
    route_weight = jnp.clip(0.2 + 0.8 * jax.random.uniform(splits[3], (TOKENS, 2), jnp.float32) ** steps_of(splits[3], (TOKENS, 2), ((0, 64),), -0.2, 0.2), 0.2, 1.0)
    w_gate = scatter_about(splits[4], (EXPERTS * SPAN, D, FF // SPAN), D ** -0.5, 0.125, ((0, 64), (2, 4)))
    w_up = scatter_about(splits[5], (EXPERTS * SPAN, D, FF // SPAN), D ** -0.5, 0.125, ((0, 64), (2, 4)))
    w_down = scatter_about(splits[6], (EXPERTS * SPAN, FF // SPAN, D), FF ** -0.5, 0.09375, ((0, 64), (1, 4)))
    out_proj = draw_out_proj(jax.random.fold_in(splits[13], 71), 0)
    conv_out = draw_conv_out(jax.random.fold_in(splits[13], 71), 0)
    glu_value = scatter_about(splits[9], (TOKENS, DB), 1.0, 6.0, ((0, 64), (1, 4)))
    glu_gate = scatter_about(splits[10], (TOKENS, DB), 1.5, 9.0, ((0, 64), (1, 4)))
    taps = scatter_about(splits[11], (WIDTH, DB), WIDTH ** -0.5, 1.0, ((1, 4),), jnp.float32)
    norm_gain = jnp.clip(1.0 + 0.18 * jax.random.normal(splits[12], (DB,), jnp.float32), 0.1, 1.9)
    return {"moe_input": moe_input, "out_cotangent": out_cotangent, "routes": routes, "route_weight": route_weight, "w_gate": w_gate, "w_up": w_up, "w_down": w_down, "out_proj": out_proj, "conv_out": conv_out, "glu_value": glu_value, "glu_gate": glu_gate, "taps": taps, "norm_gain": norm_gain}


def swish_slope(pre, sig):
    return sig * (1.0 + pre * (1.0 - sig))

def reference(moe_input, out_cotangent, routes, route_weight, w_gate, w_up, w_down, out_proj, conv_out, glu_value, glu_gate, taps, norm_gain):
    f32 = jnp.float32
    bf16 = jnp.bfloat16
    blocks = routes.reshape(N_SP, 2 * TOK_DEV)
    one_hot = (blocks[:, :, None] == jnp.arange(EXPERTS, dtype=jnp.int32)[None, None, :]).astype(jnp.int32)
    earlier = jnp.cumsum(one_hot, axis=1) - one_hot
    slot_index = lax.optimization_barrier(jnp.sum(earlier * one_hot, axis=2)).astype(jnp.int32)
    target = blocks * CAP + slot_index
    token_ids = jnp.arange(N_SP, dtype=jnp.int32)[:, None] * TOK_DEV + jnp.arange(2 * TOK_DEV, dtype=jnp.int32)[None, :] // 2
    matches = jnp.arange(EXPERTS * CAP, dtype=jnp.int32)[None, :, None] == target[:, None, :]
    source = lax.optimization_barrier(jnp.sum(jnp.where(matches, token_ids[:, None, :], 0), axis=2)).astype(jnp.int32)
    weights = lax.optimization_barrier(jnp.sum(jnp.where(matches, route_weight.reshape(N_SP, 1, 2 * TOK_DEV), 0.0), axis=2))
    filled = jnp.any(matches, axis=2)

    def by_expert(table):
        return jnp.transpose(table.reshape(N_SP, EXPERTS, CAP), (1, 0, 2)).reshape(EXPERTS, N_SP * CAP)
    ff_dev = FF // (SPAN * N_TP)
    contract_rows = (((0,), (0,)), ((), ()))

    def one_expert(inputs):
        expert, source_row, weight_row, filled_row = inputs
        expert_rows = jnp.where(filled_row[:, None], moe_input[source_row], jnp.zeros((), bf16))
        expert_cot = (weight_row[:, None] * out_cotangent[source_row].astype(f32)).astype(bf16)
        gate_w = jnp.transpose(lax.dynamic_slice_in_dim(w_gate, expert * SPAN, SPAN, 0), (1, 0, 2)).reshape(D, FF)
        up_w = jnp.transpose(lax.dynamic_slice_in_dim(w_up, expert * SPAN, SPAN, 0), (1, 0, 2)).reshape(D, FF)
        down_w = lax.dynamic_slice_in_dim(w_down, expert * SPAN, SPAN, 0).reshape(FF, D)
        gate_pre = jnp.dot(expert_rows, gate_w, preferred_element_type=f32)
        up_pre = jnp.dot(expert_rows, up_w, preferred_element_type=f32)
        gate_sig = jax.nn.sigmoid(gate_pre)
        hidden = (gate_pre * gate_sig * up_pre).astype(bf16)
        d_hidden = lax.dot_general(expert_cot, down_w, (((1,), (1,)), ((), ())), preferred_element_type=f32)
        grad_down = lax.dot_general(hidden, expert_cot, contract_rows, preferred_element_type=f32).astype(bf16)
        d_gate = (d_hidden * up_pre * swish_slope(gate_pre, gate_sig)).astype(bf16)
        d_up = (d_hidden * gate_pre * gate_sig).astype(bf16)
        grad_gate = lax.dot_general(expert_rows, d_gate, contract_rows, preferred_element_type=f32).astype(bf16)
        grad_up = lax.dot_general(expert_rows, d_up, contract_rows, preferred_element_type=f32).astype(bf16)
        row_count = expert_rows.shape[0]
        partial_value = jnp.einsum('rsjf,dsjf->sjrd', d_gate.reshape(row_count, SPAN, N_TP, ff_dev).astype(f32), gate_w.reshape(D, SPAN, N_TP, ff_dev).astype(f32))
        partial_value = partial_value + jnp.einsum('rsjf,dsjf->sjrd', d_up.reshape(row_count, SPAN, N_TP, ff_dev).astype(f32), up_w.reshape(D, SPAN, N_TP, ff_dev).astype(f32))
        partial_value = lax.optimization_barrier(partial_value.astype(bf16))
        span_part = lax.optimization_barrier(lax.optimization_barrier(jnp.sum(partial_value.astype(f32), axis=1)).astype(bf16))
        slot_grad = lax.optimization_barrier(jnp.sum(span_part.astype(f32), axis=0))
        gate_blocks = jnp.transpose(grad_gate.reshape(D, SPAN, FF // SPAN), (1, 0, 2))
        up_blocks = jnp.transpose(grad_up.reshape(D, SPAN, FF // SPAN), (1, 0, 2))
        down_blocks = grad_down.reshape(SPAN, FF // SPAN, D)
        return (gate_blocks, up_blocks, down_blocks, slot_grad)
    gate_all, up_all, down_all, slot_grads = lax.map(one_expert, (jnp.arange(EXPERTS, dtype=jnp.int32), by_expert(source), by_expert(weights), by_expert(filled)))
    grad_gate = gate_all.reshape(EXPERTS * SPAN, D, FF // SPAN)
    grad_up = up_all.reshape(EXPERTS * SPAN, D, FF // SPAN)
    grad_down = down_all.reshape(EXPERTS * SPAN, FF // SPAN, D)
    slot_table = slot_grads.reshape(EXPERTS, N_SP, CAP, D)
    per_route = slot_table[blocks, jnp.arange(N_SP, dtype=jnp.int32)[:, None], slot_index]
    moe_grad = lax.optimization_barrier(jnp.sum(per_route.reshape(TOKENS, 2, D), axis=1))
    resid_grad = (out_cotangent.astype(f32) + moe_grad).astype(bf16)
    conv_vals = conv_out.astype(f32)
    mean = lax.optimization_barrier(jnp.sum(conv_vals, axis=1, keepdims=True)) / DB
    square_mean = lax.optimization_barrier(jnp.sum(conv_vals * conv_vals, axis=1, keepdims=True)) / DB
    rstd = lax.rsqrt(square_mean - mean * mean + 1e-05)
    normed = (conv_vals - mean) * rstd
    zpre = normed * norm_gain[None, :]
    zsig = jax.nn.sigmoid(zpre)
    mixed = (zpre * zsig).astype(bf16)
    grad_proj = lax.dot_general(resid_grad, mixed, contract_rows, preferred_element_type=f32)
    d_mixed = jnp.dot(resid_grad, out_proj, preferred_element_type=f32)
    d_norm = d_mixed * swish_slope(zpre, zsig) * norm_gain[None, :]
    first_sum = lax.optimization_barrier(jnp.sum(d_norm, axis=1, keepdims=True)) / DB
    second_sum = lax.optimization_barrier(jnp.sum(d_norm * normed, axis=1, keepdims=True)) / DB
    conv_grad = (rstd * (d_norm - first_sum - normed * second_sum)).astype(bf16)
    extended = jnp.pad(conv_grad.astype(f32), ((0, WIDTH - 1), (0, 0)))
    unit_grad = lax.conv_general_dilated(extended[None], taps[:, None, :], (1,), 'VALID', dimension_numbers=('NWC', 'WIO', 'NWC'), feature_group_count=DB, precision=lax.Precision.HIGHEST)[0]
    gate_sig_in = jax.nn.sigmoid(glu_gate.astype(f32))
    grad_glu_value = (unit_grad * gate_sig_in).astype(bf16)
    grad_glu_gate = (unit_grad * glu_value.astype(f32) * gate_sig_in * (1.0 - gate_sig_in)).astype(bf16)
    return (grad_gate, grad_up, grad_down, grad_proj, grad_glu_value, grad_glu_gate)
```

```python
import jax
import jax.numpy as jnp
from jax import lax
from jax.experimental import pallas as pl
from jax.experimental.pallas import tpu as pltpu
from jax.sharding import PartitionSpec as P

DB = 1024
WIDTH = 31
SPAN = 4
MESH = pl.DeviceIdType.MESH
BF = jnp.bfloat16
F32 = jnp.float32
NT = (((1,), (1,)), ((), ()))
NN = (((1,), (0,)), ((), ()))
TN = (((0,), (0,)), ((), ()))


def mm(a, b, dims):
    return lax.dot_general(a, b, dims, preferred_element_type=F32)


def swish_slope(pre, sig):
    return sig * (1.0 + pre * (1.0 - sig))


def expert_kernel(
    routes_ref, weight_ref, x_hbm, cot_hbm, wg_hbm, wu_hbm, wd_hbm,
    gg_hbm, gu_hbm, gd_hbm, res_ref,
    xq, cq, perm, sendbuf, xc, wg, wu, wd, act_t, dg_t, du_t, gout,
    part, sib_in, in_a, in_b, in_c, in_d, in_e, total, ret,
    load_sem, out_sem, own_sem, a2a_send, a2a_recv, ag_send, ag_recv,
    sb_send, sb_recv, rs_send, rs_recv, ret_send, ret_recv, res_send, res_recv,
):
    sp = lax.axis_index("sp")
    y = lax.axis_index("tp")
    c = lax.rem(sp, 2)
    x = lax.rem(sp // 2, 4)
    z = sp // 8
    xh = x // 2
    xl = lax.rem(x, 2)
    g = lax.rem(xl + xh, 2)
    og = 1 - g
    oc = 1 - c
    me = sp // 4
    yp, ym, y2 = lax.rem(y + 1, 4), lax.rem(y + 3, 4), lax.rem(y + 2, 4)

    def holder(q):
        qh = lax.rem(q, 2)
        qx = qh * 2 + lax.rem(g + qh, 2)
        return ((q // 2) * 8 + qx * 2 + c, y)

    dev_x = (z * 8 + (xh * 2 + 1 - xl) * 2 + c, y)
    dev_s = (z * 8 + x * 2 + oc, y)
    dev_p = (sp, yp)
    dev_m = (sp, ym)

    def remote(src, dst, ss, rs, dev):
        return pltpu.make_async_remote_copy(
            src_ref=src, dst_ref=dst, send_sem=ss, recv_sem=rs, device_id=dev,
            device_id_type=MESH,
        )

    barrier = pltpu.get_barrier_semaphore()

    def greet(k, _):
        pl.semaphore_signal(barrier, inc=1, device_id=holder(lax.rem(me + k, 16)), device_id_type=MESH)
        return 0

    lax.fori_loop(1, 16, greet, 0)
    for dev in (dev_x, dev_s, dev_p, dev_m):
        pl.semaphore_signal(barrier, inc=1, device_id=dev, device_id_type=MESH)

    cols = pl.ds(pl.multiple_of(y * 512, 512), 512)
    load_x = pltpu.make_async_copy(x_hbm.at[:, cols], xq, load_sem.at[0])
    load_c = pltpu.make_async_copy(cot_hbm.at[:, cols], cq, load_sem.at[1])
    load_x.start()
    load_c.start()
    loads = [
        pltpu.make_async_copy(wg_hbm, wg, load_sem.at[2]),
        pltpu.make_async_copy(wu_hbm, wu, load_sem.at[3]),
        pltpu.make_async_copy(wd_hbm, wd, load_sem.at[4]),
    ]
    for copy in loads:
        copy.start()

    r0 = routes_ref[0:1, :]
    r1 = routes_ref[1:2, :]
    ids = lax.broadcasted_iota(jnp.int32, (16, 128), 0)
    e0 = ids == r0
    e1 = ids == r1
    named = jnp.where(e0, 1.0, 0.0) + jnp.where(e1, 1.0, 0.0)
    before = jnp.where(
        lax.broadcasted_iota(jnp.int32, (128, 128), 0)
        < lax.broadcasted_iota(jnp.int32, (128, 128), 1),
        1.0, 0.0,
    ).astype(BF)
    earlier = mm(named.astype(BF), before, NN)
    t0 = r0.astype(F32) * 16.0 + jnp.sum(jnp.where(e0, earlier, 0.0), axis=0, keepdims=True)
    t1 = r1.astype(F32) * 16.0 + jnp.sum(jnp.where(e1, earlier, 0.0), axis=0, keepdims=True)
    place = lax.broadcasted_iota(jnp.int32, (256, 128), 0).astype(F32)
    p0 = place == t0
    p1 = place == t1
    perm_val = (jnp.where(p0, 1.0, 0.0) + jnp.where(p1, 1.0, 0.0)).astype(BF)
    perm[...] = perm_val
    w0 = weight_ref[0:1, :]
    w1 = weight_ref[1:2, :]
    w_slot = jnp.sum(jnp.where(p0, w0, 0.0) + jnp.where(p1, w1, 0.0), axis=1, keepdims=True)
    load_x.wait()
    sendbuf[0] = mm(perm_val, xq[...], NN).astype(BF)
    load_c.wait()
    sendbuf[1] = (w_slot * mm(perm_val, cq[...], NN)).astype(BF)

    pl.semaphore_wait(barrier, 19)

    m_own = g * 2 + c

    def rows_of(q):
        return pl.ds(pl.multiple_of(q * 16, 16), 16)

    for a in range(2):

        def push(k, _, a=a):
            q = lax.rem(me + k, 16)
            remote(
                sendbuf.at[a, rows_of(q)], xc.at[a, m_own, y, rows_of(me)],
                a2a_send.at[a, q], a2a_recv.at[a, me], holder(q),
            ).start()
            return 0

        lax.fori_loop(1, 16, push, 0)
    own = [
        pltpu.make_async_copy(
            sendbuf.at[a, rows_of(me)], xc.at[a, m_own, y, rows_of(me)], own_sem.at[a]
        )
        for a in range(2)
    ]
    own[0].start()
    own[1].start()

    def a2a_wait(a):
        def one(k, _):
            q = lax.rem(me + 16 - k, 16)
            remote(
                sendbuf.at[a, rows_of(q)], xc.at[a, m_own, y, rows_of(q)],
                a2a_send.at[a, q], a2a_recv.at[a, q], holder(q),
            ).wait_recv()
            return 0

        lax.fori_loop(1, 16, one, 0)
        own[a].wait()

    first, second = pl.ds(0, 128), pl.ds(128, 128)
    listed = [(g, y), (g, ym), (g, yp), (g, y2), (og, y), (og, ym), (og, yp), (og, y2)]

    def block(a, gg, cc, yy):
        return xc.at[a, gg * 2 + cc, yy]

    def ag_copy(a, kind, ref, dev):
        return remote(ref, ref, ag_send.at[a, kind], ag_recv.at[a, kind], dev)

    def ag_out(a, kind):
        if kind >= 8:
            gg, yy = listed[kind - 8]
            return ag_copy(a, kind, block(a, gg, c, yy), dev_s)
        ref, dev = (
            (block(a, g, c, y), dev_x),
            (block(a, g, c, y), dev_p),
            (block(a, g, c, y), dev_m),
            (block(a, g, c, ym).at[first], dev_p),
            (block(a, g, c, yp).at[second], dev_m),
            (block(a, og, c, y), dev_p),
            (block(a, og, c, y), dev_m),
            (block(a, g, c, y2), dev_x),
        )[kind]
        return ag_copy(a, kind, ref, dev)

    def ag_in(a, kind):
        if kind >= 8:
            gg, yy = listed[kind - 8]
            return ag_copy(a, kind, block(a, gg, oc, yy), dev_s)
        ref, dev = (
            (block(a, og, c, y), dev_x),
            (block(a, g, c, ym), dev_m),
            (block(a, g, c, yp), dev_p),
            (block(a, g, c, y2).at[first], dev_m),
            (block(a, g, c, y2).at[second], dev_p),
            (block(a, og, c, ym), dev_m),
            (block(a, og, c, yp), dev_p),
            (block(a, og, c, y2), dev_x),
        )[kind]
        return ag_copy(a, kind, ref, dev)

    def go(a, *kinds):
        for kind in kinds:
            ag_out(a, kind).start()

    def got(a, *kinds):
        for kind in kinds:
            ag_in(a, kind).wait_recv()

    a2a_wait(0)
    go(0, 0, 1, 2, 8)
    a2a_wait(1)
    go(1, 0, 1, 2, 8)
    got(0, 1)
    go(0, 3, 9)
    got(0, 2)
    go(0, 4, 10)
    got(1, 1)
    go(1, 3, 9)
    got(1, 2)
    go(1, 4, 10)
    got(0, 0)
    go(0, 5, 6, 12)
    got(1, 0)
    go(1, 5, 6, 12)
    got(0, 3, 4)
    go(0, 7, 11)
    got(1, 3, 4)
    go(1, 7, 11)

    for copy in loads:
        copy.wait()

    def forward(m):
        pre_g = jnp.zeros((256, 224), F32)
        pre_u = jnp.zeros((256, 224), F32)
        d_act = jnp.zeros((256, 224), F32)
        for q in range(4):
            span = slice(q * 512, q * 512 + 512)
            rows = xc[0, m, q]
            pre_g += mm(rows, wg[:, span], NT)
            pre_u += mm(rows, wu[:, span], NT)
            d_act += mm(xc[1, m, q], wd[:, span], NT)
        sig = jax.nn.sigmoid(pre_g)
        d_gate = (d_act * pre_u * swish_slope(pre_g, sig)).astype(BF)
        d_up = (d_act * pre_g * sig).astype(BF)
        act_t[m] = (pre_g * sig * pre_u).T.astype(BF)
        dg_t[m] = d_gate.T
        du_t[m] = d_up.T
        return d_gate, d_up

    def back(m, d_gate, d_up, yy):
        span = pl.ds(pl.multiple_of(yy * 512, 512), 512)
        part[m, yy] = (mm(d_gate, wg[:, span], NN) + mm(d_up, wu[:, span], NN)).astype(BF)

    def sib_copy(gg, j, yy):
        return remote(
            part.at[gg * 2 + oc, yy], sib_in.at[gg, yy],
            sb_send.at[gg, j], sb_recv.at[gg, j], dev_s,
        )

    order = (y2, yp, ym, y)

    def whole(gg, cc, sent):
        m = gg * 2 + cc
        d_gate, d_up = forward(m)
        for j, yy in enumerate(order):
            back(m, d_gate, d_up, yy)
            if sent:
                sib_copy(gg, j, yy).start()

    whole(g, c, False)
    got(0, 8, 9, 10, 11)
    got(1, 8, 9, 10, 11)
    got(0, 5)
    go(0, 13)
    got(0, 6)
    go(0, 14)
    got(0, 7)
    go(0, 15)
    whole(g, oc, True)
    got(1, 5)
    go(1, 13)
    got(1, 6)
    go(1, 14)
    got(1, 7)
    go(1, 15)
    whole(og, c, False)
    got(0, 12, 13, 14, 15)
    got(1, 12, 13, 14, 15)
    whole(og, oc, True)

    def pair_sum(gg, j):
        yy = order[j]
        sib_copy_in = remote(
            part.at[gg * 2 + oc, yy], sib_in.at[gg, yy],
            sb_send.at[gg, j], sb_recv.at[gg, j], dev_s,
        )
        sib_copy_in.wait_recv()
        m = gg * 2 + c
        part[m, yy] = (part[m, yy].astype(F32) + sib_in[gg, yy].astype(F32)).astype(BF)

    def rs_copy(kind, src, dst, dev):
        return remote(src, dst, rs_send.at[kind], rs_recv.at[kind], dev)

    m_g, m_o = g * 2 + c, og * 2 + c
    pair_sum(og, 0)
    send_a = rs_copy(0, part.at[m_o, y2], in_a, dev_x)
    send_a.start()
    pair_sum(og, 1)
    send_bp = rs_copy(1, part.at[m_o, yp], in_b.at[0], dev_p)
    send_bp.start()
    pair_sum(og, 2)
    send_bm = rs_copy(2, part.at[m_o, ym], in_b.at[1], dev_m)
    send_bm.start()
    for j in range(3):
        pair_sum(g, j)
    pair_sum(og, 3)
    pair_sum(g, 3)

    def weight_grad(i, source, a):
        def tile(q, _):
            acc = mm(source[0], xc[a, 0, q], NN)
            for m in range(1, 4):
                acc += mm(source[m], xc[a, m, q], NN)
            gout[i, :, pl.ds(pl.multiple_of(q * 512, 512), 512)] = acc.astype(BF)
            return 0

        lax.fori_loop(0, 4, tile, 0)

    weight_grad(0, dg_t, 0)
    outs = [
        pltpu.make_async_copy(gout.at[i], ref, out_sem.at[i])
        for i, ref in enumerate((gg_hbm, gu_hbm, gd_hbm))
    ]
    outs[0].start()
    weight_grad(1, du_t, 0)
    outs[1].start()
    send_a.wait_recv()
    part[m_g, y2] = (part[m_g, y2].astype(F32) + in_a[...].astype(F32)).astype(BF)
    send_cp = rs_copy(3, part.at[m_g, y2, first], in_c.at[0], dev_p)
    send_cm = rs_copy(4, part.at[m_g, y2, second], in_c.at[1], dev_m)
    send_cp.start()
    send_cm.start()
    send_bp.wait_recv()
    send_bm.wait_recv()
    part[m_o, y] = (
        part[m_o, y].astype(F32) + in_b[0].astype(F32) + in_b[1].astype(F32)
    ).astype(BF)
    send_d = rs_copy(5, part.at[m_o, y], in_d, dev_x)
    send_d.start()
    weight_grad(2, act_t, 1)
    outs[2].start()
    send_cp.wait_recv()
    part[m_g, yp, first] = (part[m_g, yp, first].astype(F32) + in_c[0].astype(F32)).astype(BF)
    send_ep = rs_copy(6, part.at[m_g, yp], in_e.at[0], dev_p)
    send_ep.start()
    send_cm.wait_recv()
    part[m_g, ym, second] = (part[m_g, ym, second].astype(F32) + in_c[1].astype(F32)).astype(BF)
    send_em = rs_copy(7, part.at[m_g, ym], in_e.at[1], dev_m)
    send_em.start()
    send_d.wait_recv()
    send_ep.wait_recv()
    send_em.wait_recv()
    total[...] = (
        part[m_g, y].astype(F32) + in_d[...].astype(F32)
        + in_e[0].astype(F32) + in_e[1].astype(F32)
    ).astype(BF)

    def push_back(k, _):
        q = lax.rem(me + k, 16)
        remote(
            total.at[rows_of(q)], ret.at[rows_of(me)], ret_send.at[q], ret_recv.at[me], holder(q)
        ).start()
        return 0

    lax.fori_loop(1, 16, push_back, 0)
    own_back = pltpu.make_async_copy(total.at[rows_of(me)], ret.at[rows_of(me)], own_sem.at[0])
    own_back.start()

    def wait_back(k, _):
        q = lax.rem(me + 16 - k, 16)
        remote(
            total.at[rows_of(q)], ret.at[rows_of(q)], ret_send.at[q], ret_recv.at[q], holder(q)
        ).wait_recv()
        return 0

    lax.fori_loop(1, 16, wait_back, 0)
    own_back.wait()
    moe = mm(perm[...], ret[...], TN)
    res_ref[y] = (cq[...].astype(F32) + moe).astype(BF)

    half0, half1 = pl.ds(0, 64), pl.ds(64, 64)

    def res_copy(kind, ref, dev):
        return remote(ref, ref, res_send.at[kind], res_recv.at[kind], dev)

    sends = [res_copy(0, res_ref.at[y], dev_p), res_copy(1, res_ref.at[y], dev_m)]
    sends[0].start()
    sends[1].start()
    res_copy(0, res_ref.at[ym], dev_m).wait_recv()
    sends.append(res_copy(2, res_ref.at[ym, half0], dev_p))
    sends[2].start()
    res_copy(1, res_ref.at[yp], dev_p).wait_recv()
    sends.append(res_copy(3, res_ref.at[yp, half1], dev_m))
    sends[3].start()
    res_copy(2, res_ref.at[y2, half0], dev_m).wait_recv()
    res_copy(3, res_ref.at[y2, half1], dev_p).wait_recv()

    for copy in outs:
        copy.wait()
    for a in range(2):

        def drain(k, _, a=a):
            q = lax.rem(me + k, 16)
            remote(
                sendbuf.at[a, rows_of(q)], xc.at[a, m_own, y, rows_of(me)],
                a2a_send.at[a, q], a2a_recv.at[a, me], holder(q),
            ).wait_send()
            return 0

        lax.fori_loop(1, 16, drain, 0)
        for kind in range(16):
            ag_out(a, kind).wait_send()

    def drain_back(k, _):
        q = lax.rem(me + k, 16)
        remote(
            total.at[rows_of(q)], ret.at[rows_of(me)], ret_send.at[q], ret_recv.at[me], holder(q)
        ).wait_send()
        return 0

    lax.fori_loop(1, 16, drain_back, 0)
    for gg in (g, og):
        for j, yy in enumerate(order):
            sib_copy(gg, j, yy).wait_send()
    for copy in (send_a, send_bp, send_bm, send_cp, send_cm, send_d, send_ep, send_em, *sends):
        copy.wait_send()


def expert_stage(routes_t, weight_t, moe_input, out_cot, wg, wu, wd):
    units, width = wg.shape
    vmem = pl.BlockSpec(memory_space=pltpu.VMEM)
    hbm = pl.BlockSpec(memory_space=pl.ANY)
    dma = pltpu.SemaphoreType.DMA
    grad = jax.ShapeDtypeStruct((units, width), BF)
    return pl.pallas_call(
        expert_kernel,
        out_shape=(grad, grad, grad, jax.ShapeDtypeStruct((4, 128, 512), BF)),
        in_specs=[vmem, vmem, hbm, hbm, hbm, hbm, hbm],
        out_specs=(hbm, hbm, hbm, vmem),
        scratch_shapes=[
            pltpu.VMEM((128, 512), BF),
            pltpu.VMEM((128, 512), BF),
            pltpu.VMEM((256, 128), BF),
            pltpu.VMEM((2, 256, 512), BF),
            pltpu.VMEM((2, 4, 4, 256, 512), BF),
            pltpu.VMEM((units, width), BF),
            pltpu.VMEM((units, width), BF),
            pltpu.VMEM((units, width), BF),
            pltpu.VMEM((4, units, 256), BF),
            pltpu.VMEM((4, units, 256), BF),
            pltpu.VMEM((4, units, 256), BF),
            pltpu.VMEM((3, units, width), BF),
            pltpu.VMEM((4, 4, 256, 512), BF),
            pltpu.VMEM((2, 4, 256, 512), BF),
            pltpu.VMEM((256, 512), BF),
            pltpu.VMEM((2, 256, 512), BF),
            pltpu.VMEM((2, 128, 512), BF),
            pltpu.VMEM((256, 512), BF),
            pltpu.VMEM((2, 256, 512), BF),
            pltpu.VMEM((256, 512), BF),
            pltpu.VMEM((256, 512), BF),
            dma((5,)), dma((3,)), dma((2,)),
            dma((2, 16)), dma((2, 16)), dma((2, 16)), dma((2, 16)),
            dma((2, 4)), dma((2, 4)), dma((8,)), dma((8,)),
            dma((16,)), dma((16,)), dma((4,)), dma((4,)),
        ],
        compiler_params=pltpu.CompilerParams(
            collective_id=0, has_side_effects=True, vmem_limit_bytes=60 * 1024 * 1024
        ),
        name="expert_stage",
    )(routes_t, weight_t, moe_input, out_cot, wg, wu, wd)


def in_blocks(array, dim, size):
    lengths = array.shape
    blocks = array.reshape(*lengths[:dim], size, lengths[dim] // size, *lengths[dim + 1 :])
    return jnp.moveaxis(blocks, dim, 0)


def sum_at_owner(array, axis, dim):
    size = lax.axis_size(axis)
    blocks = lax.all_to_all(in_blocks(array, dim, size), axis, 0, 0, tiled=True)
    return jnp.sum(blocks.astype(jnp.float32), axis=0)


def from_behind(block, axis, distance):
    devices = range(lax.axis_size(axis))
    route = [(i - distance, i) for i in devices if i - distance in devices]
    return lax.ppermute(block, axis, route)


def local(
    moe_input,
    out_cotangent,
    routes,
    route_weight,
    w_gate,
    w_up,
    w_down,
    out_proj,
    conv_out,
    glu_value,
    glu_gate,
    taps,
    norm_gain,
):
    grad_gate, grad_up, grad_down, resid = expert_stage(
        routes.T, route_weight.T, moe_input, out_cotangent,
        w_gate[0].T, w_up[0].T, w_down[0],
    )
    resid_grad = jnp.swapaxes(resid, 1, 2).reshape(2048, 128)
    conv_vals = conv_out.astype(jnp.float32)
    total_sum, square_sum = lax.psum(
        (jnp.sum(conv_vals, axis=1), jnp.sum(conv_vals * conv_vals, axis=1)), "tp"
    )
    mean = total_sum[:, None] / DB
    rstd = lax.rsqrt(square_sum[:, None] / DB - mean * mean + 1e-05)
    normed = (conv_vals - mean) * rstd
    zpre = normed * norm_gain[None, :]
    zsig = jax.nn.sigmoid(zpre)
    mixed = (zpre * zsig).astype(jnp.bfloat16)
    grad_proj = sum_at_owner(
        jnp.dot(resid_grad, mixed, preferred_element_type=jnp.float32).astype(jnp.bfloat16), "sp", 0
    )
    d_mixed = lax.dot_general(
        resid_grad, out_proj, (((0,), (0,)), ((), ())), preferred_element_type=jnp.float32
    )
    d_norm = d_mixed * swish_slope(zpre, zsig) * norm_gain[None, :]
    first_sum, second_sum = lax.psum(
        (jnp.sum(d_norm, axis=1), jnp.sum(d_norm * normed, axis=1)), "tp"
    )
    conv_grad = (
        rstd * (d_norm - first_sum[:, None] / DB - normed * second_sum[:, None] / DB)
    ).astype(jnp.bfloat16)
    later_rows = from_behind(conv_grad[: WIDTH - 1], "sp", -1)
    extended = jnp.concatenate([conv_grad, later_rows], axis=0).astype(jnp.float32)
    unit_grad = lax.conv_general_dilated(
        extended[None],
        taps[:, None, :],
        (1,),
        "VALID",
        dimension_numbers=("NWC", "WIO", "NWC"),
        feature_group_count=taps.shape[1],
        precision=lax.Precision.HIGHEST,
    )[0]
    gate_sig_in = jax.nn.sigmoid(glu_gate.astype(jnp.float32))
    grad_glu_value = (unit_grad * gate_sig_in).astype(jnp.bfloat16)
    grad_glu_gate = (
        unit_grad * glu_value.astype(jnp.float32) * gate_sig_in * (1.0 - gate_sig_in)
    ).astype(jnp.bfloat16)
    return (grad_gate.T[None], grad_up.T[None], grad_down[None], grad_proj, grad_glu_value, grad_glu_gate)


def solution(mesh):
    in_specs = (
        P("sp", None),
        P("sp", None),
        P("sp", None),
        P("sp", None),
        P("sp", None, "tp"),
        P("sp", None, "tp"),
        P("sp", "tp", None),
        P(None, "tp"),
        P("sp", "tp"),
        P("sp", "tp"),
        P("sp", "tp"),
        P(None, "tp"),
        P("tp"),
    )
    out_specs = (
        P("sp", None, "tp"),
        P("sp", None, "tp"),
        P("sp", "tp", None),
        P("sp", "tp"),
        P("sp", "tp"),
        P("sp", "tp"),
    )
    return jax.shard_map(local, mesh=mesh, in_specs=in_specs, out_specs=out_specs, check_vma=False)
```

```python
import jax
import jax.numpy as jnp
from jax import lax
from jax.experimental import pallas as pl
from jax.experimental.pallas import tpu as pltpu
from jax.sharding import PartitionSpec as P

DB = 1024
WIDTH = 31
MESH = pl.DeviceIdType.MESH
BF = jnp.bfloat16
F32 = jnp.float32
NT = (((1,), (1,)), ((), ()))
NN = (((1,), (0,)), ((), ()))
TN = (((0,), (0,)), ((), ()))


def mm(a, b, dims):
    return lax.dot_general(a, b, dims, preferred_element_type=F32)


def swish_slope(pre, sig):
    return sig * (1.0 + pre * (1.0 - sig))


def backward_kernel(
    routes_ref, weight_ref, conv_ref, value_ref, gate_ref, taps_ref, gain_ref,
    x_hbm, cot_hbm, wg_hbm, wu_hbm, wd_hbm, proj_hbm,
    gg_hbm, gu_hbm, gd_hbm, gp_ref, gv_ref, gt_ref,
    xq, cq, perm, sendbuf, xc, wg, wu, wd, act_t, dg_t, du_t, gout,
    part, sib_in, in_a, in_b, in_c, in_d, in_e, total, ret,
    res_ref, proj, normed, slope, mixed, scale, st_out, st_in, ext, halo_out, halo_in,
    gp, gp_sib, gp_x, gp_row, gp_z,
    load_sem, out_sem, own_sem, a2a_send, a2a_recv, ag_send, ag_recv,
    sb_send, sb_recv, rs_send, rs_recv, ret_send, ret_recv, res_send, res_recv,
    st_send, st_recv, halo_sem, gs_send, gs_recv, gx_send, gx_recv, gz_send, gz_recv,
):
    sp = lax.axis_index("sp")
    y = lax.axis_index("tp")
    c = lax.rem(sp, 2)
    x = lax.rem(sp // 2, 4)
    z = sp // 8
    xh = x // 2
    xl = lax.rem(x, 2)
    g = lax.rem(xl + xh, 2)
    og = 1 - g
    oc = 1 - c
    me = sp // 4
    yp, ym, y2 = lax.rem(y + 1, 4), lax.rem(y + 3, 4), lax.rem(y + 2, 4)

    def holder(q):
        qh = lax.rem(q, 2)
        qx = qh * 2 + lax.rem(g + qh, 2)
        return ((q // 2) * 8 + qx * 2 + c, y)

    dev_x = (z * 8 + (xh * 2 + 1 - xl) * 2 + c, y)
    dev_s = (z * 8 + x * 2 + oc, y)
    dev_p = (sp, yp)
    dev_m = (sp, ym)
    dev_2 = (sp, y2)
    dev_prev = (lax.rem(sp + 63, 64), y)
    dev_next = (lax.rem(sp + 1, 64), y)
    others_x = (xh * 2 + 1 - xl, (1 - xh) * 2 + xl, (1 - xh) * 2 + 1 - xl)

    def at_x(xx):
        return (z * 8 + xx * 2 + c, y)

    def at_z(zz):
        return (zz * 8 + x * 2 + c, y)

    def remote(src, dst, ss, rs, dev):
        return pltpu.make_async_remote_copy(
            src_ref=src, dst_ref=dst, send_sem=ss, recv_sem=rs, device_id=dev,
            device_id_type=MESH,
        )

    barrier = pltpu.get_barrier_semaphore()

    def greet(k, _):
        pl.semaphore_signal(barrier, inc=1, device_id=holder(lax.rem(me + k, 16)), device_id_type=MESH)
        return 0

    lax.fori_loop(1, 16, greet, 0)
    greeted = (
        dev_x, dev_s, dev_p, dev_m, dev_2, at_x(others_x[1]), at_x(others_x[2]), dev_prev, dev_next
    )
    for dev in greeted:
        pl.semaphore_signal(barrier, inc=1, device_id=dev, device_id_type=MESH)

    cols = pl.ds(pl.multiple_of(y * 512, 512), 512)
    load_x = pltpu.make_async_copy(x_hbm.at[:, cols], xq, load_sem.at[0])
    load_c = pltpu.make_async_copy(cot_hbm.at[:, cols], cq, load_sem.at[1])
    load_x.start()
    load_c.start()
    loads = [
        pltpu.make_async_copy(wg_hbm, wg, load_sem.at[2]),
        pltpu.make_async_copy(wu_hbm, wu, load_sem.at[3]),
        pltpu.make_async_copy(wd_hbm, wd, load_sem.at[4]),
    ]
    for copy in loads:
        copy.start()
    load_proj = pltpu.make_async_copy(proj_hbm, proj, load_sem.at[5])
    load_proj.start()

    r0 = routes_ref[0:1, :]
    r1 = routes_ref[1:2, :]
    ids = lax.broadcasted_iota(jnp.int32, (16, 128), 0)
    e0 = ids == r0
    e1 = ids == r1
    named = jnp.where(e0, 1.0, 0.0) + jnp.where(e1, 1.0, 0.0)
    before = jnp.where(
        lax.broadcasted_iota(jnp.int32, (128, 128), 0)
        < lax.broadcasted_iota(jnp.int32, (128, 128), 1),
        1.0, 0.0,
    ).astype(BF)
    earlier = mm(named.astype(BF), before, NN)
    t0 = r0.astype(F32) * 16.0 + jnp.sum(jnp.where(e0, earlier, 0.0), axis=0, keepdims=True)
    t1 = r1.astype(F32) * 16.0 + jnp.sum(jnp.where(e1, earlier, 0.0), axis=0, keepdims=True)
    place = lax.broadcasted_iota(jnp.int32, (256, 128), 0).astype(F32)
    p0 = place == t0
    p1 = place == t1
    perm_val = (jnp.where(p0, 1.0, 0.0) + jnp.where(p1, 1.0, 0.0)).astype(BF)
    perm[...] = perm_val
    w0 = weight_ref[0:1, :]
    w1 = weight_ref[1:2, :]
    w_slot = jnp.sum(jnp.where(p0, w0, 0.0) + jnp.where(p1, w1, 0.0), axis=1, keepdims=True)
    load_x.wait()
    sendbuf[0] = mm(perm_val, xq[...], NN).astype(BF)
    load_c.wait()
    sendbuf[1] = (w_slot * mm(perm_val, cq[...], NN)).astype(BF)

    pl.semaphore_wait(barrier, 24)

    m_own = g * 2 + c

    def rows_of(q):
        return pl.ds(pl.multiple_of(q * 16, 16), 16)

    for a in range(2):

        def push(k, _, a=a):
            q = lax.rem(me + k, 16)
            remote(
                sendbuf.at[a, rows_of(q)], xc.at[a, m_own, y, rows_of(me)],
                a2a_send.at[a, q], a2a_recv.at[a, me], holder(q),
            ).start()
            return 0

        lax.fori_loop(1, 16, push, 0)
    own = [
        pltpu.make_async_copy(
            sendbuf.at[a, rows_of(me)], xc.at[a, m_own, y, rows_of(me)], own_sem.at[a]
        )
        for a in range(2)
    ]
    own[0].start()
    own[1].start()

    def a2a_wait(a):
        def one(k, _):
            q = lax.rem(me + 16 - k, 16)
            remote(
                sendbuf.at[a, rows_of(q)], xc.at[a, m_own, y, rows_of(q)],
                a2a_send.at[a, q], a2a_recv.at[a, q], holder(q),
            ).wait_recv()
            return 0

        lax.fori_loop(1, 16, one, 0)
        own[a].wait()

    lane = lax.broadcasted_iota(jnp.int32, (128, 128), 1)

    def sums_out(phase, one, two):
        cols2 = jnp.where(lane == 0, one, 0.0) + jnp.where(lane == 1, two, 0.0)
        st_out[phase] = cols2.T[0:8, :]
        return [
            remote(
                st_out.at[phase], st_in.at[phase, j], st_send.at[phase, j], st_recv.at[phase, j], dev
            )
            for j, dev in enumerate((dev_p, dev_m, dev_2))
        ]

    def sums_in(phase, copies):
        for copy in copies:
            copy.wait_recv()
        tot = (st_out[phase] + st_in[phase, 2]) + (st_in[phase, 0] + st_in[phase, 1])
        tall = jnp.concatenate([tot, jnp.zeros((120, 128), F32)], axis=0).T
        return tall[:, 0:1], tall[:, 1:2]

    conv_vals = conv_ref[...].astype(F32)
    stats = sums_out(
        0,
        jnp.sum(conv_vals, axis=1, keepdims=True),
        jnp.sum(conv_vals * conv_vals, axis=1, keepdims=True),
    )
    for copy in stats:
        copy.start()

    first, second = pl.ds(0, 128), pl.ds(128, 128)
    listed = [(g, y), (g, ym), (g, yp), (g, y2), (og, y), (og, ym), (og, yp), (og, y2)]

    def block(a, gg, cc, yy):
        return xc.at[a, gg * 2 + cc, yy]

    def ag_copy(a, kind, ref, dev):
        return remote(ref, ref, ag_send.at[a, kind], ag_recv.at[a, kind], dev)

    def ag_out(a, kind):
        if kind >= 8:
            gg, yy = listed[kind - 8]
            return ag_copy(a, kind, block(a, gg, c, yy), dev_s)
        ref, dev = (
            (block(a, g, c, y), dev_x),
            (block(a, g, c, y), dev_p),
            (block(a, g, c, y), dev_m),
            (block(a, g, c, ym).at[first], dev_p),
            (block(a, g, c, yp).at[second], dev_m),
            (block(a, og, c, y), dev_p),
            (block(a, og, c, y), dev_m),
            (block(a, g, c, y2), dev_x),
        )[kind]
        return ag_copy(a, kind, ref, dev)

    def ag_in(a, kind):
        if kind >= 8:
            gg, yy = listed[kind - 8]
            return ag_copy(a, kind, block(a, gg, oc, yy), dev_s)
        ref, dev = (
            (block(a, og, c, y), dev_x),
            (block(a, g, c, ym), dev_m),
            (block(a, g, c, yp), dev_p),
            (block(a, g, c, y2).at[first], dev_m),
            (block(a, g, c, y2).at[second], dev_p),
            (block(a, og, c, ym), dev_m),
            (block(a, og, c, yp), dev_p),
            (block(a, og, c, y2), dev_x),
        )[kind]
        return ag_copy(a, kind, ref, dev)

    def go(a, *kinds):
        for kind in kinds:
            ag_out(a, kind).start()

    def got(a, *kinds):
        for kind in kinds:
            ag_in(a, kind).wait_recv()

    a2a_wait(0)
    go(0, 0, 1, 2, 8)
    a2a_wait(1)
    go(1, 0, 1, 2, 8)
    got(0, 1)
    go(0, 3, 9)
    got(0, 2)
    go(0, 4, 10)
    got(1, 1)
    go(1, 3, 9)
    got(1, 2)
    go(1, 4, 10)
    got(0, 0)
    go(0, 5, 6, 12)
    got(1, 0)
    go(1, 5, 6, 12)
    sum1, sum2 = sums_in(0, stats)
    mean = sum1 / DB
    rstd = lax.rsqrt(sum2 / DB - mean * mean + 1e-05)
    norm_val = (conv_ref[...].astype(F32) - mean) * rstd
    zpre = norm_val * gain_ref[...]
    zsig = jax.nn.sigmoid(zpre)
    normed[...] = norm_val
    mixed[...] = (zpre * zsig).astype(BF)
    slope[...] = swish_slope(zpre, zsig) * gain_ref[...]
    scale[...] = jnp.broadcast_to(rstd, (128, 256))
    got(0, 3, 4)
    go(0, 7, 11)
    got(1, 3, 4)
    go(1, 7, 11)

    for copy in loads:
        copy.wait()

    def forward(m):
        pre_g = jnp.zeros((256, 224), F32)
        pre_u = jnp.zeros((256, 224), F32)
        d_act = jnp.zeros((256, 224), F32)
        for q in range(4):
            span = slice(q * 512, q * 512 + 512)
            rows = xc[0, m, q]
            pre_g += mm(rows, wg[:, span], NT)
            pre_u += mm(rows, wu[:, span], NT)
            d_act += mm(xc[1, m, q], wd[:, span], NT)
        sig = jax.nn.sigmoid(pre_g)
        d_gate = (d_act * pre_u * swish_slope(pre_g, sig)).astype(BF)
        d_up = (d_act * pre_g * sig).astype(BF)
        act_t[m] = (pre_g * sig * pre_u).T.astype(BF)
        dg_t[m] = d_gate.T
        du_t[m] = d_up.T
        return d_gate, d_up

    def back(m, d_gate, d_up, yy):
        span = pl.ds(pl.multiple_of(yy * 512, 512), 512)
        part[m, yy] = (mm(d_gate, wg[:, span], NN) + mm(d_up, wu[:, span], NN)).astype(BF)

    def sib_copy(gg, j, yy):
        return remote(
            part.at[gg * 2 + oc, yy], sib_in.at[gg, yy],
            sb_send.at[gg, j], sb_recv.at[gg, j], dev_s,
        )

    order = (y2, yp, ym, y)

    def whole(gg, cc, sent):
        m = gg * 2 + cc
        d_gate, d_up = forward(m)
        for j, yy in enumerate(order):
            back(m, d_gate, d_up, yy)
            if sent:
                sib_copy(gg, j, yy).start()

    whole(g, c, False)
    got(0, 8, 9, 10, 11)
    got(1, 8, 9, 10, 11)
    got(0, 5)
    go(0, 13)
    got(0, 6)
    go(0, 14)
    got(0, 7)
    go(0, 15)
    whole(g, oc, True)
    got(1, 5)
    go(1, 13)
    got(1, 6)
    go(1, 14)
    got(1, 7)
    go(1, 15)
    whole(og, c, False)
    got(0, 12, 13, 14, 15)
    got(1, 12, 13, 14, 15)
    whole(og, oc, True)

    def pair_sum(gg, j):
        yy = order[j]
        sib_copy_in = remote(
            part.at[gg * 2 + oc, yy], sib_in.at[gg, yy],
            sb_send.at[gg, j], sb_recv.at[gg, j], dev_s,
        )
        sib_copy_in.wait_recv()
        m = gg * 2 + c
        part[m, yy] = (part[m, yy].astype(F32) + sib_in[gg, yy].astype(F32)).astype(BF)

    def rs_copy(kind, src, dst, dev):
        return remote(src, dst, rs_send.at[kind], rs_recv.at[kind], dev)

    m_g, m_o = g * 2 + c, og * 2 + c
    pair_sum(og, 0)
    send_a = rs_copy(0, part.at[m_o, y2], in_a, dev_x)
    send_a.start()
    pair_sum(og, 1)
    send_bp = rs_copy(1, part.at[m_o, yp], in_b.at[0], dev_p)
    send_bp.start()
    pair_sum(og, 2)
    send_bm = rs_copy(2, part.at[m_o, ym], in_b.at[1], dev_m)
    send_bm.start()
    for j in range(3):
        pair_sum(g, j)
    pair_sum(og, 3)
    pair_sum(g, 3)

    def weight_grad(i, source, a):
        def tile(q, _):
            acc = mm(source[0], xc[a, 0, q], NN)
            for m in range(1, 4):
                acc += mm(source[m], xc[a, m, q], NN)
            gout[i, :, pl.ds(pl.multiple_of(q * 512, 512), 512)] = acc.astype(BF)
            return 0

        lax.fori_loop(0, 4, tile, 0)

    weight_grad(0, dg_t, 0)
    outs = [
        pltpu.make_async_copy(gout.at[i], ref, out_sem.at[i])
        for i, ref in enumerate((gg_hbm, gu_hbm, gd_hbm))
    ]
    outs[0].start()
    weight_grad(1, du_t, 0)
    outs[1].start()
    send_a.wait_recv()
    part[m_g, y2] = (part[m_g, y2].astype(F32) + in_a[...].astype(F32)).astype(BF)
    send_cp = rs_copy(3, part.at[m_g, y2, first], in_c.at[0], dev_p)
    send_cm = rs_copy(4, part.at[m_g, y2, second], in_c.at[1], dev_m)
    send_cp.start()
    send_cm.start()
    send_bp.wait_recv()
    send_bm.wait_recv()
    part[m_o, y] = (
        part[m_o, y].astype(F32) + in_b[0].astype(F32) + in_b[1].astype(F32)
    ).astype(BF)
    send_d = rs_copy(5, part.at[m_o, y], in_d, dev_x)
    send_d.start()
    weight_grad(2, act_t, 1)
    outs[2].start()
    send_cp.wait_recv()
    part[m_g, yp, first] = (part[m_g, yp, first].astype(F32) + in_c[0].astype(F32)).astype(BF)
    send_ep = rs_copy(6, part.at[m_g, yp], in_e.at[0], dev_p)
    send_ep.start()
    send_cm.wait_recv()
    part[m_g, ym, second] = (part[m_g, ym, second].astype(F32) + in_c[1].astype(F32)).astype(BF)
    send_em = rs_copy(7, part.at[m_g, ym], in_e.at[1], dev_m)
    send_em.start()
    send_d.wait_recv()
    send_ep.wait_recv()
    send_em.wait_recv()
    total[...] = (
        part[m_g, y].astype(F32) + in_d[...].astype(F32)
        + in_e[0].astype(F32) + in_e[1].astype(F32)
    ).astype(BF)

    def push_back(k, _):
        q = lax.rem(me + k, 16)
        remote(
            total.at[rows_of(q)], ret.at[rows_of(me)], ret_send.at[q], ret_recv.at[me], holder(q)
        ).start()
        return 0

    lax.fori_loop(1, 16, push_back, 0)
    own_back = pltpu.make_async_copy(total.at[rows_of(me)], ret.at[rows_of(me)], own_sem.at[0])
    own_back.start()

    def wait_back(k, _):
        q = lax.rem(me + 16 - k, 16)
        remote(
            total.at[rows_of(q)], ret.at[rows_of(q)], ret_send.at[q], ret_recv.at[q], holder(q)
        ).wait_recv()
        return 0

    lax.fori_loop(1, 16, wait_back, 0)
    own_back.wait()
    moe = mm(perm[...], ret[...], TN)
    res_ref[y] = (cq[...].astype(F32) + moe).astype(BF)

    half0, half1 = pl.ds(0, 64), pl.ds(64, 64)

    def res_copy(kind, ref, dev):
        return remote(ref, ref, res_send.at[kind], res_recv.at[kind], dev)

    sends = [res_copy(0, res_ref.at[y], dev_p), res_copy(1, res_ref.at[y], dev_m)]
    sends[0].start()
    sends[1].start()
    load_proj.wait()

    def gp_copy(q, j):
        pair = pl.ds(q * 2, 2)
        return remote(
            gp.at[oc, :, pair], gp_sib.at[:, pair], gs_send.at[j], gs_recv.at[j], dev_s
        )

    def proj_terms(q, j):
        feats = res_ref[q]
        term = mm(feats, mixed[...], TN)
        for i in range(8):
            for cc in range(2):
                gp[cc, i % 4, q * 2 + i // 4] = term[i * 64 + cc * 32 : i * 64 + cc * 32 + 32].astype(BF)
        gp_copy(q, j).start()
        return mm(feats, proj[pl.ds(pl.multiple_of(q * 512, 512), 512), :], NN)

    d_mixed = proj_terms(y, 0)
    res_copy(0, res_ref.at[ym], dev_m).wait_recv()
    sends.append(res_copy(2, res_ref.at[ym, half0], dev_p))
    sends[2].start()
    res_copy(1, res_ref.at[yp], dev_p).wait_recv()
    sends.append(res_copy(3, res_ref.at[yp, half1], dev_m))
    sends[3].start()
    d_mixed += proj_terms(ym, 1)
    d_mixed += proj_terms(yp, 2)
    res_copy(2, res_ref.at[y2, half0], dev_m).wait_recv()
    res_copy(3, res_ref.at[y2, half1], dev_p).wait_recv()
    d_mixed += proj_terms(y2, 3)
    d_norm = d_mixed * slope[...]
    norm_val = normed[...]
    stats2 = sums_out(
        1,
        jnp.sum(d_norm, axis=1, keepdims=True),
        jnp.sum(d_norm * norm_val, axis=1, keepdims=True),
    )
    for copy in stats2:
        copy.start()

    for j, q in enumerate((y, ym, yp, y2)):
        gp_copy(q, j).wait_recv()

    def pair_rows(xx):
        gp[c, xx] = (gp[c, xx].astype(F32) + gp_sib[xx].astype(F32)).astype(BF)

    def gx_copy(j):
        return remote(
            gp.at[c, others_x[j]], gp_x.at[j], gx_send.at[j], gx_recv.at[j], at_x(others_x[j])
        )

    for j in (1, 2, 0):
        pair_rows(others_x[j])
        gx_copy(j).start()
    pair_rows(x)

    first_sum, second_sum = sums_in(1, stats2)
    conv_grad = (
        scale[...] * (d_norm - first_sum / DB - norm_val * (second_sum / DB))
    ).astype(BF)
    halo_out[...] = conv_grad[0:32]
    halo = remote(halo_out, halo_in, halo_sem.at[0], halo_sem.at[1], dev_prev)
    halo.start()
    ext[0:128, :] = conv_grad.astype(F32)

    def correlate(start, count):
        acc = jnp.zeros((count, 256), F32)
        for k in range(WIDTH):
            acc += ext[start + k : start + k + count, :] * taps_ref[k : k + 1, :]
        return acc

    def glu_grads(start, count, unit_grad):
        span = slice(start, start + count)
        sig = jax.nn.sigmoid(gate_ref[span, :].astype(F32))
        gv_ref[span, :] = (unit_grad * sig).astype(BF)
        gt_ref[span, :] = (
            unit_grad * value_ref[span, :].astype(F32) * sig * (1.0 - sig)
        ).astype(BF)

    glu_grads(0, 64, correlate(0, 64))
    glu_grads(64, 32, correlate(64, 32))

    for j in range(3):
        gx_copy(j).wait_recv()

    def gz_copy(k):
        zz = lax.rem(z + k, 8)
        return remote(gp_row.at[zz], gp_z.at[k], gz_send.at[k], gz_recv.at[k], at_z(zz))

    gp_row[...] = (
        (gp[c, x].astype(F32) + gp_x[0].astype(F32)) + (gp_x[1].astype(F32) + gp_x[2].astype(F32))
    ).astype(BF)
    for k in (4, 3, 5, 2, 6, 1, 7):
        gz_copy(k).start()

    halo.wait_recv()
    keep = jnp.where(sp < 63, 1.0, 0.0)
    ext[128:160, :] = halo_in[...].astype(F32) * keep
    glu_grads(96, 32, correlate(96, 32))

    rows_sum = gp_row[z].astype(F32)
    for k in range(1, 8):
        gz_copy(k).wait_recv()
        rows_sum += gp_z[k].astype(F32)
    gp_ref[...] = rows_sum

    for copy in outs:
        copy.wait()
    for a in range(2):

        def drain(k, _, a=a):
            q = lax.rem(me + k, 16)
            remote(
                sendbuf.at[a, rows_of(q)], xc.at[a, m_own, y, rows_of(me)],
                a2a_send.at[a, q], a2a_recv.at[a, me], holder(q),
            ).wait_send()
            return 0

        lax.fori_loop(1, 16, drain, 0)
        for kind in range(16):
            ag_out(a, kind).wait_send()

    def drain_back(k, _):
        q = lax.rem(me + k, 16)
        remote(
            total.at[rows_of(q)], ret.at[rows_of(me)], ret_send.at[q], ret_recv.at[me], holder(q)
        ).wait_send()
        return 0

    lax.fori_loop(1, 16, drain_back, 0)
    for gg in (g, og):
        for j, yy in enumerate(order):
            sib_copy(gg, j, yy).wait_send()
    for copy in (send_a, send_bp, send_bm, send_cp, send_cm, send_d, send_ep, send_em, *sends):
        copy.wait_send()
    for copy in (*stats, *stats2, halo):
        copy.wait_send()
    for j, q in enumerate((y, ym, yp, y2)):
        gp_copy(q, j).wait_send()
    for j in range(3):
        gx_copy(j).wait_send()
    for k in range(1, 8):
        gz_copy(k).wait_send()


def local(
    moe_input,
    out_cotangent,
    routes,
    route_weight,
    w_gate,
    w_up,
    w_down,
    out_proj,
    conv_out,
    glu_value,
    glu_gate,
    taps,
    norm_gain,
):
    units, width = w_down.shape[1:]
    tokens, channels = conv_out.shape
    vmem = pl.BlockSpec(memory_space=pltpu.VMEM)
    hbm = pl.BlockSpec(memory_space=pl.ANY)
    dma = pltpu.SemaphoreType.DMA
    grad = jax.ShapeDtypeStruct((units, width), BF)
    glu = jax.ShapeDtypeStruct((tokens, channels), BF)
    gg, gu, gd, gp, gv, gt = pl.pallas_call(
        backward_kernel,
        out_shape=(grad, grad, grad, jax.ShapeDtypeStruct((32, channels), F32), glu, glu),
        in_specs=[vmem] * 7 + [hbm] * 6,
        out_specs=(hbm, hbm, hbm, vmem, vmem, vmem),
        scratch_shapes=[
            pltpu.VMEM((128, 512), BF),
            pltpu.VMEM((128, 512), BF),
            pltpu.VMEM((256, 128), BF),
            pltpu.VMEM((2, 256, 512), BF),
            pltpu.VMEM((2, 4, 4, 256, 512), BF),
            pltpu.VMEM((units, width), BF),
            pltpu.VMEM((units, width), BF),
            pltpu.VMEM((units, width), BF),
            pltpu.VMEM((4, units, 256), BF),
            pltpu.VMEM((4, units, 256), BF),
            pltpu.VMEM((4, units, 256), BF),
            pltpu.VMEM((3, units, width), BF),
            pltpu.VMEM((4, 4, 256, 512), BF),
            pltpu.VMEM((2, 4, 256, 512), BF),
            pltpu.VMEM((256, 512), BF),
            pltpu.VMEM((2, 256, 512), BF),
            pltpu.VMEM((2, 128, 512), BF),
            pltpu.VMEM((256, 512), BF),
            pltpu.VMEM((2, 256, 512), BF),
            pltpu.VMEM((256, 512), BF),
            pltpu.VMEM((256, 512), BF),
            pltpu.VMEM((4, 128, 512), BF),
            pltpu.VMEM((width, 256), BF),
            pltpu.VMEM((128, 256), F32),
            pltpu.VMEM((128, 256), F32),
            pltpu.VMEM((128, 256), BF),
            pltpu.VMEM((128, 256), F32),
            pltpu.VMEM((2, 8, 128), F32),
            pltpu.VMEM((2, 3, 8, 128), F32),
            pltpu.VMEM((160, 256), F32),
            pltpu.VMEM((32, 256), BF),
            pltpu.VMEM((32, 256), BF),
            pltpu.VMEM((2, 4, 8, 32, 256), BF),
            pltpu.VMEM((4, 8, 32, 256), BF),
            pltpu.VMEM((3, 8, 32, 256), BF),
            pltpu.VMEM((8, 32, 256), BF),
            pltpu.VMEM((8, 32, 256), BF),
            dma((6,)), dma((3,)), dma((2,)),
            dma((2, 16)), dma((2, 16)), dma((2, 16)), dma((2, 16)),
            dma((2, 4)), dma((2, 4)), dma((8,)), dma((8,)),
            dma((16,)), dma((16,)), dma((4,)), dma((4,)),
            dma((2, 3)), dma((2, 3)), dma((2,)),
            dma((4,)), dma((4,)), dma((3,)), dma((3,)), dma((8,)), dma((8,)),
        ],
        compiler_params=pltpu.CompilerParams(
            collective_id=0, has_side_effects=True, vmem_limit_bytes=60 * 1024 * 1024
        ),
        name="backward",
    )(
        routes.T, route_weight.T, conv_out, glu_value, glu_gate, taps, norm_gain[None, :],
        moe_input, out_cotangent, w_gate[0].T, w_up[0].T, w_down[0], out_proj,
    )
    return (gg.T[None], gu.T[None], gd[None], gp, gv, gt)


def solution(mesh):
    in_specs = (
        P("sp", None),
        P("sp", None),
        P("sp", None),
        P("sp", None),
        P("sp", None, "tp"),
        P("sp", None, "tp"),
        P("sp", "tp", None),
        P(None, "tp"),
        P("sp", "tp"),
        P("sp", "tp"),
        P("sp", "tp"),
        P(None, "tp"),
        P("tp"),
    )
    out_specs = (
        P("sp", None, "tp"),
        P("sp", None, "tp"),
        P("sp", "tp", None),
        P("sp", "tp"),
        P("sp", "tp"),
        P("sp", "tp"),
    )
    return jax.shard_map(local, mesh=mesh, in_specs=in_specs, out_specs=out_specs, check_vma=False)
```

```python
import jax
import jax.numpy as jnp
from jax import lax
from jax.experimental import pallas as pl
from jax.experimental.pallas import tpu as pltpu
from jax.sharding import PartitionSpec as P

DB = 1024
WIDTH = 31
MESH = pl.DeviceIdType.MESH
BF = jnp.bfloat16
F32 = jnp.float32
NT = (((1,), (1,)), ((), ()))
NN = (((1,), (0,)), ((), ()))
TN = (((0,), (0,)), ((), ()))


def mm(a, b, dims):
    return lax.dot_general(a, b, dims, preferred_element_type=F32)


def swish_slope(pre, sig):
    return sig * (1.0 + pre * (1.0 - sig))


def backward_kernel(
    routes_ref, weight_ref, gain_ref,
    x_hbm, cot_hbm, wg_hbm, wu_hbm, wd_hbm, proj_hbm, conv_hbm, value_hbm, gate_hbm, taps_hbm,
    gg_ref, gu_ref, gd_ref, gp_ref, gv_ref, gt_ref,
    xq, cq, perm, sendbuf, xc, wg, wu, wd, act_t, dg_t, du_t,
    part, sib_in, in_a, in_b, in_c, in_d, in_e, total, ret,
    conv_ref, value_ref, gate_ref, taps_ref, res_ref, proj, normed, slope, mixed, scale, st_out, st_in, ext, halo_out, halo_in,
    gp, gp_sib, gp_x, gp_row, gp_z,
    load_sem, own_sem, a2a_send, a2a_recv, ag_send, ag_recv,
    sb_send, sb_recv, rs_send, rs_recv, ret_send, ret_recv, res_send, res_recv,
    st_send, st_recv, halo_sem, gs_send, gs_recv, gx_send, gx_recv, gz_send, gz_recv,
):
    sp = lax.axis_index("sp")
    y = lax.axis_index("tp")
    c = lax.rem(sp, 2)
    x = lax.rem(sp // 2, 4)
    z = sp // 8
    xh = x // 2
    xl = lax.rem(x, 2)
    g = lax.rem(xl + xh, 2)
    og = 1 - g
    oc = 1 - c
    me = sp // 4
    yp, ym, y2 = lax.rem(y + 1, 4), lax.rem(y + 3, 4), lax.rem(y + 2, 4)

    def holder(q):
        qh = lax.rem(q, 2)
        qx = qh * 2 + lax.rem(g + qh, 2)
        return ((q // 2) * 8 + qx * 2 + c, y)

    dev_x = (z * 8 + (xh * 2 + 1 - xl) * 2 + c, y)
    dev_s = (z * 8 + x * 2 + oc, y)
    dev_p = (sp, yp)
    dev_m = (sp, ym)
    dev_2 = (sp, y2)
    dev_prev = (lax.rem(sp + 63, 64), y)
    dev_next = (lax.rem(sp + 1, 64), y)
    others_x = (xh * 2 + 1 - xl, (1 - xh) * 2 + xl, (1 - xh) * 2 + 1 - xl)

    def at_x(xx):
        return (z * 8 + xx * 2 + c, y)

    def at_z(zz):
        return (zz * 8 + x * 2 + c, y)

    def remote(src, dst, ss, rs, dev):
        return pltpu.make_async_remote_copy(
            src_ref=src, dst_ref=dst, send_sem=ss, recv_sem=rs, device_id=dev,
            device_id_type=MESH,
        )

    barrier = pltpu.get_barrier_semaphore()

    def greet(k, _):
        pl.semaphore_signal(barrier, inc=1, device_id=holder(lax.rem(me + k, 16)), device_id_type=MESH)
        return 0

    lax.fori_loop(1, 16, greet, 0)
    greeted = (
        dev_x, dev_s, dev_p, dev_m, dev_2, at_x(others_x[1]), at_x(others_x[2]), dev_prev, dev_next
    )
    for dev in greeted:
        pl.semaphore_signal(barrier, inc=1, device_id=dev, device_id_type=MESH)

    cols = pl.ds(pl.multiple_of(y * 512, 512), 512)
    load_x = pltpu.make_async_copy(x_hbm.at[:, cols], xq, load_sem.at[0])
    load_c = pltpu.make_async_copy(cot_hbm.at[:, cols], cq, load_sem.at[1])
    load_x.start()
    load_c.start()
    loads = [
        pltpu.make_async_copy(wg_hbm, wg, load_sem.at[2]),
        pltpu.make_async_copy(wu_hbm, wu, load_sem.at[3]),
        pltpu.make_async_copy(wd_hbm, wd, load_sem.at[4]),
    ]
    for copy in loads:
        copy.start()
    load_conv = pltpu.make_async_copy(conv_hbm, conv_ref, load_sem.at[5])
    load_conv.start()
    late_loads = [
        pltpu.make_async_copy(src, dst, load_sem.at[6 + i])
        for i, (src, dst) in enumerate((
            (proj_hbm, proj), (value_hbm, value_ref), (gate_hbm, gate_ref), (taps_hbm, taps_ref)
        ))
    ]
    for copy in late_loads:
        copy.start()

    r0 = routes_ref[0:1, :]
    r1 = routes_ref[1:2, :]
    ids = lax.broadcasted_iota(jnp.int32, (16, 128), 0)
    e0 = ids == r0
    e1 = ids == r1
    named = jnp.where(e0, 1.0, 0.0) + jnp.where(e1, 1.0, 0.0)
    before = jnp.where(
        lax.broadcasted_iota(jnp.int32, (128, 128), 0)
        < lax.broadcasted_iota(jnp.int32, (128, 128), 1),
        1.0, 0.0,
    ).astype(BF)
    earlier = mm(named.astype(BF), before, NN)
    t0 = r0.astype(F32) * 16.0 + jnp.sum(jnp.where(e0, earlier, 0.0), axis=0, keepdims=True)
    t1 = r1.astype(F32) * 16.0 + jnp.sum(jnp.where(e1, earlier, 0.0), axis=0, keepdims=True)
    place = lax.broadcasted_iota(jnp.int32, (256, 128), 0).astype(F32)
    p0 = place == t0
    p1 = place == t1
    perm_val = (jnp.where(p0, 1.0, 0.0) + jnp.where(p1, 1.0, 0.0)).astype(BF)
    perm[...] = perm_val
    w0 = weight_ref[0:1, :]
    w1 = weight_ref[1:2, :]
    w_slot = jnp.sum(jnp.where(p0, w0, 0.0) + jnp.where(p1, w1, 0.0), axis=1, keepdims=True)
    load_x.wait()
    sendbuf[0] = mm(perm_val, xq[...], NN).astype(BF)
    load_c.wait()
    sendbuf[1] = (w_slot * mm(perm_val, cq[...], NN)).astype(BF)

    pl.semaphore_wait(barrier, 24)

    m_own = g * 2 + c

    def rows_of(q):
        return pl.ds(pl.multiple_of(q * 16, 16), 16)

    for a in range(2):

        def push(k, _, a=a):
            q = lax.rem(me + k, 16)
            remote(
                sendbuf.at[a, rows_of(q)], xc.at[a, m_own, y, rows_of(me)],
                a2a_send.at[a, q], a2a_recv.at[a, me], holder(q),
            ).start()
            return 0

        lax.fori_loop(1, 16, push, 0)
    own = [
        pltpu.make_async_copy(
            sendbuf.at[a, rows_of(me)], xc.at[a, m_own, y, rows_of(me)], own_sem.at[a]
        )
        for a in range(2)
    ]
    own[0].start()
    own[1].start()

    def a2a_wait(a):
        def one(k, _):
            q = lax.rem(me + 16 - k, 16)
            remote(
                sendbuf.at[a, rows_of(q)], xc.at[a, m_own, y, rows_of(q)],
                a2a_send.at[a, q], a2a_recv.at[a, q], holder(q),
            ).wait_recv()
            return 0

        lax.fori_loop(1, 16, one, 0)
        own[a].wait()

    lane = lax.broadcasted_iota(jnp.int32, (128, 128), 1)

    def sums_out(phase, one, two):
        cols2 = jnp.where(lane == 0, one, 0.0) + jnp.where(lane == 1, two, 0.0)
        st_out[phase] = cols2.T[0:8, :]
        return [
            remote(
                st_out.at[phase], st_in.at[phase, j], st_send.at[phase, j], st_recv.at[phase, j], dev
            )
            for j, dev in enumerate((dev_p, dev_m, dev_2))
        ]

    def sums_in(phase, copies):
        for copy in copies:
            copy.wait_recv()
        tot = (st_out[phase] + st_in[phase, 2]) + (st_in[phase, 0] + st_in[phase, 1])
        tall = jnp.concatenate([tot, jnp.zeros((120, 128), F32)], axis=0).T
        return tall[:, 0:1], tall[:, 1:2]

    load_conv.wait()
    conv_vals = conv_ref[...].astype(F32)
    stats = sums_out(
        0,
        jnp.sum(conv_vals, axis=1, keepdims=True),
        jnp.sum(conv_vals * conv_vals, axis=1, keepdims=True),
    )
    for copy in stats:
        copy.start()

    first, second = pl.ds(0, 128), pl.ds(128, 128)
    listed = [(g, y), (g, ym), (g, yp), (g, y2), (og, y), (og, ym), (og, yp), (og, y2)]

    def block(a, gg, cc, yy):
        return xc.at[a, gg * 2 + cc, yy]

    def ag_copy(a, kind, ref, dev):
        return remote(ref, ref, ag_send.at[a, kind], ag_recv.at[a, kind], dev)

    def ag_out(a, kind):
        if kind >= 8:
            gg, yy = listed[kind - 8]
            return ag_copy(a, kind, block(a, gg, c, yy), dev_s)
        ref, dev = (
            (block(a, g, c, y), dev_x),
            (block(a, g, c, y), dev_p),
            (block(a, g, c, y), dev_m),
            (block(a, g, c, ym).at[first], dev_p),
            (block(a, g, c, yp).at[second], dev_m),
            (block(a, og, c, y), dev_p),
            (block(a, og, c, y), dev_m),
            (block(a, g, c, y2), dev_x),
        )[kind]
        return ag_copy(a, kind, ref, dev)

    def ag_in(a, kind):
        if kind >= 8:
            gg, yy = listed[kind - 8]
            return ag_copy(a, kind, block(a, gg, oc, yy), dev_s)
        ref, dev = (
            (block(a, og, c, y), dev_x),
            (block(a, g, c, ym), dev_m),
            (block(a, g, c, yp), dev_p),
            (block(a, g, c, y2).at[first], dev_m),
            (block(a, g, c, y2).at[second], dev_p),
            (block(a, og, c, ym), dev_m),
            (block(a, og, c, yp), dev_p),
            (block(a, og, c, y2), dev_x),
        )[kind]
        return ag_copy(a, kind, ref, dev)

    def go(a, *kinds):
        for kind in kinds:
            ag_out(a, kind).start()

    def got(a, *kinds):
        for kind in kinds:
            ag_in(a, kind).wait_recv()

    a2a_wait(0)
    go(0, 0, 1, 2, 8)
    a2a_wait(1)
    go(1, 0, 1, 2, 8)
    got(0, 1)
    go(0, 3, 9)
    got(0, 2)
    go(0, 4, 10)
    got(1, 1)
    go(1, 3, 9)
    got(1, 2)
    go(1, 4, 10)
    got(0, 0)
    go(0, 5, 6, 12)
    got(1, 0)
    go(1, 5, 6, 12)
    sum1, sum2 = sums_in(0, stats)
    mean = sum1 / DB
    rstd = lax.rsqrt(sum2 / DB - mean * mean + 1e-05)
    norm_val = (conv_ref[...].astype(F32) - mean) * rstd
    zpre = norm_val * gain_ref[...]
    zsig = jax.nn.sigmoid(zpre)
    normed[...] = norm_val
    mixed[...] = (zpre * zsig).astype(BF)
    slope[...] = swish_slope(zpre, zsig) * gain_ref[...]
    scale[...] = jnp.broadcast_to(rstd, (128, 256))
    got(0, 3, 4)
    go(0, 7, 11)
    got(1, 3, 4)
    go(1, 7, 11)

    for copy in loads:
        copy.wait()

    def forward(m):
        pre_g = jnp.zeros((256, 224), F32)
        pre_u = jnp.zeros((256, 224), F32)
        d_act = jnp.zeros((256, 224), F32)
        for q in range(4):
            span = slice(q * 512, q * 512 + 512)
            rows = xc[0, m, q]
            pre_g += mm(rows, wg[:, span], NT)
            pre_u += mm(rows, wu[:, span], NT)
            d_act += mm(xc[1, m, q], wd[:, span], NT)
        sig = jax.nn.sigmoid(pre_g)
        d_gate = (d_act * pre_u * swish_slope(pre_g, sig)).astype(BF)
        d_up = (d_act * pre_g * sig).astype(BF)
        act_t[m] = (pre_g * sig * pre_u).T.astype(BF)
        dg_t[m] = d_gate.T
        du_t[m] = d_up.T
        return d_gate, d_up

    def back(m, d_gate, d_up, yy):
        span = pl.ds(pl.multiple_of(yy * 512, 512), 512)
        part[m, yy] = (mm(d_gate, wg[:, span], NN) + mm(d_up, wu[:, span], NN)).astype(BF)

    def sib_copy(gg, j, yy):
        return remote(
            part.at[gg * 2 + oc, yy], sib_in.at[gg, yy],
            sb_send.at[gg, j], sb_recv.at[gg, j], dev_s,
        )

    order = (y2, yp, ym, y)

    def whole(gg, cc, sent):
        m = gg * 2 + cc
        d_gate, d_up = forward(m)
        for j, yy in enumerate(order):
            back(m, d_gate, d_up, yy)
            if sent:
                sib_copy(gg, j, yy).start()

    whole(g, c, False)
    got(0, 8, 9, 10, 11)
    got(1, 8, 9, 10, 11)
    got(0, 5)
    go(0, 13)
    got(0, 6)
    go(0, 14)
    got(0, 7)
    go(0, 15)
    whole(g, oc, True)
    got(1, 5)
    go(1, 13)
    got(1, 6)
    go(1, 14)
    got(1, 7)
    go(1, 15)
    whole(og, c, False)
    got(0, 12, 13, 14, 15)
    got(1, 12, 13, 14, 15)
    whole(og, oc, True)

    def pair_sum(gg, j):
        yy = order[j]
        sib_copy_in = remote(
            part.at[gg * 2 + oc, yy], sib_in.at[gg, yy],
            sb_send.at[gg, j], sb_recv.at[gg, j], dev_s,
        )
        sib_copy_in.wait_recv()
        m = gg * 2 + c
        part[m, yy] = (part[m, yy].astype(F32) + sib_in[gg, yy].astype(F32)).astype(BF)

    def rs_copy(kind, src, dst, dev):
        return remote(src, dst, rs_send.at[kind], rs_recv.at[kind], dev)

    m_g, m_o = g * 2 + c, og * 2 + c
    pair_sum(og, 0)
    send_a = rs_copy(0, part.at[m_o, y2], in_a, dev_x)
    send_a.start()
    pair_sum(og, 1)
    send_bp = rs_copy(1, part.at[m_o, yp], in_b.at[0], dev_p)
    send_bp.start()
    pair_sum(og, 2)
    send_bm = rs_copy(2, part.at[m_o, ym], in_b.at[1], dev_m)
    send_bm.start()
    for j in range(3):
        pair_sum(g, j)
    pair_sum(og, 3)
    pair_sum(g, 3)

    def weight_grad(out_ref, source, a):
        def tile(q, _):
            acc = mm(source[0], xc[a, 0, q], NN)
            for m in range(1, 4):
                acc += mm(source[m], xc[a, m, q], NN)
            out_ref[:, pl.ds(pl.multiple_of(q * 512, 512), 512)] = acc.astype(BF)
            return 0

        lax.fori_loop(0, 4, tile, 0)

    weight_grad(gg_ref, dg_t, 0)
    weight_grad(gu_ref, du_t, 0)
    send_a.wait_recv()
    part[m_g, y2] = (part[m_g, y2].astype(F32) + in_a[...].astype(F32)).astype(BF)
    send_cp = rs_copy(3, part.at[m_g, y2, first], in_c.at[0], dev_p)
    send_cm = rs_copy(4, part.at[m_g, y2, second], in_c.at[1], dev_m)
    send_cp.start()
    send_cm.start()
    send_bp.wait_recv()
    send_bm.wait_recv()
    part[m_o, y] = (
        part[m_o, y].astype(F32) + in_b[0].astype(F32) + in_b[1].astype(F32)
    ).astype(BF)
    send_d = rs_copy(5, part.at[m_o, y], in_d, dev_x)
    send_d.start()
    weight_grad(gd_ref, act_t, 1)
    send_cp.wait_recv()
    part[m_g, yp, first] = (part[m_g, yp, first].astype(F32) + in_c[0].astype(F32)).astype(BF)
    send_ep = rs_copy(6, part.at[m_g, yp], in_e.at[0], dev_p)
    send_ep.start()
    send_cm.wait_recv()
    part[m_g, ym, second] = (part[m_g, ym, second].astype(F32) + in_c[1].astype(F32)).astype(BF)
    send_em = rs_copy(7, part.at[m_g, ym], in_e.at[1], dev_m)
    send_em.start()
    send_d.wait_recv()
    send_ep.wait_recv()
    send_em.wait_recv()
    total[...] = (
        part[m_g, y].astype(F32) + in_d[...].astype(F32)
        + in_e[0].astype(F32) + in_e[1].astype(F32)
    ).astype(BF)

    def push_back(k, _):
        q = lax.rem(me + k, 16)
        remote(
            total.at[rows_of(q)], ret.at[rows_of(me)], ret_send.at[q], ret_recv.at[me], holder(q)
        ).start()
        return 0

    lax.fori_loop(1, 16, push_back, 0)
    own_back = pltpu.make_async_copy(total.at[rows_of(me)], ret.at[rows_of(me)], own_sem.at[0])
    own_back.start()

    def wait_back(k, _):
        q = lax.rem(me + 16 - k, 16)
        remote(
            total.at[rows_of(q)], ret.at[rows_of(q)], ret_send.at[q], ret_recv.at[q], holder(q)
        ).wait_recv()
        return 0

    lax.fori_loop(1, 16, wait_back, 0)
    own_back.wait()
    moe = mm(perm[...], ret[...], TN)
    res_ref[y] = (cq[...].astype(F32) + moe).astype(BF)

    half0, half1 = pl.ds(0, 64), pl.ds(64, 64)

    def res_copy(kind, ref, dev):
        return remote(ref, ref, res_send.at[kind], res_recv.at[kind], dev)

    def res_out(kind):
        ref, dev = (
            (res_ref.at[y, half0], dev_p), (res_ref.at[y, half1], dev_p),
            (res_ref.at[y, half1], dev_m), (res_ref.at[y, half0], dev_m),
            (res_ref.at[ym, half0], dev_p), (res_ref.at[yp, half1], dev_m),
        )[kind]
        return res_copy(kind, ref, dev)

    def res_in(kind):
        ref, dev = (
            (res_ref.at[ym, half0], dev_m), (res_ref.at[ym, half1], dev_m),
            (res_ref.at[yp, half1], dev_p), (res_ref.at[yp, half0], dev_p),
            (res_ref.at[y2, half0], dev_m), (res_ref.at[y2, half1], dev_p),
        )[kind]
        return res_copy(kind, ref, dev)

    for kind in (0, 2, 1, 3):
        res_out(kind).start()
    for copy in late_loads:
        copy.wait()

    def pair_of(q):
        return pl.ds(q * 2, 2)

    def gp_copy(q, j):
        return remote(
            gp.at[oc, :, pair_of(q)], gp_sib.at[:, pair_of(q)], gs_send.at[j], gs_recv.at[j], dev_s
        )

    def proj_terms(q, j):
        feats = res_ref[q]
        term = mm(feats, mixed[...], TN)
        for i in range(8):
            for cc in range(2):
                gp[cc, i % 4, q * 2 + i // 4] = term[i * 64 + cc * 32 : i * 64 + cc * 32 + 32].astype(BF)
        gp_copy(q, j).start()
        return mm(feats, proj[pl.ds(pl.multiple_of(q * 512, 512), 512), :], NN)

    def gx_copy(q, j, i):
        return remote(
            gp.at[c, others_x[i], pair_of(q)], gp_x.at[i, pair_of(q)],
            gx_send.at[j, i], gx_recv.at[j, i], at_x(others_x[i]),
        )

    def over_x(q, j):
        gp_copy(q, j).wait_recv()
        gp[c, :, pair_of(q)] = (
            gp[c, :, pair_of(q)].astype(F32) + gp_sib[:, pair_of(q)].astype(F32)
        ).astype(BF)
        for i in (1, 2, 0):
            gx_copy(q, j, i).start()

    def gz_copy(to, slot):
        return remote(gp_row.at[to], gp_z.at[slot], gz_send.at[to], gz_recv.at[slot], at_z(to))

    def over_z(q, j):
        for i in range(3):
            gx_copy(q, j, i).wait_recv()
        pair = pair_of(q)
        gp_row[pair] = (
            (gp[c, x, pair].astype(F32) + gp_x[0, pair].astype(F32))
            + (gp_x[1, pair].astype(F32) + gp_x[2, pair].astype(F32))
        ).astype(BF)
        for i in range(2):

            @pl.when(q * 2 + i != z)
            def _():
                gz_copy(q * 2 + i, z).start()

    d_mixed = proj_terms(y, 0)
    res_in(0).wait_recv()
    res_out(4).start()
    res_in(2).wait_recv()
    res_out(5).start()
    over_x(y, 0)
    res_in(1).wait_recv()
    d_mixed += proj_terms(ym, 1)
    res_in(3).wait_recv()
    d_mixed += proj_terms(yp, 2)
    over_x(ym, 1)
    over_x(yp, 2)
    res_in(4).wait_recv()
    res_in(5).wait_recv()
    d_mixed += proj_terms(y2, 3)
    d_norm = d_mixed * slope[...]
    norm_val = normed[...]
    stats2 = sums_out(
        1,
        jnp.sum(d_norm, axis=1, keepdims=True),
        jnp.sum(d_norm * norm_val, axis=1, keepdims=True),
    )
    for copy in stats2:
        copy.start()
    over_x(y2, 3)
    over_z(y, 0)
    over_z(ym, 1)
    over_z(yp, 2)

    first_sum, second_sum = sums_in(1, stats2)
    conv_grad = (
        scale[...] * (d_norm - first_sum / DB - norm_val * (second_sum / DB))
    ).astype(BF)
    halo_out[...] = conv_grad[0:32]
    halo = remote(halo_out, halo_in, halo_sem.at[0], halo_sem.at[1], dev_prev)
    halo.start()
    ext[0:128, :] = conv_grad.astype(F32)

    def correlate(start, count):
        acc = jnp.zeros((count, 256), F32)
        for k in range(WIDTH):
            acc += ext[start + k : start + k + count, :] * taps_ref[k : k + 1, :]
        return acc

    def glu_grads(start, count, unit_grad):
        span = slice(start, start + count)
        sig = jax.nn.sigmoid(gate_ref[span, :].astype(F32))
        gv_ref[span, :] = (unit_grad * sig).astype(BF)
        gt_ref[span, :] = (
            unit_grad * value_ref[span, :].astype(F32) * sig * (1.0 - sig)
        ).astype(BF)

    glu_grads(0, 64, correlate(0, 64))
    glu_grads(64, 32, correlate(64, 32))

    over_z(y2, 3)
    halo.wait_recv()
    keep = jnp.where(sp < 63, 1.0, 0.0)
    ext[128:160, :] = halo_in[...].astype(F32) * keep
    glu_grads(96, 32, correlate(96, 32))

    rows_sum = gp_row[z].astype(F32)
    for k in range(1, 8):
        zz = lax.rem(z + k, 8)
        gz_copy(zz, zz).wait_recv()
        rows_sum += gp_z[zz].astype(F32)
    gp_ref[...] = rows_sum

    for a in range(2):

        def drain(k, _, a=a):
            q = lax.rem(me + k, 16)
            remote(
                sendbuf.at[a, rows_of(q)], xc.at[a, m_own, y, rows_of(me)],
                a2a_send.at[a, q], a2a_recv.at[a, me], holder(q),
            ).wait_send()
            return 0

        lax.fori_loop(1, 16, drain, 0)
        for kind in range(16):
            ag_out(a, kind).wait_send()

    def drain_back(k, _):
        q = lax.rem(me + k, 16)
        remote(
            total.at[rows_of(q)], ret.at[rows_of(me)], ret_send.at[q], ret_recv.at[me], holder(q)
        ).wait_send()
        return 0

    lax.fori_loop(1, 16, drain_back, 0)
    for gg in (g, og):
        for j, yy in enumerate(order):
            sib_copy(gg, j, yy).wait_send()
    for copy in (send_a, send_bp, send_bm, send_cp, send_cm, send_d, send_ep, send_em):
        copy.wait_send()
    for copy in (*stats, *stats2, halo):
        copy.wait_send()
    for kind in range(6):
        res_out(kind).wait_send()
    for j, q in enumerate((y, ym, yp, y2)):
        gp_copy(q, j).wait_send()
        for i in range(3):
            gx_copy(q, j, i).wait_send()
    for k in range(1, 8):
        gz_copy(lax.rem(z + k, 8), z).wait_send()


def write_kernel(*refs):
    copies = [pltpu.make_async_copy(refs[i], refs[6 + i], refs[12].at[i]) for i in range(6)]
    for copy in copies:
        copy.start()
    for copy in copies:
        copy.wait()


def local(
    moe_input,
    out_cotangent,
    routes,
    route_weight,
    w_gate,
    w_up,
    w_down,
    out_proj,
    conv_out,
    glu_value,
    glu_gate,
    taps,
    norm_gain,
):
    units, width = w_down.shape[1:]
    tokens, channels = conv_out.shape
    vmem = pl.BlockSpec(memory_space=pltpu.VMEM)
    hbm = pl.BlockSpec(memory_space=pl.ANY)
    dma = pltpu.SemaphoreType.DMA
    grad = jax.ShapeDtypeStruct((units, width), BF)
    glu = jax.ShapeDtypeStruct((tokens, channels), BF)
    shapes = (grad, grad, grad, jax.ShapeDtypeStruct((32, channels), F32), glu, glu)
    results = pl.pallas_call(
        backward_kernel,
        out_shape=[pltpu.VMEM(a.shape, a.dtype) for a in shapes],
        in_specs=[vmem] * 3 + [hbm] * 10,
        out_specs=[vmem] * 6,
        scratch_shapes=[
            pltpu.VMEM((128, 512), BF),
            pltpu.VMEM((128, 512), BF),
            pltpu.VMEM((256, 128), BF),
            pltpu.VMEM((2, 256, 512), BF),
            pltpu.VMEM((2, 4, 4, 256, 512), BF),
            pltpu.VMEM((units, width), BF),
            pltpu.VMEM((units, width), BF),
            pltpu.VMEM((units, width), BF),
            pltpu.VMEM((4, units, 256), BF),
            pltpu.VMEM((4, units, 256), BF),
            pltpu.VMEM((4, units, 256), BF),
            pltpu.VMEM((4, 4, 256, 512), BF),
            pltpu.VMEM((2, 4, 256, 512), BF),
            pltpu.VMEM((256, 512), BF),
            pltpu.VMEM((2, 256, 512), BF),
            pltpu.VMEM((2, 128, 512), BF),
            pltpu.VMEM((256, 512), BF),
            pltpu.VMEM((2, 256, 512), BF),
            pltpu.VMEM((256, 512), BF),
            pltpu.VMEM((256, 512), BF),
            pltpu.VMEM((tokens, channels), BF),
            pltpu.VMEM((tokens, channels), BF),
            pltpu.VMEM((tokens, channels), BF),
            pltpu.VMEM((WIDTH, channels), F32),
            pltpu.VMEM((4, 128, 512), BF),
            pltpu.VMEM((width, 256), BF),
            pltpu.VMEM((128, 256), F32),
            pltpu.VMEM((128, 256), F32),
            pltpu.VMEM((128, 256), BF),
            pltpu.VMEM((128, 256), F32),
            pltpu.VMEM((2, 8, 128), F32),
            pltpu.VMEM((2, 3, 8, 128), F32),
            pltpu.VMEM((160, 256), F32),
            pltpu.VMEM((32, 256), BF),
            pltpu.VMEM((32, 256), BF),
            pltpu.VMEM((2, 4, 8, 32, 256), BF),
            pltpu.VMEM((4, 8, 32, 256), BF),
            pltpu.VMEM((3, 8, 32, 256), BF),
            pltpu.VMEM((8, 32, 256), BF),
            pltpu.VMEM((8, 32, 256), BF),
            dma((10,)), dma((2,)),
            dma((2, 16)), dma((2, 16)), dma((2, 16)), dma((2, 16)),
            dma((2, 4)), dma((2, 4)), dma((8,)), dma((8,)),
            dma((16,)), dma((16,)), dma((6,)), dma((6,)),
            dma((2, 3)), dma((2, 3)), dma((2,)),
            dma((4,)), dma((4,)), dma((4, 3)), dma((4, 3)), dma((8,)), dma((8,)),
        ],
        compiler_params=pltpu.CompilerParams(
            collective_id=0, has_side_effects=True, vmem_limit_bytes=60 * 1024 * 1024
        ),
        name="backward",
    )(
        routes.T, route_weight.T, norm_gain[None, :],
        moe_input, out_cotangent, w_gate[0].T, w_up[0].T, w_down[0], out_proj,
        conv_out, glu_value, glu_gate, taps,
    )
    gg, gu, gd, gp, gv, gt = pl.pallas_call(
        write_kernel,
        out_shape=shapes,
        in_specs=[vmem] * 6,
        out_specs=[hbm] * 6,
        scratch_shapes=[dma((6,))],
        compiler_params=pltpu.CompilerParams(vmem_limit_bytes=1024 * 1024),
        name="write_out",
    )(*(pltpu.with_memory_space_constraint(r, pltpu.VMEM) for r in results))
    return (gg.T[None], gu.T[None], gd[None], gp, gv, gt)


def solution(mesh):
    in_specs = (
        P("sp", None),
        P("sp", None),
        P("sp", None),
        P("sp", None),
        P("sp", None, "tp"),
        P("sp", None, "tp"),
        P("sp", "tp", None),
        P(None, "tp"),
        P("sp", "tp"),
        P("sp", "tp"),
        P("sp", "tp"),
        P(None, "tp"),
        P("tp"),
    )
    out_specs = (
        P("sp", None, "tp"),
        P("sp", None, "tp"),
        P("sp", "tp", None),
        P("sp", "tp"),
        P("sp", "tp"),
        P("sp", "tp"),
    )
    return jax.shard_map(local, mesh=mesh, in_specs=in_specs, out_specs=out_specs, check_vma=False)
```

```python
import jax
import jax.numpy as jnp
from jax import lax
from jax.experimental import pallas as pl
from jax.experimental.pallas import tpu as pltpu
from jax.sharding import PartitionSpec as P

DB = 1024
WIDTH = 31
MESH = pl.DeviceIdType.MESH
BF = jnp.bfloat16
F32 = jnp.float32
NEAR = (0, 1, 7, 2, 6, 3, 5, 4)
NT = (((1,), (1,)), ((), ()))
NN = (((1,), (0,)), ((), ()))
TN = (((0,), (0,)), ((), ()))


def mm(a, b, dims):
    return lax.dot_general(a, b, dims, preferred_element_type=F32)


def swish_slope(pre, sig):
    return sig * (1.0 + pre * (1.0 - sig))


def backward_kernel(
    routes_ref, weight_ref, gain_ref,
    x_hbm, cot_hbm, wg_hbm, wu_hbm, wd_hbm, proj_hbm, conv_hbm, value_hbm, gate_hbm, taps_hbm,
    gg_ref, gu_ref, gd_ref, gp_ref, gv_ref, gt_ref,
    xq, cq, perm, sendbuf, xc, wg, wu, wd, act_t, dg_t, du_t,
    part, sib_in, in_a, in_b, in_c, in_d, in_e, total, ret,
    conv_ref, value_ref, gate_ref, taps_ref, res_ref, proj, normed, slope, mixed, scale, st_out, st_in, ext, halo_out, halo_in,
    gp, gp_sib, gp_x, gp_row, gp_z,
    load_sem, own_sem, a2a_send, a2a_recv, ag_send, ag_recv,
    sb_send, sb_recv, rs_send, rs_recv, ret_send, ret_recv, res_send, res_recv,
    st_send, st_recv, halo_sem, gs_send, gs_recv, gx_send, gx_recv, gz_send, gz_recv,
):
    sp = lax.axis_index("sp")
    y = lax.axis_index("tp")
    c = lax.rem(sp, 2)
    x = lax.rem(sp // 2, 4)
    z = sp // 8
    xh = x // 2
    xl = lax.rem(x, 2)
    g = lax.rem(xl + xh, 2)
    og = 1 - g
    oc = 1 - c
    me = sp // 4
    yp, ym, y2 = lax.rem(y + 1, 4), lax.rem(y + 3, 4), lax.rem(y + 2, 4)

    def holder(zz, hh):
        return (zz * 8 + (hh * 2 + lax.rem(g + hh, 2)) * 2 + c, y)

    def to_of(p):
        return lax.rem(z + 8 - NEAR[p // 2], 8), (xh if p % 2 == 0 else 1 - xh)

    def from_of(p):
        return lax.rem(z + NEAR[p // 2], 8), (xh if p % 2 == 0 else 1 - xh)

    dev_x = (z * 8 + (xh * 2 + 1 - xl) * 2 + c, y)
    dev_s = (z * 8 + x * 2 + oc, y)
    dev_p = (sp, yp)
    dev_m = (sp, ym)
    dev_2 = (sp, y2)
    dev_prev = (lax.rem(sp + 63, 64), y)
    dev_next = (lax.rem(sp + 1, 64), y)
    others_x = (xh * 2 + 1 - xl, (1 - xh) * 2 + xl, (1 - xh) * 2 + 1 - xl)

    def at_x(xx):
        return (z * 8 + xx * 2 + c, y)

    def at_z(zz):
        return (zz * 8 + x * 2 + c, y)

    def remote(src, dst, ss, rs, dev):
        return pltpu.make_async_remote_copy(
            src_ref=src, dst_ref=dst, send_sem=ss, recv_sem=rs, device_id=dev,
            device_id_type=MESH,
        )

    barrier = pltpu.get_barrier_semaphore()

    for p in range(1, 16):
        pl.semaphore_signal(barrier, inc=1, device_id=holder(*to_of(p)), device_id_type=MESH)
    greeted = (
        dev_x, dev_s, dev_p, dev_m, dev_2, at_x(others_x[1]), at_x(others_x[2]), dev_prev, dev_next
    )
    for dev in greeted:
        pl.semaphore_signal(barrier, inc=1, device_id=dev, device_id_type=MESH)

    cols = pl.ds(pl.multiple_of(y * 512, 512), 512)
    load_x = pltpu.make_async_copy(x_hbm.at[:, cols], xq, load_sem.at[0])
    load_c = pltpu.make_async_copy(cot_hbm.at[:, cols], cq, load_sem.at[1])
    load_x.start()
    load_c.start()
    loads = [
        pltpu.make_async_copy(wg_hbm, wg, load_sem.at[2]),
        pltpu.make_async_copy(wu_hbm, wu, load_sem.at[3]),
        pltpu.make_async_copy(wd_hbm, wd, load_sem.at[4]),
    ]
    for copy in loads:
        copy.start()
    load_conv = pltpu.make_async_copy(conv_hbm, conv_ref, load_sem.at[5])
    load_conv.start()
    late_loads = [
        pltpu.make_async_copy(src, dst, load_sem.at[6 + i])
        for i, (src, dst) in enumerate((
            (proj_hbm, proj), (value_hbm, value_ref), (gate_hbm, gate_ref), (taps_hbm, taps_ref)
        ))
    ]
    for copy in late_loads:
        copy.start()

    r0 = routes_ref[0:1, :]
    r1 = routes_ref[1:2, :]
    ids = lax.broadcasted_iota(jnp.int32, (16, 128), 0)
    e0 = ids == r0
    e1 = ids == r1
    named = jnp.where(e0, 1.0, 0.0) + jnp.where(e1, 1.0, 0.0)
    before = jnp.where(
        lax.broadcasted_iota(jnp.int32, (128, 128), 0)
        < lax.broadcasted_iota(jnp.int32, (128, 128), 1),
        1.0, 0.0,
    ).astype(BF)
    earlier = mm(named.astype(BF), before, NN)
    t0 = r0.astype(F32) * 16.0 + jnp.sum(jnp.where(e0, earlier, 0.0), axis=0, keepdims=True)
    t1 = r1.astype(F32) * 16.0 + jnp.sum(jnp.where(e1, earlier, 0.0), axis=0, keepdims=True)
    place = lax.broadcasted_iota(jnp.int32, (256, 128), 0).astype(F32)
    p0 = place == t0
    p1 = place == t1
    perm_val = (jnp.where(p0, 1.0, 0.0) + jnp.where(p1, 1.0, 0.0)).astype(BF)
    perm[...] = perm_val
    w0 = weight_ref[0:1, :]
    w1 = weight_ref[1:2, :]
    w_slot = jnp.sum(jnp.where(p0, w0, 0.0) + jnp.where(p1, w1, 0.0), axis=1, keepdims=True)
    load_x.wait()
    sendbuf[0] = mm(perm_val, xq[...], NN).astype(BF)
    load_c.wait()
    sendbuf[1] = (w_slot * mm(perm_val, cq[...], NN)).astype(BF)

    pl.semaphore_wait(barrier, 24)

    m_own = g * 2 + c

    def rows_of(q):
        return pl.ds(pl.multiple_of(q * 16, 16), 16)

    def place_of(a, p):
        return xc.at[a, p // 8, m_own, y, pl.ds(p % 8 * 16, 16)]

    def out_copy(a, p):
        zz, hh = to_of(p)
        return remote(
            sendbuf.at[a, rows_of(zz * 2 + hh)], place_of(a, p),
            a2a_send.at[a, p], a2a_recv.at[a, p], holder(zz, hh),
        )

    def a2a_wait(a, h):
        for p in range(8 * h, 8 * h + 8):
            if p == 0:
                own[a].wait()
            else:
                out_copy(a, p).wait_recv()

    own = [
        pltpu.make_async_copy(sendbuf.at[a, rows_of(me)], place_of(a, 0), own_sem.at[a])
        for a in range(2)
    ]
    for h in range(2):
        for a in range(2):
            if h == 0:
                own[a].start()
            for p in range(max(8 * h, 1), 8 * h + 8):
                out_copy(a, p).start()

    lane = lax.broadcasted_iota(jnp.int32, (128, 128), 1)

    def sums_out(phase, one, two):
        cols2 = jnp.where(lane == 0, one, 0.0) + jnp.where(lane == 1, two, 0.0)
        st_out[phase] = cols2.T[0:8, :]
        return [
            remote(
                st_out.at[phase], st_in.at[phase, j], st_send.at[phase, j], st_recv.at[phase, j], dev
            )
            for j, dev in enumerate((dev_p, dev_m, dev_2))
        ]

    def sums_in(phase, copies):
        for copy in copies:
            copy.wait_recv()
        tot = (st_out[phase] + st_in[phase, 2]) + (st_in[phase, 0] + st_in[phase, 1])
        tall = jnp.concatenate([tot, jnp.zeros((120, 128), F32)], axis=0).T
        return tall[:, 0:1], tall[:, 1:2]

    load_conv.wait()
    conv_vals = conv_ref[...].astype(F32)
    stats = sums_out(
        0,
        jnp.sum(conv_vals, axis=1, keepdims=True),
        jnp.sum(conv_vals * conv_vals, axis=1, keepdims=True),
    )
    for copy in stats:
        copy.start()

    first, second = pl.ds(0, 64), pl.ds(64, 64)
    listed = [(g, y), (g, ym), (g, yp), (g, y2), (og, y), (og, ym), (og, yp), (og, y2)]

    def block(a, h, gg, cc, yy):
        return xc.at[a, h, gg * 2 + cc, yy]

    def ag_copy(a, h, kind, ref, dev):
        return remote(ref, ref, ag_send.at[a * 2 + h, kind], ag_recv.at[a * 2 + h, kind], dev)

    def ag_out(a, h, kind):
        if kind >= 8:
            gg, yy = listed[kind - 8]
            return ag_copy(a, h, kind, block(a, h, gg, c, yy), dev_s)
        ref, dev = (
            (block(a, h, g, c, y), dev_x),
            (block(a, h, g, c, y), dev_p),
            (block(a, h, g, c, y), dev_m),
            (block(a, h, g, c, ym).at[first], dev_p),
            (block(a, h, g, c, yp).at[second], dev_m),
            (block(a, h, og, c, y), dev_p),
            (block(a, h, og, c, y), dev_m),
            (block(a, h, g, c, y2), dev_x),
        )[kind]
        return ag_copy(a, h, kind, ref, dev)

    def ag_in(a, h, kind):
        if kind >= 8:
            gg, yy = listed[kind - 8]
            return ag_copy(a, h, kind, block(a, h, gg, oc, yy), dev_s)
        ref, dev = (
            (block(a, h, og, c, y), dev_x),
            (block(a, h, g, c, ym), dev_m),
            (block(a, h, g, c, yp), dev_p),
            (block(a, h, g, c, y2).at[first], dev_m),
            (block(a, h, g, c, y2).at[second], dev_p),
            (block(a, h, og, c, ym), dev_m),
            (block(a, h, og, c, yp), dev_p),
            (block(a, h, og, c, y2), dev_x),
        )[kind]
        return ag_copy(a, h, kind, ref, dev)

    def go(a, h, *kinds):
        for kind in kinds:
            ag_out(a, h, kind).start()

    def got(a, h, *kinds):
        for kind in kinds:
            ag_in(a, h, kind).wait_recv()

    def relay_y(a, h):
        got(a, h, 1)
        go(a, h, 3, 9)
        got(a, h, 2)
        go(a, h, 4, 10)

    def relay_x(a, h):
        got(a, h, 0)
        go(a, h, 5, 6, 12)

    def relay_far(a, h):
        got(a, h, 3, 4)
        go(a, h, 7, 11)

    def relay_last(a, h):
        got(a, h, 5)
        go(a, h, 13)
        got(a, h, 6)
        go(a, h, 14)
        got(a, h, 7)
        go(a, h, 15)

    def pair(gg):
        return pl.ds(gg * 2, 2)

    def rows_at(a, h, gg, q):
        return xc[a, h, pair(gg), q].reshape(256, 512)

    def forward(h, gg):
        pre_g = jnp.zeros((256, 224), F32)
        pre_u = jnp.zeros((256, 224), F32)
        d_act = jnp.zeros((256, 224), F32)
        for q in range(4):
            span = slice(q * 512, q * 512 + 512)
            rows = rows_at(0, h, gg, q)
            pre_g += mm(rows, wg[:, span], NT)
            pre_u += mm(rows, wu[:, span], NT)
            d_act += mm(rows_at(1, h, gg, q), wd[:, span], NT)
        sig = jax.nn.sigmoid(pre_g)
        d_gate = (d_act * pre_u * swish_slope(pre_g, sig)).astype(BF)
        d_up = (d_act * pre_g * sig).astype(BF)
        slot = h * 2 + gg
        act_t[slot] = (pre_g * sig * pre_u).T.astype(BF)
        dg_t[slot] = d_gate.T
        du_t[slot] = d_up.T
        return d_gate, d_up

    def back(h, gg, grads, yy):
        span = pl.ds(pl.multiple_of(yy * 512, 512), 512)
        term = mm(grads[0], wg[:, span], NN) + mm(grads[1], wu[:, span], NN)
        part[h, pair(gg), yy] = term.astype(BF).reshape(2, 128, 512)

    order = (y2, yp, ym, y)

    def sib_copy(h, gg, j):
        at = (0 if gg is g else 4) + j
        return remote(
            part.at[h, gg * 2 + oc, order[j]], sib_in.at[h, gg, order[j]],
            sb_send.at[h, at], sb_recv.at[h, at], dev_s,
        )

    def whole(h, gg, *between):
        grads = forward(h, gg)
        for j in range(4):
            back(h, gg, grads, order[j])
            sib_copy(h, gg, j).start()
            if j < len(between):
                between[j]()

    m_g, m_o = g * 2 + c, og * 2 + c

    def pair_sum(h, gg, j):
        sib_copy(h, gg, j).wait_recv()
        at = (h, gg * 2 + c, order[j])
        part[at] = (part[at].astype(F32) + sib_in[h, gg, order[j]].astype(F32)).astype(BF)

    def rs_copy(h, kind):
        src, dst, dev = (
            (part.at[h, m_o, y2, first], in_a.at[h, first], dev_x),
            (part.at[h, m_o, y2, second], in_a.at[h, second], dev_x),
            (part.at[h, m_o, yp], in_b.at[h, 0], dev_p),
            (part.at[h, m_o, ym], in_b.at[h, 1], dev_m),
            (part.at[h, m_g, y2, first], in_c.at[h, 0], dev_p),
            (part.at[h, m_g, y2, second], in_c.at[h, 1], dev_m),
            (part.at[h, m_o, y], in_d.at[h], dev_x),
            (part.at[h, m_g, yp, second], in_e.at[h, 0, second], dev_p),
            (part.at[h, m_g, ym, first], in_e.at[h, 1, first], dev_m),
            (part.at[h, m_g, yp, first], in_e.at[h, 0, first], dev_p),
            (part.at[h, m_g, ym, second], in_e.at[h, 1, second], dev_m),
        )[kind]
        return remote(src, dst, rs_send.at[h, kind], rs_recv.at[h, kind], dev)

    def rs_open(h):
        pair_sum(h, og, 0)
        rs_copy(h, 0).start()
        rs_copy(h, 1).start()
        pair_sum(h, og, 1)
        rs_copy(h, 2).start()
        pair_sum(h, og, 2)
        rs_copy(h, 3).start()

    def rs_own(h):
        for j, kind in ((1, 7), (2, 8), (0, None)):
            pair_sum(h, g, j)
            if kind:
                rs_copy(h, kind).start()
        pair_sum(h, og, 3)
        pair_sum(h, g, 3)

    def add_to(at, *terms):
        value = part[at].astype(F32)
        for term in terms:
            value += term.astype(F32)
        part[at] = value.astype(BF)

    def rs_far(h):
        rs_copy(h, 0).wait_recv()
        add_to((h, m_g, y2, first), in_a[h, first])
        rs_copy(h, 4).start()
        rs_copy(h, 1).wait_recv()
        add_to((h, m_g, y2, second), in_a[h, second])
        rs_copy(h, 5).start()

    def rs_cross(h):
        rs_copy(h, 2).wait_recv()
        rs_copy(h, 3).wait_recv()
        add_to((h, m_o, y), in_b[h, 0], in_b[h, 1])
        rs_copy(h, 6).start()

    def rs_near(h):
        rs_copy(h, 4).wait_recv()
        add_to((h, m_g, yp, first), in_c[h, 0])
        rs_copy(h, 9).start()
        rs_copy(h, 5).wait_recv()
        add_to((h, m_g, ym, second), in_c[h, 1])
        rs_copy(h, 10).start()

    def ret_copy(p):
        zz, hh = from_of(p)
        return remote(
            total.at[p // 8, pl.ds(p % 8 * 16, 16)], ret.at[rows_of(me)],
            ret_send.at[p], ret_recv.at[p], holder(zz, hh),
        )

    own_back = pltpu.make_async_copy(total.at[0, pl.ds(0, 16)], ret.at[rows_of(me)], own_sem.at[0])

    def rs_close(h):
        for kind in range(6, 11):
            rs_copy(h, kind).wait_recv()
        total[h] = (
            part[h, m_g, y].astype(F32) + in_d[h].astype(F32)
            + in_e[h, 0].astype(F32) + in_e[h, 1].astype(F32)
        ).astype(BF)
        for p in range(8 * h, 8 * h + 8):
            if p == 0:
                own_back.start()
            else:
                ret_copy(p).start()

    def weight_grad(out_ref, source, a):
        def tile(q, _):
            acc = jnp.zeros((source.shape[1], 512), F32)
            for h in range(2):
                for gg in range(2):
                    acc += mm(source[h * 2 + gg], rows_at(a, h, gg, q), NN)
            out_ref[:, pl.ds(pl.multiple_of(q * 512, 512), 512)] = acc.astype(BF)
            return 0

        lax.fori_loop(0, 4, tile, 0)

    a2a_wait(0, 0)
    go(0, 0, 0, 1, 2, 8)
    a2a_wait(1, 0)
    go(1, 0, 0, 1, 2, 8)
    relay_y(0, 0)
    relay_y(1, 0)
    relay_x(0, 0)
    relay_x(1, 0)
    a2a_wait(0, 1)
    go(0, 1, 0, 1, 2, 8)
    sum1, sum2 = sums_in(0, stats)
    mean = sum1 / DB
    rstd = lax.rsqrt(sum2 / DB - mean * mean + 1e-05)
    norm_val = (conv_ref[...].astype(F32) - mean) * rstd
    zpre = norm_val * gain_ref[...]
    zsig = jax.nn.sigmoid(zpre)
    normed[...] = norm_val
    mixed[...] = (zpre * zsig).astype(BF)
    slope[...] = swish_slope(zpre, zsig) * gain_ref[...]
    scale[...] = jnp.broadcast_to(rstd, (128, 256))
    relay_far(0, 0)
    relay_far(1, 0)
    a2a_wait(1, 1)
    go(1, 1, 0, 1, 2, 8)
    for copy in loads:
        copy.wait()
    got(0, 0, 8, 9, 10, 11)
    got(1, 0, 8, 9, 10, 11)
    whole(0, g)
    relay_last(0, 0)
    relay_last(1, 0)
    relay_y(0, 1)
    got(0, 0, 12, 13, 14, 15)
    got(1, 0, 12, 13, 14, 15)
    whole(0, og, lambda: relay_y(1, 1), lambda: relay_x(0, 1), lambda: relay_x(1, 1))
    rs_open(0)
    rs_own(0)
    relay_far(0, 1)
    relay_far(1, 1)
    got(0, 1, 8, 9, 10, 11)
    got(1, 1, 8, 9, 10, 11)
    whole(1, g)
    rs_far(0)
    relay_last(0, 1)
    relay_last(1, 1)
    got(0, 1, 12, 13, 14, 15)
    got(1, 1, 12, 13, 14, 15)
    whole(1, og)
    rs_open(1)
    rs_cross(0)
    rs_own(1)
    rs_near(0)
    weight_grad(gg_ref, dg_t, 0)
    weight_grad(gu_ref, du_t, 0)
    rs_far(1)
    rs_cross(1)
    rs_near(1)
    rs_close(0)
    weight_grad(gd_ref, act_t, 1)
    rs_close(1)

    for p in range(1, 16):
        ret_copy(p).wait_recv()
    own_back.wait()
    moe = mm(perm[...], ret[...], TN)
    res_ref[y] = (cq[...].astype(F32) + moe).astype(BF)

    half0, half1 = pl.ds(0, 64), pl.ds(64, 64)

    def res_copy(kind, ref, dev):
        return remote(ref, ref, res_send.at[kind], res_recv.at[kind], dev)

    def res_out(kind):
        ref, dev = (
            (res_ref.at[y, half0], dev_p), (res_ref.at[y, half1], dev_p),
            (res_ref.at[y, half1], dev_m), (res_ref.at[y, half0], dev_m),
            (res_ref.at[ym, half0], dev_p), (res_ref.at[yp, half1], dev_m),
        )[kind]
        return res_copy(kind, ref, dev)

    def res_in(kind):
        ref, dev = (
            (res_ref.at[ym, half0], dev_m), (res_ref.at[ym, half1], dev_m),
            (res_ref.at[yp, half1], dev_p), (res_ref.at[yp, half0], dev_p),
            (res_ref.at[y2, half0], dev_m), (res_ref.at[y2, half1], dev_p),
        )[kind]
        return res_copy(kind, ref, dev)

    for kind in (0, 2, 1, 3):
        res_out(kind).start()
    for copy in late_loads:
        copy.wait()

    def pair_of(q):
        return pl.ds(q * 2, 2)

    def gp_copy(q, j):
        return remote(
            gp.at[oc, :, pair_of(q)], gp_sib.at[:, pair_of(q)], gs_send.at[j], gs_recv.at[j], dev_s
        )

    def proj_terms(q, j):
        feats = res_ref[q]
        term = mm(feats, mixed[...], TN)
        for i in range(8):
            for cc in range(2):
                gp[cc, i % 4, q * 2 + i // 4] = term[i * 64 + cc * 32 : i * 64 + cc * 32 + 32].astype(BF)
        gp_copy(q, j).start()
        return mm(feats, proj[pl.ds(pl.multiple_of(q * 512, 512), 512), :], NN)

    def gx_copy(q, j, i):
        return remote(
            gp.at[c, others_x[i], pair_of(q)], gp_x.at[i, pair_of(q)],
            gx_send.at[j, i], gx_recv.at[j, i], at_x(others_x[i]),
        )

    def over_x(q, j):
        gp_copy(q, j).wait_recv()
        gp[c, :, pair_of(q)] = (
            gp[c, :, pair_of(q)].astype(F32) + gp_sib[:, pair_of(q)].astype(F32)
        ).astype(BF)
        for i in (1, 2, 0):
            gx_copy(q, j, i).start()

    def gz_copy(to, slot):
        return remote(gp_row.at[to], gp_z.at[slot], gz_send.at[to], gz_recv.at[slot], at_z(to))

    def over_z(q, j):
        for i in range(3):
            gx_copy(q, j, i).wait_recv()
        pair = pair_of(q)
        gp_row[pair] = (
            (gp[c, x, pair].astype(F32) + gp_x[0, pair].astype(F32))
            + (gp_x[1, pair].astype(F32) + gp_x[2, pair].astype(F32))
        ).astype(BF)
        for i in range(2):

            @pl.when(q * 2 + i != z)
            def _():
                gz_copy(q * 2 + i, z).start()

    d_mixed = proj_terms(y, 0)
    res_in(0).wait_recv()
    res_out(4).start()
    res_in(2).wait_recv()
    res_out(5).start()
    over_x(y, 0)
    res_in(1).wait_recv()
    d_mixed += proj_terms(ym, 1)
    res_in(3).wait_recv()
    d_mixed += proj_terms(yp, 2)
    over_x(ym, 1)
    over_x(yp, 2)
    res_in(4).wait_recv()
    res_in(5).wait_recv()
    d_mixed += proj_terms(y2, 3)
    d_norm = d_mixed * slope[...]
    norm_val = normed[...]
    stats2 = sums_out(
        1,
        jnp.sum(d_norm, axis=1, keepdims=True),
        jnp.sum(d_norm * norm_val, axis=1, keepdims=True),
    )
    for copy in stats2:
        copy.start()
    over_x(y2, 3)
    over_z(y, 0)
    over_z(ym, 1)
    over_z(yp, 2)

    first_sum, second_sum = sums_in(1, stats2)
    conv_grad = (
        scale[...] * (d_norm - first_sum / DB - norm_val * (second_sum / DB))
    ).astype(BF)
    halo_out[...] = conv_grad[0:32]
    halo = remote(halo_out, halo_in, halo_sem.at[0], halo_sem.at[1], dev_prev)
    halo.start()
    ext[0:128, :] = conv_grad.astype(F32)

    def correlate(start, count):
        acc = jnp.zeros((count, 256), F32)
        for k in range(WIDTH):
            acc += ext[start + k : start + k + count, :] * taps_ref[k : k + 1, :]
        return acc

    def glu_grads(start, count, unit_grad):
        span = slice(start, start + count)
        sig = jax.nn.sigmoid(gate_ref[span, :].astype(F32))
        gv_ref[span, :] = (unit_grad * sig).astype(BF)
        gt_ref[span, :] = (
            unit_grad * value_ref[span, :].astype(F32) * sig * (1.0 - sig)
        ).astype(BF)

    glu_grads(0, 64, correlate(0, 64))
    glu_grads(64, 32, correlate(64, 32))

    over_z(y2, 3)
    halo.wait_recv()
    keep = jnp.where(sp < 63, 1.0, 0.0)
    ext[128:160, :] = halo_in[...].astype(F32) * keep
    glu_grads(96, 32, correlate(96, 32))

    rows_sum = gp_row[z].astype(F32)
    for k in range(1, 8):
        zz = lax.rem(z + k, 8)
        gz_copy(zz, zz).wait_recv()
        rows_sum += gp_z[zz].astype(F32)
    gp_ref[...] = rows_sum

    for a in range(2):
        for p in range(1, 16):
            out_copy(a, p).wait_send()
        for h in range(2):
            for kind in range(16):
                ag_out(a, h, kind).wait_send()
    for h in range(2):
        for gg in (g, og):
            for j in range(4):
                sib_copy(h, gg, j).wait_send()
        for kind in range(11):
            rs_copy(h, kind).wait_send()
    for p in range(1, 16):
        ret_copy(p).wait_send()
    for copy in (*stats, *stats2, halo):
        copy.wait_send()
    for kind in range(6):
        res_out(kind).wait_send()
    for j, q in enumerate((y, ym, yp, y2)):
        gp_copy(q, j).wait_send()
        for i in range(3):
            gx_copy(q, j, i).wait_send()
    for k in range(1, 8):
        gz_copy(lax.rem(z + k, 8), z).wait_send()


def write_kernel(*refs):
    copies = [pltpu.make_async_copy(refs[i], refs[6 + i], refs[12].at[i]) for i in range(6)]
    for copy in copies:
        copy.start()
    for copy in copies:
        copy.wait()


def local(
    moe_input,
    out_cotangent,
    routes,
    route_weight,
    w_gate,
    w_up,
    w_down,
    out_proj,
    conv_out,
    glu_value,
    glu_gate,
    taps,
    norm_gain,
):
    units, width = w_down.shape[1:]
    tokens, channels = conv_out.shape
    vmem = pl.BlockSpec(memory_space=pltpu.VMEM)
    hbm = pl.BlockSpec(memory_space=pl.ANY)
    dma = pltpu.SemaphoreType.DMA
    grad = jax.ShapeDtypeStruct((units, width), BF)
    glu = jax.ShapeDtypeStruct((tokens, channels), BF)
    shapes = (grad, grad, grad, jax.ShapeDtypeStruct((32, channels), F32), glu, glu)
    results = pl.pallas_call(
        backward_kernel,
        out_shape=[pltpu.VMEM(a.shape, a.dtype) for a in shapes],
        in_specs=[vmem] * 3 + [hbm] * 10,
        out_specs=[vmem] * 6,
        scratch_shapes=[
            pltpu.VMEM((128, 512), BF),
            pltpu.VMEM((128, 512), BF),
            pltpu.VMEM((256, 128), BF),
            pltpu.VMEM((2, 256, 512), BF),
            pltpu.VMEM((2, 2, 4, 4, 128, 512), BF),
            pltpu.VMEM((units, width), BF),
            pltpu.VMEM((units, width), BF),
            pltpu.VMEM((units, width), BF),
            pltpu.VMEM((4, units, 256), BF),
            pltpu.VMEM((4, units, 256), BF),
            pltpu.VMEM((4, units, 256), BF),
            pltpu.VMEM((2, 4, 4, 128, 512), BF),
            pltpu.VMEM((2, 2, 4, 128, 512), BF),
            pltpu.VMEM((2, 128, 512), BF),
            pltpu.VMEM((2, 2, 128, 512), BF),
            pltpu.VMEM((2, 2, 64, 512), BF),
            pltpu.VMEM((2, 128, 512), BF),
            pltpu.VMEM((2, 2, 128, 512), BF),
            pltpu.VMEM((2, 128, 512), BF),
            pltpu.VMEM((256, 512), BF),
            pltpu.VMEM((tokens, channels), BF),
            pltpu.VMEM((tokens, channels), BF),
            pltpu.VMEM((tokens, channels), BF),
            pltpu.VMEM((WIDTH, channels), F32),
            pltpu.VMEM((4, 128, 512), BF),
            pltpu.VMEM((width, 256), BF),
            pltpu.VMEM((128, 256), F32),
            pltpu.VMEM((128, 256), F32),
            pltpu.VMEM((128, 256), BF),
            pltpu.VMEM((128, 256), F32),
            pltpu.VMEM((2, 8, 128), F32),
            pltpu.VMEM((2, 3, 8, 128), F32),
            pltpu.VMEM((160, 256), F32),
            pltpu.VMEM((32, 256), BF),
            pltpu.VMEM((32, 256), BF),
            pltpu.VMEM((2, 4, 8, 32, 256), BF),
            pltpu.VMEM((4, 8, 32, 256), BF),
            pltpu.VMEM((3, 8, 32, 256), BF),
            pltpu.VMEM((8, 32, 256), BF),
            pltpu.VMEM((8, 32, 256), BF),
            dma((10,)), dma((2,)),
            dma((2, 16)), dma((2, 16)), dma((4, 16)), dma((4, 16)),
            dma((2, 8)), dma((2, 8)), dma((2, 11)), dma((2, 11)),
            dma((16,)), dma((16,)), dma((6,)), dma((6,)),
            dma((2, 3)), dma((2, 3)), dma((2,)),
            dma((4,)), dma((4,)), dma((4, 3)), dma((4, 3)), dma((8,)), dma((8,)),
        ],
        compiler_params=pltpu.CompilerParams(
            collective_id=0, has_side_effects=True, vmem_limit_bytes=60 * 1024 * 1024
        ),
        name="backward",
    )(
        routes.T, route_weight.T, norm_gain[None, :],
        moe_input, out_cotangent, w_gate[0].T, w_up[0].T, w_down[0], out_proj,
        conv_out, glu_value, glu_gate, taps,
    )
    gg, gu, gd, gp, gv, gt = pl.pallas_call(
        write_kernel,
        out_shape=shapes,
        in_specs=[vmem] * 6,
        out_specs=[hbm] * 6,
        scratch_shapes=[dma((6,))],
        compiler_params=pltpu.CompilerParams(vmem_limit_bytes=1024 * 1024),
        name="write_out",
    )(*(pltpu.with_memory_space_constraint(r, pltpu.VMEM) for r in results))
    return (gg.T[None], gu.T[None], gd[None], gp, gv, gt)


def solution(mesh):
    in_specs = (
        P("sp", None),
        P("sp", None),
        P("sp", None),
        P("sp", None),
        P("sp", None, "tp"),
        P("sp", None, "tp"),
        P("sp", "tp", None),
        P(None, "tp"),
        P("sp", "tp"),
        P("sp", "tp"),
        P("sp", "tp"),
        P(None, "tp"),
        P("tp"),
    )
    out_specs = (
        P("sp", None, "tp"),
        P("sp", None, "tp"),
        P("sp", "tp", None),
        P("sp", "tp"),
        P("sp", "tp"),
        P("sp", "tp"),
    )
    return jax.shard_map(local, mesh=mesh, in_specs=in_specs, out_specs=out_specs, check_vma=False)
```

```python
import jax
import jax.numpy as jnp
from jax import lax
from jax.experimental import pallas as pl
from jax.experimental.pallas import tpu as pltpu
from jax.sharding import PartitionSpec as P

DB = 1024
WIDTH = 31
MESH = pl.DeviceIdType.MESH
BF = jnp.bfloat16
F32 = jnp.float32
NEAR = (0, 1, 7, 2, 6, 3, 5, 4)
NT = (((1,), (1,)), ((), ()))
NN = (((1,), (0,)), ((), ()))
TN = (((0,), (0,)), ((), ()))


def mm(a, b, dims):
    return lax.dot_general(a, b, dims, preferred_element_type=F32)


def swish_slope(pre, sig):
    return sig * (1.0 + pre * (1.0 - sig))


def backward_kernel(
    gain_ref, routes_hbm, weight_hbm,
    x_hbm, cot_hbm, wg_hbm, wu_hbm, wd_hbm, proj_hbm, conv_hbm, value_hbm, gate_hbm, taps_hbm,
    gg_ref, gu_ref, gd_ref, gp_ref, gv_ref, gt_ref,
    xq, cq, xq2, cq2, perm, sendbuf, sendbuf2, xc, wg, wu, wd, act_t, dg_t, du_t,
    part, sib_in, in_a, in_b, in_c, in_d, in_e, total, ret,
    routes_ref, weight_ref, conv_ref, value_ref, gate_ref, taps_ref, res_ref, proj, normed, slope, mixed, scale, st_out, st_in, ext, halo_out, halo_in,
    gp, gp_sib, gp_x, gp_row, gp_z,
    load_sem, own_sem, a2a_send, a2a_recv, far_send, far_recv, ag_send, ag_recv,
    sb_send, sb_recv, rs_send, rs_recv, ret_send, ret_recv, res_send, res_recv,
    st_send, st_recv, halo_sem, gs_send, gs_recv, gx_send, gx_recv, gz_send, gz_recv,
):
    sp = lax.axis_index("sp")
    y = lax.axis_index("tp")
    c = lax.rem(sp, 2)
    x = lax.rem(sp // 2, 4)
    z = sp // 8
    xh = x // 2
    xl = lax.rem(x, 2)
    g = lax.rem(xl + xh, 2)
    og = 1 - g
    oc = 1 - c
    me = sp // 4
    yp, ym, y2 = lax.rem(y + 1, 4), lax.rem(y + 3, 4), lax.rem(y + 2, 4)

    def holder(zz, hh):
        return (zz * 8 + (hh * 2 + lax.rem(g + hh, 2)) * 2 + c, y)

    def to_of(p):
        return lax.rem(z + 8 - NEAR[p // 2], 8), (xh if p % 2 == 0 else 1 - xh)

    def from_of(p):
        return lax.rem(z + NEAR[p // 2], 8), (xh if p % 2 == 0 else 1 - xh)

    dev_x = (z * 8 + (xh * 2 + 1 - xl) * 2 + c, y)
    dev_s = (z * 8 + x * 2 + oc, y)
    dev_p = (sp, yp)
    dev_m = (sp, ym)
    dev_2 = (sp, y2)
    dev_prev = (lax.rem(sp + 63, 64), y)
    dev_next = (lax.rem(sp + 1, 64), y)
    others_x = (xh * 2 + 1 - xl, (1 - xh) * 2 + xl, (1 - xh) * 2 + 1 - xl)

    def at_x(xx):
        return (z * 8 + xx * 2 + c, y)

    def at_z(zz):
        return (zz * 8 + x * 2 + c, y)

    def remote(src, dst, ss, rs, dev):
        return pltpu.make_async_remote_copy(
            src_ref=src, dst_ref=dst, send_sem=ss, recv_sem=rs, device_id=dev,
            device_id_type=MESH,
        )

    def all_sent(ref, sem):
        remote(ref, ref, sem, sem, dev_s).wait_send()

    def all_in(ref, sem):
        remote(ref, ref, sem, sem, dev_s).wait_recv()

    load_r = pltpu.make_async_copy(routes_hbm, routes_ref, load_sem.at[12])
    load_w = pltpu.make_async_copy(weight_hbm, weight_ref, load_sem.at[13])
    load_r.start()
    load_w.start()
    cols = pl.ds(pl.multiple_of(y * 512, 512), 512)
    load_x = pltpu.make_async_copy(x_hbm.at[:, cols], xq, load_sem.at[0])
    load_c = pltpu.make_async_copy(cot_hbm.at[:, cols], cq, load_sem.at[1])
    load_x.start()
    load_c.start()
    cols2 = pl.ds(pl.multiple_of(y2 * 512, 512), 512)
    load_far = [
        pltpu.make_async_copy(x_hbm.at[:, cols2], xq2, load_sem.at[10]),
        pltpu.make_async_copy(cot_hbm.at[:, cols2], cq2, load_sem.at[11]),
    ]
    for copy in load_far:
        copy.start()
    loads = [
        pltpu.make_async_copy(wg_hbm, wg, load_sem.at[2]),
        pltpu.make_async_copy(wu_hbm, wu, load_sem.at[3]),
        pltpu.make_async_copy(wd_hbm, wd, load_sem.at[4]),
    ]
    for copy in loads:
        copy.start()
    load_conv = pltpu.make_async_copy(conv_hbm, conv_ref, load_sem.at[5])
    load_conv.start()
    late_loads = [
        pltpu.make_async_copy(src, dst, load_sem.at[6 + i])
        for i, (src, dst) in enumerate((
            (proj_hbm, proj), (value_hbm, value_ref), (gate_hbm, gate_ref), (taps_hbm, taps_ref)
        ))
    ]
    for copy in late_loads:
        copy.start()

    barrier = pltpu.get_barrier_semaphore()

    for p in range(1, 16):
        pl.semaphore_signal(barrier, inc=1, device_id=holder(*to_of(p)), device_id_type=MESH)
    greeted = (
        dev_x, dev_s, dev_p, dev_m, dev_2, at_x(others_x[1]), at_x(others_x[2]), dev_prev, dev_next
    )
    for dev in greeted:
        pl.semaphore_signal(barrier, inc=1, device_id=dev, device_id_type=MESH)

    load_r.wait()
    load_w.wait()

    r0 = routes_ref[0:1, :]
    r1 = routes_ref[1:2, :]
    ids = lax.broadcasted_iota(jnp.int32, (16, 128), 0)
    e0 = ids == r0
    e1 = ids == r1
    named = jnp.where(e0, 1.0, 0.0) + jnp.where(e1, 1.0, 0.0)
    before = jnp.where(
        lax.broadcasted_iota(jnp.int32, (128, 128), 0)
        < lax.broadcasted_iota(jnp.int32, (128, 128), 1),
        1.0, 0.0,
    ).astype(BF)
    earlier = mm(named.astype(BF), before, NN)
    t0 = r0.astype(F32) * 16.0 + jnp.sum(jnp.where(e0, earlier, 0.0), axis=0, keepdims=True)
    t1 = r1.astype(F32) * 16.0 + jnp.sum(jnp.where(e1, earlier, 0.0), axis=0, keepdims=True)
    place = lax.broadcasted_iota(jnp.int32, (256, 128), 0).astype(F32)
    p0 = place == t0
    p1 = place == t1
    perm_val = (jnp.where(p0, 1.0, 0.0) + jnp.where(p1, 1.0, 0.0)).astype(BF)
    perm[...] = perm_val
    w0 = weight_ref[0:1, :]
    w1 = weight_ref[1:2, :]
    w_slot = jnp.sum(jnp.where(p0, w0, 0.0) + jnp.where(p1, w1, 0.0), axis=1, keepdims=True)
    load_x.wait()
    sendbuf[0] = mm(perm_val, xq[...], NN).astype(BF)
    load_c.wait()
    sendbuf[1] = (w_slot * mm(perm_val, cq[...], NN)).astype(BF)

    pl.semaphore_wait(barrier, 24)

    m_own = g * 2 + c

    def rows_of(q):
        return pl.ds(pl.multiple_of(q * 16, 16), 16)

    def place_of(a, p):
        return xc.at[a, p // 8, m_own, y, pl.ds(p % 8 * 16, 16)]

    def out_copy(a, p):
        zz, hh = to_of(p)
        return remote(
            sendbuf.at[a, rows_of(zz * 2 + hh)], place_of(a, p),
            a2a_send.at[a], a2a_recv.at[a, p // 8], holder(zz, hh),
        )

    def a2a_wait(a, h):
        if h == 0:
            own[a].wait()
        all_in(xc.at[a, h, m_own, y, pl.ds(0, 112 + 16 * h)], a2a_recv.at[a, h])

    def far_copy(a, p):
        zz, hh = to_of(p)
        return remote(
            sendbuf2.at[a, rows_of(zz * 2 + hh)], xc.at[a, 0, m_own, y2, pl.ds(p * 16, 16)],
            far_send.at[a], far_recv.at[a], holder(zz, hh),
        )

    own = [
        pltpu.make_async_copy(sendbuf.at[a, rows_of(me)], place_of(a, 0), own_sem.at[a])
        for a in range(2)
    ]
    own2 = [
        pltpu.make_async_copy(
            sendbuf2.at[a, rows_of(me)], xc.at[a, 0, m_own, y2, pl.ds(0, 16)], own_sem.at[2 + a]
        )
        for a in range(2)
    ]

    def push(h):
        for a in range(2):
            for p in reversed(range(8 * h, 8 * h + 8)):
                if p == 0:
                    own[a].start()
                else:
                    out_copy(a, p).start()

    def push_far(a):
        for p in reversed(range(1, 8)):
            far_copy(a, p).start()
        own2[a].start()

    def far_wait(a):
        own2[a].wait()
        all_in(xc.at[a, 0, m_own, y2, pl.ds(0, 112)], far_recv.at[a])

    push(0)
    load_far[0].wait()
    sendbuf2[0] = mm(perm_val, xq2[...], NN).astype(BF)
    load_far[1].wait()
    sendbuf2[1] = (w_slot * mm(perm_val, cq2[...], NN)).astype(BF)

    lane = lax.broadcasted_iota(jnp.int32, (128, 128), 1)

    def sums_out(phase, one, two):
        cols2 = jnp.where(lane == 0, one, 0.0) + jnp.where(lane == 1, two, 0.0)
        st_out[phase] = cols2.T[0:8, :]
        return [
            remote(
                st_out.at[phase], st_in.at[phase, j], st_send.at[phase], st_recv.at[phase], dev
            )
            for j, dev in enumerate((dev_p, dev_m, dev_2))
        ]

    def sums_in(phase):
        all_in(st_in.at[phase], st_recv.at[phase])
        tot = (st_out[phase] + st_in[phase, 2]) + (st_in[phase, 0] + st_in[phase, 1])
        tall = jnp.concatenate([tot, jnp.zeros((120, 128), F32)], axis=0).T
        return tall[:, 0:1], tall[:, 1:2]

    load_conv.wait()
    conv_vals = conv_ref[...].astype(F32)
    stats = sums_out(
        0,
        jnp.sum(conv_vals, axis=1, keepdims=True),
        jnp.sum(conv_vals * conv_vals, axis=1, keepdims=True),
    )
    for copy in stats:
        copy.start()

    first, second = pl.ds(0, 64), pl.ds(64, 64)
    listed = [(g, y), (g, ym), (g, yp), (g, y2), (og, y), (og, ym), (og, yp), (og, y2)]

    def block(a, h, gg, cc, yy):
        return xc.at[a, h, gg * 2 + cc, yy]

    def ag_copy(a, h, kind, ref, dev):
        lot = 4 if kind in (3, 4) else 8 if kind >= 8 else 0
        slot = kind if kind < 8 else 5 + kind // 4
        slot = slot + 1 if kind >= 8 else slot
        return remote(
            ref, ref, ag_send.at[a * 2 + h + lot], ag_recv.at[a * 2 + h, slot], dev
        )

    def ag_out(a, h, kind):
        if kind >= 8:
            gg, yy = listed[kind - 8]
            return ag_copy(a, h, kind, block(a, h, gg, c, yy), dev_s)
        ref, dev = (
            (block(a, h, g, c, y), dev_x),
            (block(a, h, g, c, y), dev_p),
            (block(a, h, g, c, y), dev_m),
            (block(a, h, g, c, ym).at[first], dev_p),
            (block(a, h, g, c, yp).at[second], dev_m),
            (block(a, h, og, c, y), dev_p),
            (block(a, h, og, c, y), dev_m),
            (block(a, h, g, c, y2), dev_x),
        )[kind]
        return ag_copy(a, h, kind, ref, dev)

    def ag_in(a, h, kind):
        if kind >= 8:
            gg, yy = listed[kind - 8]
            return ag_copy(a, h, kind, block(a, h, gg, oc, yy), dev_s)
        ref, dev = (
            (block(a, h, og, c, y), dev_x),
            (block(a, h, g, c, ym), dev_m),
            (block(a, h, g, c, yp), dev_p),
            (block(a, h, g, c, y2).at[first], dev_m),
            (block(a, h, g, c, y2).at[second], dev_p),
            (block(a, h, og, c, ym), dev_m),
            (block(a, h, og, c, yp), dev_p),
            (block(a, h, og, c, y2), dev_x),
        )[kind]
        return ag_copy(a, h, kind, ref, dev)

    def go(a, h, *kinds):
        for kind in kinds:
            ag_out(a, h, kind).start()

    def got(a, h, *kinds):
        for kind in kinds:
            ag_in(a, h, kind).wait_recv()

    def sib_got(a, h, gg):
        all_in(xc.at[a, h, gg * 2 + oc], ag_recv.at[a * 2 + h, 8 if gg is g else 9])

    def relay_y(a, h):
        got(a, h, 1)
        go(a, h, *((3, 9) if h else (9,)))
        got(a, h, 2)
        go(a, h, *((4, 10) if h else (10,)))

    def relay_x(a, h):
        got(a, h, 0)
        go(a, h, 5, 6, 12)

    def relay_far(a, h):
        if h:
            got(a, h, 3, 4)
        else:
            far_wait(a)
        go(a, h, 7, 11)

    def relay_last(a, h):
        got(a, h, 5)
        go(a, h, 13)
        got(a, h, 6)
        go(a, h, 14)
        got(a, h, 7)
        go(a, h, 15)

    def pair(gg):
        return pl.ds(gg * 2, 2)

    def rows_at(a, h, gg, q):
        return xc[a, h, pair(gg), q].reshape(256, 512)

    def pre_acts(h, gg):
        pre_g = jnp.zeros((256, 224), F32)
        pre_u = jnp.zeros((256, 224), F32)
        for q in range(4):
            span = slice(q * 512, q * 512 + 512)
            rows = rows_at(0, h, gg, q)
            pre_g += mm(rows, wg[:, span], NT)
            pre_u += mm(rows, wu[:, span], NT)
        return pre_g, pre_u

    def forward(h, gg, pres):
        pre_g, pre_u = pres
        d_act = jnp.zeros((256, 224), F32)
        for q in range(4):
            span = slice(q * 512, q * 512 + 512)
            d_act += mm(rows_at(1, h, gg, q), wd[:, span], NT)
        sig = jax.nn.sigmoid(pre_g)
        d_gate = (d_act * pre_u * swish_slope(pre_g, sig)).astype(BF)
        d_up = (d_act * pre_g * sig).astype(BF)
        return d_gate, d_up, pre_g * sig * pre_u

    def back(h, gg, grads, yy):
        span = pl.ds(pl.multiple_of(yy * 512, 512), 512)
        term = mm(grads[0], wg[:, span], NN) + mm(grads[1], wu[:, span], NN)
        part[h, pair(gg), yy] = term.astype(BF).reshape(2, 128, 512)

    order = (y2, yp, ym, y)

    def sib_copy(h, gg, j):
        at = (0 if gg is g else 4) + j
        return remote(
            part.at[h, gg * 2 + oc, order[j]], sib_in.at[h, gg, order[j]],
            sb_send.at[h], sb_recv.at[h, at], dev_s,
        )

    def whole(h, gg, pres, *between):
        grads = forward(h, gg, pres)
        for j in range(4):
            back(h, gg, grads, order[j])
            sib_copy(h, gg, j).start()
            if j < len(between):
                between[j]()
        slot = h * 2 + gg
        act_t[slot] = grads[2].T.astype(BF)
        dg_t[slot] = grads[0].T
        du_t[slot] = grads[1].T

    m_g, m_o = g * 2 + c, og * 2 + c

    def pair_sum(h, gg, j):
        sib_copy(h, gg, j).wait_recv()
        at = (h, gg * 2 + c, order[j])
        part[at] = (part[at].astype(F32) + sib_in[h, gg, order[j]].astype(F32)).astype(BF)

    def pieces(h):
        n = 1 + h
        return n, [i for k in range(n) for i in (k, n + k)]

    def piece(h, i):
        rows = 64 // (1 + h)
        return pl.ds(i * rows, rows)

    def rs_copy(h, kind):
        n = 1 + h
        if kind < 4:
            at = piece(h, kind)
            src, dst, dev = part.at[h, m_o, y2, at], in_a.at[h, at], dev_x
        elif kind < 8:
            at = piece(h, kind - 4)
            src, dst = part.at[h, m_g, y2, at], in_c.at[h, at]
            dev = dev_p if kind - 4 < n else dev_m
        elif kind < 12:
            at = piece(h, kind - 8)
            yy, i, dev = (yp, 0, dev_p) if kind - 8 < n else (ym, 1, dev_m)
            src, dst = part.at[h, m_g, yy, at], in_e.at[h, i, at]
        else:
            src, dst, dev = (
                (part.at[h, m_o, yp], in_b.at[h, 0], dev_p),
                (part.at[h, m_o, ym], in_b.at[h, 1], dev_m),
                (part.at[h, m_o, y], in_d.at[h], dev_x),
                (part.at[h, m_g, yp, second], in_e.at[h, 0, second], dev_p),
                (part.at[h, m_g, ym, first], in_e.at[h, 1, first], dev_m),
            )[kind - 12]
        slot = kind if kind < 8 else 8 if kind in (12, 13) else 9
        lot = 0 if 4 <= kind < 8 or 12 <= kind < 15 else 1
        return remote(src, dst, rs_send.at[h, lot], rs_recv.at[h, slot], dev)

    def rs_open(h):
        pair_sum(h, og, 0)
        for i in pieces(h)[1]:
            rs_copy(h, i).start()
        pair_sum(h, og, 1)
        rs_copy(h, 12).start()
        pair_sum(h, og, 2)
        rs_copy(h, 13).start()

    def rs_own(h):
        pair_sum(h, g, 1)
        rs_copy(h, 15).start()
        pair_sum(h, g, 2)
        rs_copy(h, 16).start()
        pair_sum(h, g, 0)
        pair_sum(h, og, 3)
        pair_sum(h, g, 3)

    def add_to(at, *terms):
        value = part[at].astype(F32)
        for term in terms:
            value += term.astype(F32)
        part[at] = value.astype(BF)

    def rs_far(h):
        for i in pieces(h)[1]:
            rs_copy(h, i).wait_recv()
            add_to((h, m_g, y2, piece(h, i)), in_a[h, piece(h, i)])
            rs_copy(h, 4 + i).start()

    def rs_cross(h):
        all_in(in_b.at[h], rs_recv.at[h, 8])
        add_to((h, m_o, y), in_b[h, 0], in_b[h, 1])
        rs_copy(h, 14).start()

    def rs_near(h):
        n, turns = pieces(h)
        for i in turns:
            rs_copy(h, 4 + i).wait_recv()
            add_to((h, m_g, yp if i < n else ym, piece(h, i)), in_c[h, piece(h, i)])
            rs_copy(h, 8 + i).start()

    def ret_copy(p):
        zz, hh = from_of(p)
        return remote(
            total.at[p // 8, pl.ds(p % 8 * 16, 16)], ret.at[rows_of(me)],
            ret_send.at[0], ret_recv.at[0], holder(zz, hh),
        )

    own_back = pltpu.make_async_copy(total.at[0, pl.ds(0, 16)], ret.at[rows_of(me)], own_sem.at[0])

    def rs_close(h):
        all_in(part.at[h, 0, pl.ds(0, 3)], rs_recv.at[h, 9])
        total[h] = (
            part[h, m_g, y].astype(F32) + in_d[h].astype(F32)
            + in_e[h, 0].astype(F32) + in_e[h, 1].astype(F32)
        ).astype(BF)
        for p in reversed(range(8 * h, 8 * h + 8)):
            if p == 0:
                own_back.start()
            else:
                ret_copy(p).start()

    def weight_grad(out_ref, source, a, half):
        def tile(q, _):
            acc = jnp.zeros((source.shape[1], 512), F32)
            for h in range(2):
                for gg in range(2):
                    acc += mm(source[h * 2 + gg], rows_at(a, h, gg, q), NN)
            out_ref[:, pl.ds(pl.multiple_of(q * 512, 512), 512)] = acc.astype(BF)
            return 0

        lax.fori_loop(2 * half, 2 * half + 2, tile, 0)

    def drain_rows(a):
        all_sent(sendbuf.at[a, pl.ds(0, 240)], a2a_send.at[a])
        all_sent(sendbuf2.at[a, pl.ds(0, 112)], far_send.at[a])
        for h in range(2):
            all_sent(xc.at[a, h, pl.ds(0, 2), pl.ds(0, 3)], ag_send.at[a * 2 + h])
            all_sent(xc.at[a, h, pl.ds(0, 2)], ag_send.at[a * 2 + h + 8])
        all_sent(xc.at[a, 1, 0, 0], ag_send.at[a * 2 + 5])

    def drain_sums():
        for h in range(2):
            all_sent(part.at[h, pl.ds(0, 2)], sb_send.at[h])
            all_sent(part.at[h, 0], rs_send.at[h, 0])
            all_sent(part.at[h, 0, pl.ds(0, 3)], rs_send.at[h, 1])

    a2a_wait(0, 0)
    go(0, 0, 0, 1, 2, 8)
    push_far(0)
    push_far(1)
    push(1)
    a2a_wait(1, 0)
    go(1, 0, 0, 1, 2, 8)
    relay_x(0, 0)
    relay_x(1, 0)
    relay_y(0, 0)
    relay_y(1, 0)
    relay_far(0, 0)
    relay_far(1, 0)
    a2a_wait(0, 1)
    go(0, 1, 0, 1, 2, 8)
    sum1, sum2 = sums_in(0)
    mean = sum1 / DB
    rstd = lax.rsqrt(sum2 / DB - mean * mean + 1e-05)
    norm_val = (conv_ref[...].astype(F32) - mean) * rstd
    zpre = norm_val * gain_ref[...]
    zsig = jax.nn.sigmoid(zpre)
    normed[...] = norm_val
    mixed[...] = (zpre * zsig).astype(BF)
    slope[...] = swish_slope(zpre, zsig) * gain_ref[...]
    scale[...] = jnp.broadcast_to(rstd, (128, 256))
    for copy in loads:
        copy.wait()
    sib_got(0, 0, g)
    pres = pre_acts(0, g)
    a2a_wait(1, 1)
    go(1, 1, 0, 1, 2, 8)
    sib_got(1, 0, g)
    whole(0, g, pres)
    relay_last(0, 0)
    relay_last(1, 0)
    relay_y(0, 1)
    sib_got(0, 0, og)
    pres = pre_acts(0, og)
    sib_got(1, 0, og)
    relay_x(0, 1)
    relay_y(1, 1)
    whole(0, og, pres, lambda: relay_x(1, 1), lambda: relay_far(0, 1))
    sib_got(0, 1, g)
    pres = pre_acts(1, g)
    relay_far(1, 1)
    sib_got(1, 1, g)
    whole(1, g, pres)
    rs_open(0)
    relay_last(0, 1)
    rs_own(0)
    sib_got(0, 1, og)
    pres = pre_acts(1, og)
    relay_last(1, 1)
    sib_got(1, 1, og)
    whole(1, og, pres, lambda: rs_far(0))
    rs_open(1)
    rs_cross(0)
    rs_own(1)
    drain_rows(0)
    rs_near(0)
    weight_grad(gg_ref, dg_t, 0, 0)
    weight_grad(gg_ref, dg_t, 0, 1)
    rs_far(1)
    weight_grad(gu_ref, du_t, 0, 0)
    rs_cross(1)
    weight_grad(gu_ref, du_t, 0, 1)
    drain_rows(1)
    rs_near(1)
    rs_close(0)
    weight_grad(gd_ref, act_t, 1, 0)
    weight_grad(gd_ref, act_t, 1, 1)
    rs_close(1)
    drain_sums()

    all_in(ret.at[pl.ds(0, 240)], ret_recv.at[0])
    own_back.wait()
    moe = mm(perm[...], ret[...], TN)
    res_ref[y] = (cq[...].astype(F32) + moe).astype(BF)

    half0, half1 = pl.ds(0, 64), pl.ds(64, 64)

    def res_copy(kind, ref, dev):
        return remote(ref, ref, res_send.at[0], res_recv.at[kind], dev)

    def res_out(kind):
        ref, dev = (
            (res_ref.at[y, half0], dev_p), (res_ref.at[y, half1], dev_p),
            (res_ref.at[y, half1], dev_m), (res_ref.at[y, half0], dev_m),
            (res_ref.at[ym, half0], dev_p), (res_ref.at[yp, half1], dev_m),
        )[kind]
        return res_copy(kind, ref, dev)

    def res_in(kind):
        ref, dev = (
            (res_ref.at[ym, half0], dev_m), (res_ref.at[ym, half1], dev_m),
            (res_ref.at[yp, half1], dev_p), (res_ref.at[yp, half0], dev_p),
            (res_ref.at[y2, half0], dev_m), (res_ref.at[y2, half1], dev_p),
        )[kind]
        return res_copy(kind, ref, dev)

    for kind in (0, 2, 1, 3):
        res_out(kind).start()
    for copy in late_loads:
        copy.wait()

    def pair_of(q):
        return pl.ds(q * 2, 2)

    def gp_copy(q, j):
        return remote(
            gp.at[oc, :, pair_of(q)], gp_sib.at[:, pair_of(q)], gs_send.at[0], gs_recv.at[j], dev_s
        )

    def proj_terms(q, j):
        feats = res_ref[q]
        term = mm(feats, mixed[...], TN)
        for i in range(8):
            for cc in range(2):
                gp[cc, i % 4, q * 2 + i // 4] = term[i * 64 + cc * 32 : i * 64 + cc * 32 + 32].astype(BF)
        gp_copy(q, j).start()
        return mm(feats, proj[pl.ds(pl.multiple_of(q * 512, 512), 512), :], NN)

    def gx_copy(q, j, i):
        return remote(
            gp.at[c, others_x[i], pair_of(q)], gp_x.at[i, pair_of(q)],
            gx_send.at[0], gx_recv.at[j], at_x(others_x[i]),
        )

    def over_x(q, j):
        gp_copy(q, j).wait_recv()
        gp[c, :, pair_of(q)] = (
            gp[c, :, pair_of(q)].astype(F32) + gp_sib[:, pair_of(q)].astype(F32)
        ).astype(BF)
        for i in (1, 2, 0):
            gx_copy(q, j, i).start()

    def gz_copy(to, slot):
        return remote(gp_row.at[to], gp_z.at[slot], gz_send.at[0], gz_recv.at[0], at_z(to))

    def over_z(q, j):
        pair = pair_of(q)
        all_in(gp_x.at[:, pair], gx_recv.at[j])
        gp_row[pair] = (
            (gp[c, x, pair].astype(F32) + gp_x[0, pair].astype(F32))
            + (gp_x[1, pair].astype(F32) + gp_x[2, pair].astype(F32))
        ).astype(BF)
        for i in range(2):

            @pl.when(q * 2 + i != z)
            def _():
                gz_copy(q * 2 + i, z).start()

    d_mixed = proj_terms(y, 0)
    res_in(0).wait_recv()
    res_out(4).start()
    res_in(2).wait_recv()
    res_out(5).start()
    over_x(y, 0)
    res_in(1).wait_recv()
    d_mixed += proj_terms(ym, 1)
    res_in(3).wait_recv()
    d_mixed += proj_terms(yp, 2)
    over_x(ym, 1)
    over_x(yp, 2)
    res_in(4).wait_recv()
    res_in(5).wait_recv()
    d_mixed += proj_terms(y2, 3)
    d_norm = d_mixed * slope[...]
    norm_val = normed[...]
    stats2 = sums_out(
        1,
        jnp.sum(d_norm, axis=1, keepdims=True),
        jnp.sum(d_norm * norm_val, axis=1, keepdims=True),
    )
    for copy in stats2:
        copy.start()
    over_x(y2, 3)
    over_z(y, 0)

    first_sum, second_sum = sums_in(1)
    conv_grad = (
        scale[...] * (d_norm - first_sum / DB - norm_val * (second_sum / DB))
    ).astype(BF)
    halo_out[...] = conv_grad[0:32]
    halo = remote(halo_out, halo_in, halo_sem.at[0], halo_sem.at[1], dev_prev)
    halo.start()
    ext[0:128, :] = conv_grad.astype(F32)
    over_z(ym, 1)
    over_z(yp, 2)

    def correlate(start, count):
        acc = jnp.zeros((count, 256), F32)
        for k in range(WIDTH):
            acc += ext[start + k : start + k + count, :] * taps_ref[k : k + 1, :]
        return acc

    def glu_grads(start, count, unit_grad):
        span = slice(start, start + count)
        sig = jax.nn.sigmoid(gate_ref[span, :].astype(F32))
        gv_ref[span, :] = (unit_grad * sig).astype(BF)
        gt_ref[span, :] = (
            unit_grad * value_ref[span, :].astype(F32) * sig * (1.0 - sig)
        ).astype(BF)

    glu_grads(0, 64, correlate(0, 64))
    glu_grads(64, 32, correlate(64, 32))

    over_z(y2, 3)
    halo.wait_recv()
    keep = jnp.where(sp < 63, 1.0, 0.0)
    ext[128:160, :] = halo_in[...].astype(F32) * keep
    glu_grads(96, 32, correlate(96, 32))

    all_in(gp_z.at[pl.ds(0, 7)], gz_recv.at[0])
    rows_sum = gp_row[z].astype(F32)
    for k in range(1, 8):
        zz = lax.rem(z + k, 8)
        rows_sum += gp_z[zz].astype(F32)
    gp_ref[...] = rows_sum

    all_sent(ret.at[pl.ds(0, 240)], ret_send.at[0])
    for phase in range(2):
        all_sent(st_in.at[phase], st_send.at[phase])
    halo.wait_send()
    all_sent(res_ref.at[pl.ds(0, 3)], res_send.at[0])
    all_sent(gp.at[oc], gs_send.at[0])
    all_sent(gp_x, gx_send.at[0])
    all_sent(gp_z.at[pl.ds(0, 7)], gz_send.at[0])


def write_kernel(*refs):
    copies = [pltpu.make_async_copy(refs[i], refs[6 + i], refs[12].at[i]) for i in range(6)]
    for copy in copies:
        copy.start()
    for copy in copies:
        copy.wait()


def local(
    moe_input,
    out_cotangent,
    routes,
    route_weight,
    w_gate,
    w_up,
    w_down,
    out_proj,
    conv_out,
    glu_value,
    glu_gate,
    taps,
    norm_gain,
):
    units, width = w_down.shape[1:]
    tokens, channels = conv_out.shape
    vmem = pl.BlockSpec(memory_space=pltpu.VMEM)
    hbm = pl.BlockSpec(memory_space=pl.ANY)
    dma = pltpu.SemaphoreType.DMA
    grad = jax.ShapeDtypeStruct((units, width), BF)
    glu = jax.ShapeDtypeStruct((tokens, channels), BF)
    shapes = (grad, grad, grad, jax.ShapeDtypeStruct((32, channels), F32), glu, glu)
    results = pl.pallas_call(
        backward_kernel,
        out_shape=[pltpu.VMEM(a.shape, a.dtype) for a in shapes],
        in_specs=[vmem] + [hbm] * 12,
        out_specs=[vmem] * 6,
        scratch_shapes=[
            pltpu.VMEM((128, 512), BF),
            pltpu.VMEM((128, 512), BF),
            pltpu.VMEM((128, 512), BF),
            pltpu.VMEM((128, 512), BF),
            pltpu.VMEM((256, 128), BF),
            pltpu.VMEM((2, 256, 512), BF),
            pltpu.VMEM((2, 256, 512), BF),
            pltpu.VMEM((2, 2, 4, 4, 128, 512), BF),
            pltpu.VMEM((units, width), BF),
            pltpu.VMEM((units, width), BF),
            pltpu.VMEM((units, width), BF),
            pltpu.VMEM((4, units, 256), BF),
            pltpu.VMEM((4, units, 256), BF),
            pltpu.VMEM((4, units, 256), BF),
            pltpu.VMEM((2, 4, 4, 128, 512), BF),
            pltpu.VMEM((2, 2, 4, 128, 512), BF),
            pltpu.VMEM((2, 128, 512), BF),
            pltpu.VMEM((2, 2, 128, 512), BF),
            pltpu.VMEM((2, 128, 512), BF),
            pltpu.VMEM((2, 128, 512), BF),
            pltpu.VMEM((2, 2, 128, 512), BF),
            pltpu.VMEM((2, 128, 512), BF),
            pltpu.VMEM((256, 512), BF),
            pltpu.VMEM((2, tokens), jnp.int32),
            pltpu.VMEM((2, tokens), F32),
            pltpu.VMEM((tokens, channels), BF),
            pltpu.VMEM((tokens, channels), BF),
            pltpu.VMEM((tokens, channels), BF),
            pltpu.VMEM((WIDTH, channels), F32),
            pltpu.VMEM((4, 128, 512), BF),
            pltpu.VMEM((width, 256), BF),
            pltpu.VMEM((128, 256), F32),
            pltpu.VMEM((128, 256), F32),
            pltpu.VMEM((128, 256), BF),
            pltpu.VMEM((128, 256), F32),
            pltpu.VMEM((2, 8, 128), F32),
            pltpu.VMEM((2, 3, 8, 128), F32),
            pltpu.VMEM((160, 256), F32),
            pltpu.VMEM((32, 256), BF),
            pltpu.VMEM((32, 256), BF),
            pltpu.VMEM((2, 4, 8, 32, 256), BF),
            pltpu.VMEM((4, 8, 32, 256), BF),
            pltpu.VMEM((3, 8, 32, 256), BF),
            pltpu.VMEM((8, 32, 256), BF),
            pltpu.VMEM((8, 32, 256), BF),
            dma((14,)), dma((4,)),
            dma((2,)), dma((2, 2)), dma((2,)), dma((2,)), dma((12,)), dma((4, 10)),
            dma((2,)), dma((2, 8)), dma((2, 2)), dma((2, 10)),
            dma((1,)), dma((1,)), dma((1,)), dma((6,)),
            dma((2,)), dma((2,)), dma((2,)),
            dma((1,)), dma((4,)), dma((1,)), dma((4,)), dma((1,)), dma((1,)),
        ],
        compiler_params=pltpu.CompilerParams(
            collective_id=0, has_side_effects=True, vmem_limit_bytes=60 * 1024 * 1024
        ),
        name="backward",
    )(
        norm_gain[None, :], routes.T, route_weight.T,
        moe_input, out_cotangent, w_gate[0].T, w_up[0].T, w_down[0], out_proj,
        conv_out, glu_value, glu_gate, taps,
    )
    gg, gu, gd, gp, gv, gt = pl.pallas_call(
        write_kernel,
        out_shape=shapes,
        in_specs=[vmem] * 6,
        out_specs=[hbm] * 6,
        scratch_shapes=[dma((6,))],
        compiler_params=pltpu.CompilerParams(vmem_limit_bytes=1024 * 1024),
        name="write_out",
    )(*(pltpu.with_memory_space_constraint(r, pltpu.VMEM) for r in results))
    return (gg.T[None], gu.T[None], gd[None], gp, gv, gt)


def solution(mesh):
    in_specs = (
        P("sp", None),
        P("sp", None),
        P("sp", None),
        P("sp", None),
        P("sp", None, "tp"),
        P("sp", None, "tp"),
        P("sp", "tp", None),
        P(None, "tp"),
        P("sp", "tp"),
        P("sp", "tp"),
        P("sp", "tp"),
        P(None, "tp"),
        P("tp"),
    )
    out_specs = (
        P("sp", None, "tp"),
        P("sp", None, "tp"),
        P("sp", "tp", None),
        P("sp", "tp"),
        P("sp", "tp"),
        P("sp", "tp"),
    )
    return jax.shard_map(local, mesh=mesh, in_specs=in_specs, out_specs=out_specs, check_vma=False)
```

```python
import jax
import jax.numpy as jnp
from jax import lax
from jax.experimental import pallas as pl
from jax.experimental.pallas import tpu as pltpu
from jax.sharding import PartitionSpec as P

DB = 1024
WIDTH = 31
MESH = pl.DeviceIdType.MESH
BF = jnp.bfloat16
F32 = jnp.float32
NEAR = (0, 1, 7, 2, 6, 3, 5, 4)
NT = (((1,), (1,)), ((), ()))
NN = (((1,), (0,)), ((), ()))
TN = (((0,), (0,)), ((), ()))


def mm(a, b, dims):
    return lax.dot_general(a, b, dims, preferred_element_type=F32)


def swish_slope(pre, sig):
    return sig * (1.0 + pre * (1.0 - sig))


def backward_kernel(
    gain_ref, routes_hbm, weight_hbm,
    x_hbm, cot_hbm, wg_hbm, wu_hbm, wd_hbm, proj_hbm, conv_hbm, value_hbm, gate_hbm, taps_hbm,
    gg_ref, gu_ref, gd_ref, gp_ref, gv_ref, gt_ref,
    xq, cq, xq2, cq2, perm, sendbuf, sendbuf2, xc, wg, wu, wd, act_t, dg_t, du_t,
    part, sib_in, in_a, in_b, in_c, in_d, in_e, total, ret,
    routes_ref, weight_ref, conv_ref, value_ref, gate_ref, taps_ref, res_ref, proj, normed, slope, mixed, scale, st_out, st_in, ext, halo_out, halo_in,
    gp, gp_sib, gp_x, gp_row, gp_z,
    load_sem, own_sem, a2a_send, a2a_recv, far_send, far_recv, ag_send, ag_recv,
    sb_send, sb_recv, rs_send, rs_recv, ret_send, ret_recv, res_send, res_recv,
    st_send, st_recv, halo_sem, gs_send, gs_recv, gx_send, gx_recv, gz_send, gz_recv,
):
    sp = lax.axis_index("sp")
    y = lax.axis_index("tp")
    c = lax.rem(sp, 2)
    x = lax.rem(sp // 2, 4)
    z = sp // 8
    xh = x // 2
    xl = lax.rem(x, 2)
    g = lax.rem(xl + xh, 2)
    og = 1 - g
    oc = 1 - c
    me = sp // 4
    yp, ym, y2 = lax.rem(y + 1, 4), lax.rem(y + 3, 4), lax.rem(y + 2, 4)

    def holder(zz, hh):
        return (zz * 8 + (hh * 2 + lax.rem(g + hh, 2)) * 2 + c, y)

    def to_of(p):
        return lax.rem(z + 8 - NEAR[p // 2], 8), (xh if p % 2 == 0 else 1 - xh)

    def from_of(p):
        return lax.rem(z + NEAR[p // 2], 8), (xh if p % 2 == 0 else 1 - xh)

    dev_x = (z * 8 + (xh * 2 + 1 - xl) * 2 + c, y)
    dev_s = (z * 8 + x * 2 + oc, y)
    dev_p = (sp, yp)
    dev_m = (sp, ym)
    dev_2 = (sp, y2)
    dev_prev = (lax.rem(sp + 63, 64), y)
    dev_next = (lax.rem(sp + 1, 64), y)
    others_x = (xh * 2 + 1 - xl, (1 - xh) * 2 + xl, (1 - xh) * 2 + 1 - xl)

    def at_x(xx):
        return (z * 8 + xx * 2 + c, y)

    def at_z(zz):
        return (zz * 8 + x * 2 + c, y)

    def remote(src, dst, ss, rs, dev):
        return pltpu.make_async_remote_copy(
            src_ref=src, dst_ref=dst, send_sem=ss, recv_sem=rs, device_id=dev,
            device_id_type=MESH,
        )

    def all_sent(ref, sem):
        remote(ref, ref, sem, sem, dev_s).wait_send()

    def all_in(ref, sem):
        remote(ref, ref, sem, sem, dev_s).wait_recv()

    load_r = pltpu.make_async_copy(routes_hbm, routes_ref, load_sem.at[12])
    load_w = pltpu.make_async_copy(weight_hbm, weight_ref, load_sem.at[13])
    load_r.start()
    load_w.start()
    cols = pl.ds(pl.multiple_of(y * 512, 512), 512)
    load_x = pltpu.make_async_copy(x_hbm.at[:, cols], xq, load_sem.at[0])
    load_c = pltpu.make_async_copy(cot_hbm.at[:, cols], cq, load_sem.at[1])
    load_x.start()
    load_c.start()
    cols2 = pl.ds(pl.multiple_of(y2 * 512, 512), 512)
    load_far = [
        pltpu.make_async_copy(x_hbm.at[:, cols2], xq2, load_sem.at[10]),
        pltpu.make_async_copy(cot_hbm.at[:, cols2], cq2, load_sem.at[11]),
    ]
    for copy in load_far:
        copy.start()
    loads = [
        pltpu.make_async_copy(wg_hbm, wg, load_sem.at[2]),
        pltpu.make_async_copy(wu_hbm, wu, load_sem.at[3]),
        pltpu.make_async_copy(wd_hbm, wd, load_sem.at[4]),
    ]
    for copy in loads:
        copy.start()
    load_conv = pltpu.make_async_copy(conv_hbm, conv_ref, load_sem.at[5])
    load_conv.start()
    late_loads = [
        pltpu.make_async_copy(src, dst, load_sem.at[6 + i])
        for i, (src, dst) in enumerate((
            (proj_hbm, proj), (value_hbm, value_ref), (gate_hbm, gate_ref), (taps_hbm, taps_ref)
        ))
    ]
    for copy in late_loads:
        copy.start()

    barrier = pltpu.get_barrier_semaphore()

    for p in range(1, 16):
        pl.semaphore_signal(barrier, inc=1, device_id=holder(*to_of(p)), device_id_type=MESH)
    greeted = (
        dev_x, dev_s, dev_p, dev_m, dev_2, at_x(others_x[1]), at_x(others_x[2]), dev_prev, dev_next
    )
    for dev in greeted:
        pl.semaphore_signal(barrier, inc=1, device_id=dev, device_id_type=MESH)

    load_r.wait()
    load_w.wait()

    r0 = routes_ref[0:1, :]
    r1 = routes_ref[1:2, :]
    ids = lax.broadcasted_iota(jnp.int32, (16, 128), 0)
    e0 = ids == r0
    e1 = ids == r1
    named = jnp.where(e0, 1.0, 0.0) + jnp.where(e1, 1.0, 0.0)
    before = jnp.where(
        lax.broadcasted_iota(jnp.int32, (128, 128), 0)
        < lax.broadcasted_iota(jnp.int32, (128, 128), 1),
        1.0, 0.0,
    ).astype(BF)
    earlier = mm(named.astype(BF), before, NN)
    t0 = r0.astype(F32) * 16.0 + jnp.sum(jnp.where(e0, earlier, 0.0), axis=0, keepdims=True)
    t1 = r1.astype(F32) * 16.0 + jnp.sum(jnp.where(e1, earlier, 0.0), axis=0, keepdims=True)
    place = lax.broadcasted_iota(jnp.int32, (256, 128), 0).astype(F32)
    p0 = place == t0
    p1 = place == t1
    perm_val = (jnp.where(p0, 1.0, 0.0) + jnp.where(p1, 1.0, 0.0)).astype(BF)
    perm[...] = perm_val
    w0 = weight_ref[0:1, :]
    w1 = weight_ref[1:2, :]
    w_slot = jnp.sum(jnp.where(p0, w0, 0.0) + jnp.where(p1, w1, 0.0), axis=1, keepdims=True)
    load_x.wait()
    sendbuf[0] = mm(perm_val, xq[...], NN).astype(BF)
    load_c.wait()
    sendbuf[1] = (w_slot * mm(perm_val, cq[...], NN)).astype(BF)

    pl.semaphore_wait(barrier, 24)

    m_own = g * 2 + c

    def rows_of(q):
        return pl.ds(pl.multiple_of(q * 16, 16), 16)

    def place_of(a, p):
        return xc.at[a, p // 8, m_own, y, pl.ds(p % 8 * 16, 16)]

    def out_copy(a, p):
        zz, hh = to_of(p)
        return remote(
            sendbuf.at[a, rows_of(zz * 2 + hh)], place_of(a, p),
            a2a_send.at[a], a2a_recv.at[a, p // 8], holder(zz, hh),
        )

    def a2a_wait(a, h):
        if h == 0:
            own[a].wait()
        all_in(xc.at[a, h, m_own, y, pl.ds(0, 112 + 16 * h)], a2a_recv.at[a, h])

    def far_copy(a, p):
        zz, hh = to_of(p)
        return remote(
            sendbuf2.at[a, rows_of(zz * 2 + hh)], xc.at[a, 0, m_own, y2, pl.ds(p * 16, 16)],
            far_send.at[a], far_recv.at[a], holder(zz, hh),
        )

    own = [
        pltpu.make_async_copy(sendbuf.at[a, rows_of(me)], place_of(a, 0), own_sem.at[a])
        for a in range(2)
    ]
    own2 = [
        pltpu.make_async_copy(
            sendbuf2.at[a, rows_of(me)], xc.at[a, 0, m_own, y2, pl.ds(0, 16)], own_sem.at[2 + a]
        )
        for a in range(2)
    ]

    def push(h):
        for a in range(2):
            for p in reversed(range(8 * h, 8 * h + 8)):
                if p == 0:
                    own[a].start()
                else:
                    out_copy(a, p).start()

    def push_far(a):
        for p in reversed(range(1, 8)):
            far_copy(a, p).start()
        own2[a].start()

    def far_wait(a):
        own2[a].wait()
        all_in(xc.at[a, 0, m_own, y2, pl.ds(0, 112)], far_recv.at[a])

    push(0)
    load_far[0].wait()
    sendbuf2[0] = mm(perm_val, xq2[...], NN).astype(BF)
    load_far[1].wait()
    sendbuf2[1] = (w_slot * mm(perm_val, cq2[...], NN)).astype(BF)

    lane = lax.broadcasted_iota(jnp.int32, (128, 128), 1)

    def sums_out(phase, one, two):
        cols2 = jnp.where(lane == 0, one, 0.0) + jnp.where(lane == 1, two, 0.0)
        st_out[phase] = cols2.T[0:8, :]
        return [
            remote(
                st_out.at[phase], st_in.at[phase, j], st_send.at[phase], st_recv.at[phase], dev
            )
            for j, dev in enumerate((dev_p, dev_m, dev_2))
        ]

    def sums_in(phase):
        all_in(st_in.at[phase], st_recv.at[phase])
        tot = (st_out[phase] + st_in[phase, 2]) + (st_in[phase, 0] + st_in[phase, 1])
        tall = jnp.concatenate([tot, jnp.zeros((120, 128), F32)], axis=0).T
        return tall[:, 0:1], tall[:, 1:2]

    load_conv.wait()
    conv_vals = conv_ref[...].astype(F32)
    stats = sums_out(
        0,
        jnp.sum(conv_vals, axis=1, keepdims=True),
        jnp.sum(conv_vals * conv_vals, axis=1, keepdims=True),
    )
    for copy in stats:
        copy.start()

    first, second = pl.ds(0, 64), pl.ds(64, 64)
    listed = [(g, y), (g, ym), (g, yp), (g, y2), (og, y), (og, ym), (og, yp), (og, y2)]

    def block(a, h, gg, cc, yy):
        return xc.at[a, h, gg * 2 + cc, yy]

    def ag_copy(a, h, kind, ref, dev):
        lot = 4 if kind in (3, 4) else 8 if kind >= 8 else 0
        slot = kind if kind < 8 else 5 + kind // 4
        slot = slot + 1 if kind >= 8 else slot
        return remote(
            ref, ref, ag_send.at[a * 2 + h + lot], ag_recv.at[a * 2 + h, slot], dev
        )

    def ag_out(a, h, kind):
        if kind >= 8:
            gg, yy = listed[kind - 8]
            return ag_copy(a, h, kind, block(a, h, gg, c, yy), dev_s)
        ref, dev = (
            (block(a, h, g, c, y), dev_x),
            (block(a, h, g, c, y), dev_p),
            (block(a, h, g, c, y), dev_m),
            (block(a, h, g, c, ym).at[first], dev_p),
            (block(a, h, g, c, yp).at[second], dev_m),
            (block(a, h, og, c, y), dev_p),
            (block(a, h, og, c, y), dev_m),
            (block(a, h, g, c, y2), dev_x),
        )[kind]
        return ag_copy(a, h, kind, ref, dev)

    def ag_in(a, h, kind):
        if kind >= 8:
            gg, yy = listed[kind - 8]
            return ag_copy(a, h, kind, block(a, h, gg, oc, yy), dev_s)
        ref, dev = (
            (block(a, h, og, c, y), dev_x),
            (block(a, h, g, c, ym), dev_m),
            (block(a, h, g, c, yp), dev_p),
            (block(a, h, g, c, y2).at[first], dev_m),
            (block(a, h, g, c, y2).at[second], dev_p),
            (block(a, h, og, c, ym), dev_m),
            (block(a, h, og, c, yp), dev_p),
            (block(a, h, og, c, y2), dev_x),
        )[kind]
        return ag_copy(a, h, kind, ref, dev)

    def go(a, h, *kinds):
        for kind in kinds:
            ag_out(a, h, kind).start()

    def got(a, h, *kinds):
        for kind in kinds:
            ag_in(a, h, kind).wait_recv()

    def sib_got(a, h, gg):
        all_in(xc.at[a, h, gg * 2 + oc], ag_recv.at[a * 2 + h, 8 if gg is g else 9])

    def relay_y(a, h):
        got(a, h, 1)
        go(a, h, *((3, 9) if h else (9,)))
        got(a, h, 2)
        go(a, h, *((4, 10) if h else (10,)))

    def relay_x(a, h):
        got(a, h, 0)
        go(a, h, 5, 6, 12)

    def relay_far(a, h):
        if h:
            got(a, h, 3, 4)
        else:
            far_wait(a)
        go(a, h, 7, 11)

    def relay_last(a, h):
        got(a, h, 5)
        go(a, h, 13)
        got(a, h, 6)
        go(a, h, 14)
        got(a, h, 7)
        go(a, h, 15)

    def pair(gg):
        return pl.ds(gg * 2, 2)

    def rows_at(a, h, gg, q):
        return xc[a, h, pair(gg), q].reshape(256, 512)

    def pre_acts(h, gg):
        pre_g = jnp.zeros((256, 224), F32)
        pre_u = jnp.zeros((256, 224), F32)
        for q in range(4):
            span = slice(q * 512, q * 512 + 512)
            rows = rows_at(0, h, gg, q)
            pre_g += mm(rows, wg[:, span], NT)
            pre_u += mm(rows, wu[:, span], NT)
        return pre_g, pre_u

    def forward(h, gg, pres):
        pre_g, pre_u = pres
        d_act = jnp.zeros((256, 224), F32)
        for q in range(4):
            span = slice(q * 512, q * 512 + 512)
            d_act += mm(rows_at(1, h, gg, q), wd[:, span], NT)
        sig = jax.nn.sigmoid(pre_g)
        d_gate = (d_act * pre_u * swish_slope(pre_g, sig)).astype(BF)
        d_up = (d_act * pre_g * sig).astype(BF)
        return d_gate, d_up, pre_g * sig * pre_u

    def back(h, gg, grads, yy):
        span = pl.ds(pl.multiple_of(yy * 512, 512), 512)
        term = mm(grads[0], wg[:, span], NN) + mm(grads[1], wu[:, span], NN)
        part[h, pair(gg), yy] = term.astype(BF).reshape(2, 128, 512)

    order = (y2, yp, ym, y)

    def sib_copy(h, gg, j):
        at = (0 if gg is g else 4) + j
        return remote(
            part.at[h, gg * 2 + oc, order[j]], sib_in.at[h, gg, order[j]],
            sb_send.at[h], sb_recv.at[h, at], dev_s,
        )

    def whole(h, gg, pres, *between):
        grads = forward(h, gg, pres)
        for j in range(4):
            back(h, gg, grads, order[j])
            sib_copy(h, gg, j).start()
            if j < len(between) and between[j]:
                between[j]()
        slot = h * 2 + gg
        act_t[slot] = grads[2].T.astype(BF)
        dg_t[slot] = grads[0].T
        du_t[slot] = grads[1].T

    m_g, m_o = g * 2 + c, og * 2 + c

    def pair_sum(h, gg, j):
        sib_copy(h, gg, j).wait_recv()
        at = (h, gg * 2 + c, order[j])
        part[at] = (part[at].astype(F32) + sib_in[h, gg, order[j]].astype(F32)).astype(BF)

    def pieces(h):
        n = 1 + h
        return n, [i for k in range(n) for i in (k, n + k)]

    def piece(h, i):
        rows = 64 // (1 + h)
        return pl.ds(i * rows, rows)

    def rs_copy(h, kind):
        n = 1 + h
        if kind < 4:
            at = piece(h, kind)
            src, dst, dev = part.at[h, m_o, y2, at], in_a.at[h, at], dev_x
        elif kind < 8:
            at = piece(h, kind - 4)
            src, dst = part.at[h, m_g, y2, at], in_c.at[h, at]
            dev = dev_p if kind - 4 < n else dev_m
        elif kind < 12:
            at = piece(h, kind - 8)
            yy, i, dev = (yp, 0, dev_p) if kind - 8 < n else (ym, 1, dev_m)
            src, dst = part.at[h, m_g, yy, at], in_e.at[h, i, at]
        else:
            src, dst, dev = (
                (part.at[h, m_o, yp, first], in_b.at[h, 0, first], dev_p),
                (part.at[h, m_o, ym, first], in_b.at[h, 1, first], dev_m),
                (part.at[h, m_o, y, first], in_d.at[h, first], dev_x),
                (part.at[h, m_g, yp, second], in_e.at[h, 0, second], dev_p),
                (part.at[h, m_g, ym, first], in_e.at[h, 1, first], dev_m),
                (part.at[h, m_o, yp, second], in_b.at[h, 0, second], dev_p),
                (part.at[h, m_o, ym, second], in_b.at[h, 1, second], dev_m),
                (part.at[h, m_o, y, second], in_d.at[h, second], dev_x),
            )[kind - 12]
        slot = kind if kind < 8 else 8 if kind in (12, 13) else 10 if kind in (17, 18) else 9
        lot = 0 if kind in (4, 5, 6, 7, 12, 13, 14, 17, 18, 19) else 1
        return remote(src, dst, rs_send.at[h, lot], rs_recv.at[h, slot], dev)

    def rs_chain(h):
        pair_sum(h, og, 0)
        for i in pieces(h)[1]:
            rs_copy(h, i).start()

    def rs_open(h):
        pair_sum(h, og, 1)
        rs_copy(h, 12).start()
        rs_copy(h, 17).start()
        pair_sum(h, og, 2)
        rs_copy(h, 13).start()
        rs_copy(h, 18).start()

    def rs_own(h):
        pair_sum(h, g, 1)
        pair_sum(h, g, 2)
        pair_sum(h, g, 0)
        pair_sum(h, og, 3)
        pair_sum(h, g, 3)

    def rs_early(h):
        rs_copy(h, 15).start()
        rs_copy(h, 16).start()

    def add_to(at, *terms):
        value = part[at].astype(F32)
        for term in terms:
            value += term.astype(F32)
        part[at] = value.astype(BF)

    def rs_far(h):
        for i in pieces(h)[1]:
            rs_copy(h, i).wait_recv()
            add_to((h, m_g, y2, piece(h, i)), in_a[h, piece(h, i)])
            rs_copy(h, 4 + i).start()

    def rs_cross(h, half):
        at = (first, second)[half]
        all_in(in_b.at[h, :, at], rs_recv.at[h, 8 + 2 * half])
        add_to((h, m_o, y, at), in_b[h, 0, at], in_b[h, 1, at])
        rs_copy(h, 14 + 5 * half).start()

    def rs_near(h):
        n, turns = pieces(h)
        for i in turns:
            rs_copy(h, 4 + i).wait_recv()
            add_to((h, m_g, yp if i < n else ym, piece(h, i)), in_c[h, piece(h, i)])
            rs_copy(h, 8 + i).start()

    def ret_copy(p):
        zz, hh = from_of(p)
        return remote(
            total.at[p // 8, pl.ds(p % 8 * 16, 16)], ret.at[rows_of(me)],
            ret_send.at[0], ret_recv.at[0], holder(zz, hh),
        )

    own_back = pltpu.make_async_copy(total.at[0, pl.ds(0, 16)], ret.at[rows_of(me)], own_sem.at[0])

    def rs_close(h):
        all_in(part.at[h, 0, pl.ds(0, 3)], rs_recv.at[h, 9])
        total[h] = (
            part[h, m_g, y].astype(F32) + in_d[h].astype(F32)
            + in_e[h, 0].astype(F32) + in_e[h, 1].astype(F32)
        ).astype(BF)
        for p in reversed(range(8 * h, 8 * h + 8)):
            if p == 0:
                own_back.start()
            else:
                ret_copy(p).start()

    def weight_grad(out_ref, source, a, half):
        def tile(q, _):
            acc = jnp.zeros((source.shape[1], 512), F32)
            for h in range(2):
                for gg in range(2):
                    acc += mm(source[h * 2 + gg], rows_at(a, h, gg, q), NN)
            out_ref[:, pl.ds(pl.multiple_of(q * 512, 512), 512)] = acc.astype(BF)
            return 0

        lax.fori_loop(2 * half, 2 * half + 2, tile, 0)

    def drain_rows(a):
        all_sent(sendbuf.at[a, pl.ds(0, 240)], a2a_send.at[a])
        all_sent(sendbuf2.at[a, pl.ds(0, 112)], far_send.at[a])
        for h in range(2):
            all_sent(xc.at[a, h, pl.ds(0, 2), pl.ds(0, 3)], ag_send.at[a * 2 + h])
            all_sent(xc.at[a, h, pl.ds(0, 2)], ag_send.at[a * 2 + h + 8])
        all_sent(xc.at[a, 1, 0, 0], ag_send.at[a * 2 + 5])

    def drain_sums():
        for h in range(2):
            all_sent(part.at[h, pl.ds(0, 2)], sb_send.at[h])
            all_sent(part.at[h, 0], rs_send.at[h, 0])
            all_sent(part.at[h, 0, pl.ds(0, 3)], rs_send.at[h, 1])

    a2a_wait(0, 0)
    go(0, 0, 0, 1, 2, 8)
    push_far(0)
    push_far(1)
    push(1)
    a2a_wait(1, 0)
    go(1, 0, 0, 1, 2, 8)
    relay_x(0, 0)
    relay_x(1, 0)
    relay_y(0, 0)
    relay_y(1, 0)
    relay_far(0, 0)
    relay_far(1, 0)
    a2a_wait(0, 1)
    go(0, 1, 0, 1, 2, 8)
    sum1, sum2 = sums_in(0)
    mean = sum1 / DB
    rstd = lax.rsqrt(sum2 / DB - mean * mean + 1e-05)
    norm_val = (conv_ref[...].astype(F32) - mean) * rstd
    zpre = norm_val * gain_ref[...]
    zsig = jax.nn.sigmoid(zpre)
    normed[...] = norm_val
    mixed[...] = (zpre * zsig).astype(BF)
    slope[...] = swish_slope(zpre, zsig) * gain_ref[...]
    scale[...] = jnp.broadcast_to(rstd, (128, 256))
    for copy in loads:
        copy.wait()
    sib_got(0, 0, g)
    pres = pre_acts(0, g)
    a2a_wait(1, 1)
    go(1, 1, 0, 1, 2, 8)
    sib_got(1, 0, g)
    whole(0, g, pres)
    relay_last(0, 0)
    relay_last(1, 0)
    relay_y(0, 1)
    sib_got(0, 0, og)
    pres = pre_acts(0, og)
    sib_got(1, 0, og)
    relay_y(1, 1)
    relay_x(0, 1)
    whole(0, og, pres, lambda: relay_far(0, 1), lambda: relay_x(1, 1))
    sib_got(0, 1, g)
    pres = pre_acts(1, g)
    relay_far(1, 1)
    rs_chain(0)
    rs_open(0)
    sib_got(1, 1, g)
    whole(1, g, pres)
    rs_own(0)
    rs_early(0)
    relay_last(0, 1)
    sib_got(0, 1, og)
    relay_last(1, 1)
    pres = pre_acts(1, og)
    sib_got(1, 1, og)
    whole(1, og, pres, lambda: rs_far(0), None, lambda: rs_chain(1))
    rs_open(1)
    rs_own(1)
    weight_grad(gg_ref, dg_t, 0, 0)
    rs_cross(0, 0)
    rs_cross(0, 1)
    drain_rows(0)
    weight_grad(gg_ref, dg_t, 0, 1)
    rs_far(1)
    rs_early(1)
    rs_near(0)
    rs_cross(1, 0)
    weight_grad(gu_ref, du_t, 0, 0)
    rs_cross(1, 1)
    weight_grad(gu_ref, du_t, 0, 1)
    rs_near(1)
    weight_grad(gd_ref, act_t, 1, 0)
    drain_rows(1)
    weight_grad(gd_ref, act_t, 1, 1)
    rs_close(0)
    rs_close(1)
    drain_sums()

    all_in(ret.at[pl.ds(0, 240)], ret_recv.at[0])
    own_back.wait()
    moe = mm(perm[...], ret[...], TN)
    res_ref[y] = (cq[...].astype(F32) + moe).astype(BF)

    def slab(i):
        return pl.ds(i * 32, 32)

    def res_copy(yy, i, kind, dev):
        ref = res_ref.at[yy, slab(i)]
        return remote(ref, ref, res_send.at[0], res_recv.at[kind], dev)

    for i in range(4):
        res_copy(y, i, min(i, 2), dev_p).start()
        res_copy(y, 3 - i, 3 + min(i, 2), dev_m).start()
    for copy in late_loads:
        copy.wait()

    def pair_of(q):
        return pl.ds(q * 2, 2)

    def gp_copy(q, j):
        return remote(
            gp.at[oc, :, pair_of(q)], gp_sib.at[:, pair_of(q)], gs_send.at[0], gs_recv.at[j], dev_s
        )

    def proj_terms(q, j):
        feats = res_ref[q]
        term = mm(feats, mixed[...], TN)
        for i in range(8):
            for cc in range(2):
                gp[cc, i % 4, q * 2 + i // 4] = term[i * 64 + cc * 32 : i * 64 + cc * 32 + 32].astype(BF)
        gp_copy(q, j).start()
        return mm(feats, proj[pl.ds(pl.multiple_of(q * 512, 512), 512), :], NN)

    def gx_copy(q, j, i):
        return remote(
            gp.at[c, others_x[i], pair_of(q)], gp_x.at[i, pair_of(q)],
            gx_send.at[0], gx_recv.at[j], at_x(others_x[i]),
        )

    def over_x(q, j):
        gp_copy(q, j).wait_recv()
        gp[c, :, pair_of(q)] = (
            gp[c, :, pair_of(q)].astype(F32) + gp_sib[:, pair_of(q)].astype(F32)
        ).astype(BF)
        for i in (1, 2, 0):
            gx_copy(q, j, i).start()

    def gz_copy(to, slot):
        return remote(gp_row.at[to], gp_z.at[slot], gz_send.at[0], gz_recv.at[0], at_z(to))

    def over_z(q, j):
        pair = pair_of(q)
        all_in(gp_x.at[:, pair], gx_recv.at[j])
        gp_row[pair] = (
            (gp[c, x, pair].astype(F32) + gp_x[0, pair].astype(F32))
            + (gp_x[1, pair].astype(F32) + gp_x[2, pair].astype(F32))
        ).astype(BF)
        for i in range(2):

            @pl.when(q * 2 + i != z)
            def _():
                gz_copy(q * 2 + i, z).start()

    d_mixed = proj_terms(y, 0)
    for i in range(2):
        res_copy(ym, i, i, dev_m).wait_recv()
        res_copy(ym, i, 6, dev_p).start()
        res_copy(yp, 3 - i, 3 + i, dev_p).wait_recv()
        res_copy(yp, 3 - i, 7, dev_m).start()
    over_x(y, 0)
    all_in(res_ref.at[ym, pl.ds(64, 64)], res_recv.at[2])
    d_mixed += proj_terms(ym, 1)
    all_in(res_ref.at[yp, pl.ds(0, 64)], res_recv.at[5])
    d_mixed += proj_terms(yp, 2)
    over_x(ym, 1)
    over_x(yp, 2)
    all_in(res_ref.at[y2, pl.ds(0, 64)], res_recv.at[6])
    all_in(res_ref.at[y2, pl.ds(64, 64)], res_recv.at[7])
    d_mixed += proj_terms(y2, 3)
    d_norm = d_mixed * slope[...]
    norm_val = normed[...]
    stats2 = sums_out(
        1,
        jnp.sum(d_norm, axis=1, keepdims=True),
        jnp.sum(d_norm * norm_val, axis=1, keepdims=True),
    )
    for copy in stats2:
        copy.start()
    over_x(y2, 3)
    over_z(y, 0)

    first_sum, second_sum = sums_in(1)
    conv_grad = (
        scale[...] * (d_norm - first_sum / DB - norm_val * (second_sum / DB))
    ).astype(BF)
    halo_out[...] = conv_grad[0:32]
    halo = remote(halo_out, halo_in, halo_sem.at[0], halo_sem.at[1], dev_prev)
    halo.start()
    ext[0:128, :] = conv_grad.astype(F32)
    over_z(ym, 1)
    over_z(yp, 2)

    def correlate(start, count):
        acc = jnp.zeros((count, 256), F32)
        for k in range(WIDTH):
            acc += ext[start + k : start + k + count, :] * taps_ref[k : k + 1, :]
        return acc

    def glu_grads(start, count, unit_grad):
        span = slice(start, start + count)
        sig = jax.nn.sigmoid(gate_ref[span, :].astype(F32))
        gv_ref[span, :] = (unit_grad * sig).astype(BF)
        gt_ref[span, :] = (
            unit_grad * value_ref[span, :].astype(F32) * sig * (1.0 - sig)
        ).astype(BF)

    glu_grads(0, 64, correlate(0, 64))
    glu_grads(64, 32, correlate(64, 32))

    over_z(y2, 3)
    halo.wait_recv()
    keep = jnp.where(sp < 63, 1.0, 0.0)
    ext[128:160, :] = halo_in[...].astype(F32) * keep
    glu_grads(96, 32, correlate(96, 32))

    all_in(gp_z.at[pl.ds(0, 7)], gz_recv.at[0])
    rows_sum = gp_row[z].astype(F32)
    for k in range(1, 8):
        zz = lax.rem(z + k, 8)
        rows_sum += gp_z[zz].astype(F32)
    gp_ref[...] = rows_sum

    all_sent(ret.at[pl.ds(0, 240)], ret_send.at[0])
    for phase in range(2):
        all_sent(st_in.at[phase], st_send.at[phase])
    halo.wait_send()
    all_sent(res_ref.at[pl.ds(0, 3)], res_send.at[0])
    all_sent(gp.at[oc], gs_send.at[0])
    all_sent(gp_x, gx_send.at[0])
    all_sent(gp_z.at[pl.ds(0, 7)], gz_send.at[0])


def write_kernel(*refs):
    copies = [pltpu.make_async_copy(refs[i], refs[6 + i], refs[12].at[i]) for i in range(6)]
    for copy in copies:
        copy.start()
    for copy in copies:
        copy.wait()


def local(
    moe_input,
    out_cotangent,
    routes,
    route_weight,
    w_gate,
    w_up,
    w_down,
    out_proj,
    conv_out,
    glu_value,
    glu_gate,
    taps,
    norm_gain,
):
    units, width = w_down.shape[1:]
    tokens, channels = conv_out.shape
    vmem = pl.BlockSpec(memory_space=pltpu.VMEM)
    hbm = pl.BlockSpec(memory_space=pl.ANY)
    dma = pltpu.SemaphoreType.DMA
    grad = jax.ShapeDtypeStruct((units, width), BF)
    glu = jax.ShapeDtypeStruct((tokens, channels), BF)
    shapes = (grad, grad, grad, jax.ShapeDtypeStruct((32, channels), F32), glu, glu)
    results = pl.pallas_call(
        backward_kernel,
        out_shape=[pltpu.VMEM(a.shape, a.dtype) for a in shapes],
        in_specs=[vmem] + [hbm] * 12,
        out_specs=[vmem] * 6,
        scratch_shapes=[
            pltpu.VMEM((128, 512), BF),
            pltpu.VMEM((128, 512), BF),
            pltpu.VMEM((128, 512), BF),
            pltpu.VMEM((128, 512), BF),
            pltpu.VMEM((256, 128), BF),
            pltpu.VMEM((2, 256, 512), BF),
            pltpu.VMEM((2, 256, 512), BF),
            pltpu.VMEM((2, 2, 4, 4, 128, 512), BF),
            pltpu.VMEM((units, width), BF),
            pltpu.VMEM((units, width), BF),
            pltpu.VMEM((units, width), BF),
            pltpu.VMEM((4, units, 256), BF),
            pltpu.VMEM((4, units, 256), BF),
            pltpu.VMEM((4, units, 256), BF),
            pltpu.VMEM((2, 4, 4, 128, 512), BF),
            pltpu.VMEM((2, 2, 4, 128, 512), BF),
            pltpu.VMEM((2, 128, 512), BF),
            pltpu.VMEM((2, 2, 128, 512), BF),
            pltpu.VMEM((2, 128, 512), BF),
            pltpu.VMEM((2, 128, 512), BF),
            pltpu.VMEM((2, 2, 128, 512), BF),
            pltpu.VMEM((2, 128, 512), BF),
            pltpu.VMEM((256, 512), BF),
            pltpu.VMEM((2, tokens), jnp.int32),
            pltpu.VMEM((2, tokens), F32),
            pltpu.VMEM((tokens, channels), BF),
            pltpu.VMEM((tokens, channels), BF),
            pltpu.VMEM((tokens, channels), BF),
            pltpu.VMEM((WIDTH, channels), F32),
            pltpu.VMEM((4, 128, 512), BF),
            pltpu.VMEM((width, 256), BF),
            pltpu.VMEM((128, 256), F32),
            pltpu.VMEM((128, 256), F32),
            pltpu.VMEM((128, 256), BF),
            pltpu.VMEM((128, 256), F32),
            pltpu.VMEM((2, 8, 128), F32),
            pltpu.VMEM((2, 3, 8, 128), F32),
            pltpu.VMEM((160, 256), F32),
            pltpu.VMEM((32, 256), BF),
            pltpu.VMEM((32, 256), BF),
            pltpu.VMEM((2, 4, 8, 32, 256), BF),
            pltpu.VMEM((4, 8, 32, 256), BF),
            pltpu.VMEM((3, 8, 32, 256), BF),
            pltpu.VMEM((8, 32, 256), BF),
            pltpu.VMEM((8, 32, 256), BF),
            dma((14,)), dma((4,)),
            dma((2,)), dma((2, 2)), dma((2,)), dma((2,)), dma((12,)), dma((4, 10)),
            dma((2,)), dma((2, 8)), dma((2, 2)), dma((2, 11)),
            dma((1,)), dma((1,)), dma((1,)), dma((8,)),
            dma((2,)), dma((2,)), dma((2,)),
            dma((1,)), dma((4,)), dma((1,)), dma((4,)), dma((1,)), dma((1,)),
        ],
        compiler_params=pltpu.CompilerParams(
            collective_id=0, has_side_effects=True, vmem_limit_bytes=60 * 1024 * 1024
        ),
        name="backward",
    )(
        norm_gain[None, :], routes.T, route_weight.T,
        moe_input, out_cotangent, w_gate[0].T, w_up[0].T, w_down[0], out_proj,
        conv_out, glu_value, glu_gate, taps,
    )
    gg, gu, gd, gp, gv, gt = pl.pallas_call(
        write_kernel,
        out_shape=shapes,
        in_specs=[vmem] * 6,
        out_specs=[hbm] * 6,
        scratch_shapes=[dma((6,))],
        compiler_params=pltpu.CompilerParams(vmem_limit_bytes=1024 * 1024),
        name="write_out",
    )(*(pltpu.with_memory_space_constraint(r, pltpu.VMEM) for r in results))
    return (gg.T[None], gu.T[None], gd[None], gp, gv, gt)


def solution(mesh):
    in_specs = (
        P("sp", None),
        P("sp", None),
        P("sp", None),
        P("sp", None),
        P("sp", None, "tp"),
        P("sp", None, "tp"),
        P("sp", "tp", None),
        P(None, "tp"),
        P("sp", "tp"),
        P("sp", "tp"),
        P("sp", "tp"),
        P(None, "tp"),
        P("tp"),
    )
    out_specs = (
        P("sp", None, "tp"),
        P("sp", None, "tp"),
        P("sp", "tp", None),
        P("sp", "tp"),
        P("sp", "tp"),
        P("sp", "tp"),
    )
    return jax.shard_map(local, mesh=mesh, in_specs=in_specs, out_specs=out_specs, check_vma=False)
```

```python
import jax
import jax.numpy as jnp
from jax import lax
from jax.experimental import pallas as pl
from jax.experimental.pallas import tpu as pltpu
from jax.sharding import PartitionSpec as P

DB = 1024
WIDTH = 31
MESH = pl.DeviceIdType.MESH
BF = jnp.bfloat16
F32 = jnp.float32
NEAR = (0, 1, 7, 2, 6, 3, 5, 4)
NT = (((1,), (1,)), ((), ()))
NN = (((1,), (0,)), ((), ()))
TN = (((0,), (0,)), ((), ()))


def mm(a, b, dims):
    return lax.dot_general(a, b, dims, preferred_element_type=F32)


def swish_slope(pre, sig):
    return sig * (1.0 + pre * (1.0 - sig))


def backward_kernel(
    gain_ref, routes_hbm, weight_hbm,
    x_hbm, cot_hbm, wg_hbm, wu_hbm, wd_hbm, proj_hbm, conv_hbm, value_hbm, gate_hbm, taps_hbm,
    gg_ref, gu_ref, gd_ref, gp_ref, gv_ref, gt_ref,
    xq, cq, xq2, cq2, perm, sendbuf, sendbuf2, xc, wg, wu, wd, act_t, dg_t, du_t,
    part, sib_in, in_a, in_b, in_c, in_d, in_e, total, ret,
    routes_ref, weight_ref, conv_ref, value_ref, gate_ref, taps_ref, res_ref, proj, normed, slope, mixed, mixed2, scale, st_out, st_in, ext, halo_out, halo_in,
    gp, gp_sib, gp_x, gp_row, gp_z, gp_z2, fin_out, fin_in,
    load_sem, own_sem, a2a_send, a2a_recv, far_send, far_recv, ag_send, ag_recv,
    sb_send, sb_recv, rs_send, rs_recv, ret_send, ret_recv, res_send, res_recv,
    st_send, st_recv, halo_sem, gs_send, gs_recv, gx_send, gx_recv, gz_send, gz_recv,
    mx_sem, fin_sem, gz2_send, gz2_recv,
):
    sp = lax.axis_index("sp")
    y = lax.axis_index("tp")
    c = lax.rem(sp, 2)
    x = lax.rem(sp // 2, 4)
    z = sp // 8
    xh = x // 2
    xl = lax.rem(x, 2)
    g = lax.rem(xl + xh, 2)
    og = 1 - g
    oc = 1 - c
    me = sp // 4
    yp, ym, y2 = lax.rem(y + 1, 4), lax.rem(y + 3, 4), lax.rem(y + 2, 4)

    def holder(zz, hh):
        return (zz * 8 + (hh * 2 + lax.rem(g + hh, 2)) * 2 + c, y)

    def to_of(p):
        return lax.rem(z + 8 - NEAR[p // 2], 8), (xh if p % 2 == 0 else 1 - xh)

    def from_of(p):
        return lax.rem(z + NEAR[p // 2], 8), (xh if p % 2 == 0 else 1 - xh)

    dev_x = (z * 8 + (xh * 2 + 1 - xl) * 2 + c, y)
    dev_s = (z * 8 + x * 2 + oc, y)
    dev_p = (sp, yp)
    dev_m = (sp, ym)
    dev_2 = (sp, y2)
    dev_prev = (lax.rem(sp + 63, 64), y)
    dev_next = (lax.rem(sp + 1, 64), y)
    others_x = (xh * 2 + 1 - xl, (1 - xh) * 2 + xl, (1 - xh) * 2 + 1 - xl)

    def at_x(xx):
        return (z * 8 + xx * 2 + c, y)

    def at_z(zz):
        return (zz * 8 + x * 2 + c, y)

    def remote(src, dst, ss, rs, dev):
        return pltpu.make_async_remote_copy(
            src_ref=src, dst_ref=dst, send_sem=ss, recv_sem=rs, device_id=dev,
            device_id_type=MESH,
        )

    def all_sent(ref, sem):
        remote(ref, ref, sem, sem, dev_s).wait_send()

    def all_in(ref, sem):
        remote(ref, ref, sem, sem, dev_s).wait_recv()

    load_r = pltpu.make_async_copy(routes_hbm, routes_ref, load_sem.at[12])
    load_w = pltpu.make_async_copy(weight_hbm, weight_ref, load_sem.at[13])
    load_r.start()
    load_w.start()
    cols = pl.ds(pl.multiple_of(y * 512, 512), 512)
    load_x = pltpu.make_async_copy(x_hbm.at[:, cols], xq, load_sem.at[0])
    load_c = pltpu.make_async_copy(cot_hbm.at[:, cols], cq, load_sem.at[1])
    load_x.start()
    load_c.start()
    cols2 = pl.ds(pl.multiple_of(y2 * 512, 512), 512)
    load_far = [
        pltpu.make_async_copy(x_hbm.at[:, cols2], xq2, load_sem.at[10]),
        pltpu.make_async_copy(cot_hbm.at[:, cols2], cq2, load_sem.at[11]),
    ]
    for copy in load_far:
        copy.start()
    loads = [
        pltpu.make_async_copy(wg_hbm, wg, load_sem.at[2]),
        pltpu.make_async_copy(wu_hbm, wu, load_sem.at[3]),
        pltpu.make_async_copy(wd_hbm, wd, load_sem.at[4]),
    ]
    for copy in loads:
        copy.start()
    load_conv = pltpu.make_async_copy(conv_hbm, conv_ref, load_sem.at[5])
    load_conv.start()
    late_loads = [
        pltpu.make_async_copy(src, dst, load_sem.at[6 + i])
        for i, (src, dst) in enumerate((
            (proj_hbm, proj), (value_hbm, value_ref), (gate_hbm, gate_ref), (taps_hbm, taps_ref)
        ))
    ]
    for copy in late_loads:
        copy.start()

    barrier = pltpu.get_barrier_semaphore()

    for p in range(1, 16):
        pl.semaphore_signal(barrier, inc=1, device_id=holder(*to_of(p)), device_id_type=MESH)
    greeted = (
        dev_x, dev_s, dev_p, dev_m, dev_2, at_x(others_x[1]), at_x(others_x[2]), dev_prev, dev_next
    )
    for dev in greeted:
        pl.semaphore_signal(barrier, inc=1, device_id=dev, device_id_type=MESH)

    load_r.wait()
    load_w.wait()

    r0 = routes_ref[0:1, :]
    r1 = routes_ref[1:2, :]
    ids = lax.broadcasted_iota(jnp.int32, (16, 128), 0)
    e0 = ids == r0
    e1 = ids == r1
    named = jnp.where(e0, 1.0, 0.0) + jnp.where(e1, 1.0, 0.0)
    before = jnp.where(
        lax.broadcasted_iota(jnp.int32, (128, 128), 0)
        < lax.broadcasted_iota(jnp.int32, (128, 128), 1),
        1.0, 0.0,
    ).astype(BF)
    earlier = mm(named.astype(BF), before, NN)
    t0 = r0.astype(F32) * 16.0 + jnp.sum(jnp.where(e0, earlier, 0.0), axis=0, keepdims=True)
    t1 = r1.astype(F32) * 16.0 + jnp.sum(jnp.where(e1, earlier, 0.0), axis=0, keepdims=True)
    place = lax.broadcasted_iota(jnp.int32, (256, 128), 0).astype(F32)
    p0 = place == t0
    p1 = place == t1
    perm_val = (jnp.where(p0, 1.0, 0.0) + jnp.where(p1, 1.0, 0.0)).astype(BF)
    perm[...] = perm_val
    w0 = weight_ref[0:1, :]
    w1 = weight_ref[1:2, :]
    w_slot = jnp.sum(jnp.where(p0, w0, 0.0) + jnp.where(p1, w1, 0.0), axis=1, keepdims=True)
    load_x.wait()
    sendbuf[0] = mm(perm_val, xq[...], NN).astype(BF)
    load_c.wait()
    sendbuf[1] = (w_slot * mm(perm_val, cq[...], NN)).astype(BF)

    pl.semaphore_wait(barrier, 24)

    m_own = g * 2 + c

    def rows_of(q):
        return pl.ds(pl.multiple_of(q * 16, 16), 16)

    def place_of(a, p):
        return xc.at[a, p // 8, m_own, y, pl.ds(p % 8 * 16, 16)]

    def out_copy(a, p):
        zz, hh = to_of(p)
        return remote(
            sendbuf.at[a, rows_of(zz * 2 + hh)], place_of(a, p),
            a2a_send.at[a], a2a_recv.at[a, p // 8], holder(zz, hh),
        )

    def a2a_wait(a, h):
        if h == 0:
            own[a].wait()
        all_in(xc.at[a, h, m_own, y, pl.ds(0, 112 + 16 * h)], a2a_recv.at[a, h])

    def far_copy(a, p):
        zz, hh = to_of(p)
        return remote(
            sendbuf2.at[a, rows_of(zz * 2 + hh)], xc.at[a, 0, m_own, y2, pl.ds(p * 16, 16)],
            far_send.at[a], far_recv.at[a], holder(zz, hh),
        )

    own = [
        pltpu.make_async_copy(sendbuf.at[a, rows_of(me)], place_of(a, 0), own_sem.at[a])
        for a in range(2)
    ]
    own2 = [
        pltpu.make_async_copy(
            sendbuf2.at[a, rows_of(me)], xc.at[a, 0, m_own, y2, pl.ds(0, 16)], own_sem.at[2 + a]
        )
        for a in range(2)
    ]

    def push(h):
        for a in range(2):
            for p in reversed(range(8 * h, 8 * h + 8)):
                if p == 0:
                    own[a].start()
                else:
                    out_copy(a, p).start()

    def push_far(a):
        for p in reversed(range(1, 8)):
            far_copy(a, p).start()
        own2[a].start()

    def far_wait(a):
        own2[a].wait()
        all_in(xc.at[a, 0, m_own, y2, pl.ds(0, 112)], far_recv.at[a])

    push(0)
    load_far[0].wait()
    sendbuf2[0] = mm(perm_val, xq2[...], NN).astype(BF)
    load_far[1].wait()
    sendbuf2[1] = (w_slot * mm(perm_val, cq2[...], NN)).astype(BF)

    lane = lax.broadcasted_iota(jnp.int32, (128, 128), 1)

    def sums_out(phase, one, two):
        cols2 = jnp.where(lane == 0, one, 0.0) + jnp.where(lane == 1, two, 0.0)
        st_out[phase] = cols2.T[0:8, :]
        return [
            remote(
                st_out.at[phase], st_in.at[phase, j], st_send.at[phase], st_recv.at[phase], dev
            )
            for j, dev in enumerate((dev_p, dev_m, dev_2))
        ]

    def sums_in(phase):
        all_in(st_in.at[phase], st_recv.at[phase])
        tot = (st_out[phase] + st_in[phase, 2]) + (st_in[phase, 0] + st_in[phase, 1])
        tall = jnp.concatenate([tot, jnp.zeros((120, 128), F32)], axis=0).T
        return tall[:, 0:1], tall[:, 1:2]

    load_conv.wait()
    conv_vals = conv_ref[...].astype(F32)
    stats = sums_out(
        0,
        jnp.sum(conv_vals, axis=1, keepdims=True),
        jnp.sum(conv_vals * conv_vals, axis=1, keepdims=True),
    )
    for copy in stats:
        copy.start()

    first, second = pl.ds(0, 64), pl.ds(64, 64)
    listed = [(g, y), (g, ym), (g, yp), (g, y2), (og, y), (og, ym), (og, yp), (og, y2)]

    def block(a, h, gg, cc, yy):
        return xc.at[a, h, gg * 2 + cc, yy]

    def ag_copy(a, h, kind, ref, dev):
        lot = 4 if kind in (3, 4) else 8 if kind >= 8 else 0
        slot = kind if kind < 8 else 5 + kind // 4
        slot = slot + 1 if kind >= 8 else slot
        return remote(
            ref, ref, ag_send.at[a * 2 + h + lot], ag_recv.at[a * 2 + h, slot], dev
        )

    def ag_out(a, h, kind):
        if kind >= 8:
            gg, yy = listed[kind - 8]
            return ag_copy(a, h, kind, block(a, h, gg, c, yy), dev_s)
        ref, dev = (
            (block(a, h, g, c, y), dev_x),
            (block(a, h, g, c, y), dev_p),
            (block(a, h, g, c, y), dev_m),
            (block(a, h, g, c, ym).at[first], dev_p),
            (block(a, h, g, c, yp).at[second], dev_m),
            (block(a, h, og, c, y), dev_p),
            (block(a, h, og, c, y), dev_m),
            (block(a, h, g, c, y2), dev_x),
        )[kind]
        return ag_copy(a, h, kind, ref, dev)

    def ag_in(a, h, kind):
        if kind >= 8:
            gg, yy = listed[kind - 8]
            return ag_copy(a, h, kind, block(a, h, gg, oc, yy), dev_s)
        ref, dev = (
            (block(a, h, og, c, y), dev_x),
            (block(a, h, g, c, ym), dev_m),
            (block(a, h, g, c, yp), dev_p),
            (block(a, h, g, c, y2).at[first], dev_m),
            (block(a, h, g, c, y2).at[second], dev_p),
            (block(a, h, og, c, ym), dev_m),
            (block(a, h, og, c, yp), dev_p),
            (block(a, h, og, c, y2), dev_x),
        )[kind]
        return ag_copy(a, h, kind, ref, dev)

    def go(a, h, *kinds):
        for kind in kinds:
            ag_out(a, h, kind).start()

    def got(a, h, *kinds):
        for kind in kinds:
            ag_in(a, h, kind).wait_recv()

    def sib_got(a, h, gg):
        all_in(xc.at[a, h, gg * 2 + oc], ag_recv.at[a * 2 + h, 8 if gg is g else 9])

    def relay_y(a, h):
        got(a, h, 1)
        go(a, h, *((3, 9) if h else (9,)))
        got(a, h, 2)
        go(a, h, *((4, 10) if h else (10,)))

    def relay_x(a, h):
        got(a, h, 0)
        go(a, h, 5, 6, 12)

    def relay_far(a, h):
        if h:
            got(a, h, 3, 4)
        else:
            far_wait(a)
        go(a, h, 7, 11)

    def relay_last(a, h):
        got(a, h, 5)
        go(a, h, 13)
        got(a, h, 6)
        go(a, h, 14)
        got(a, h, 7)
        go(a, h, 15)

    def pair(gg):
        return pl.ds(gg * 2, 2)

    def rows_at(a, h, gg, q):
        return xc[a, h, pair(gg), q].reshape(256, 512)

    def pre_acts(h, gg):
        pre_g = jnp.zeros((256, 224), F32)
        pre_u = jnp.zeros((256, 224), F32)
        for q in range(4):
            span = slice(q * 512, q * 512 + 512)
            rows = rows_at(0, h, gg, q)
            pre_g += mm(rows, wg[:, span], NT)
            pre_u += mm(rows, wu[:, span], NT)
        return pre_g, pre_u

    def forward(h, gg, pres):
        pre_g, pre_u = pres
        d_act = jnp.zeros((256, 224), F32)
        for q in range(4):
            span = slice(q * 512, q * 512 + 512)
            d_act += mm(rows_at(1, h, gg, q), wd[:, span], NT)
        sig = jax.nn.sigmoid(pre_g)
        d_gate = (d_act * pre_u * swish_slope(pre_g, sig)).astype(BF)
        d_up = (d_act * pre_g * sig).astype(BF)
        return d_gate, d_up, pre_g * sig * pre_u

    def back(h, gg, grads, yy):
        span = pl.ds(pl.multiple_of(yy * 512, 512), 512)
        term = mm(grads[0], wg[:, span], NN) + mm(grads[1], wu[:, span], NN)
        part[h, pair(gg), yy] = term.astype(BF).reshape(2, 128, 512)

    order = (y2, yp, ym, y)

    def sib_copy(h, gg, j):
        at = (0 if gg is g else 4) + j
        return remote(
            part.at[h, gg * 2 + oc, order[j]], sib_in.at[h, gg, order[j]],
            sb_send.at[h], sb_recv.at[h, at], dev_s,
        )

    def whole(h, gg, pres, *between):
        grads = forward(h, gg, pres)
        for j in range(4):
            back(h, gg, grads, order[j])
            sib_copy(h, gg, j).start()
            if j < len(between) and between[j]:
                between[j]()
        slot = h * 2 + gg
        act_t[slot] = grads[2].T.astype(BF)
        dg_t[slot] = grads[0].T
        du_t[slot] = grads[1].T

    m_g, m_o = g * 2 + c, og * 2 + c

    def pair_sum(h, gg, j):
        sib_copy(h, gg, j).wait_recv()
        at = (h, gg * 2 + c, order[j])
        part[at] = (part[at].astype(F32) + sib_in[h, gg, order[j]].astype(F32)).astype(BF)

    def pieces(h):
        n = 1 + h
        return n, [i for k in range(n) for i in (k, n + k)]

    def piece(h, i):
        rows = 64 // (1 + h)
        return pl.ds(i * rows, rows)

    def rs_copy(h, kind):
        n = 1 + h
        if kind < 4:
            at = piece(h, kind)
            src, dst, dev = part.at[h, m_o, y2, at], in_a.at[h, at], dev_x
        elif kind < 8:
            at = piece(h, kind - 4)
            src, dst = part.at[h, m_g, y2, at], in_c.at[h, at]
            dev = dev_p if kind - 4 < n else dev_m
        elif kind < 12:
            at = piece(h, kind - 8)
            yy, i, dev = (yp, 0, dev_p) if kind - 8 < n else (ym, 1, dev_m)
            src, dst = part.at[h, m_g, yy, at], in_e.at[h, i, at]
        else:
            src, dst, dev = (
                (part.at[h, m_o, yp, first], in_b.at[h, 0, first], dev_p),
                (part.at[h, m_o, ym, first], in_b.at[h, 1, first], dev_m),
                (part.at[h, m_o, y, first], in_d.at[h, first], dev_x),
                (part.at[h, m_g, yp, second], in_e.at[h, 0, second], dev_p),
                (part.at[h, m_g, ym, first], in_e.at[h, 1, first], dev_m),
                (part.at[h, m_o, yp, second], in_b.at[h, 0, second], dev_p),
                (part.at[h, m_o, ym, second], in_b.at[h, 1, second], dev_m),
                (part.at[h, m_o, y, second], in_d.at[h, second], dev_x),
            )[kind - 12]
        slot = kind if kind < 8 else 8 if kind in (12, 13) else 10 if kind in (17, 18) else 9
        lot = 0 if kind in (4, 5, 6, 7, 12, 13, 14, 17, 18, 19) else 1
        return remote(src, dst, rs_send.at[h, lot], rs_recv.at[h, slot], dev)

    def rs_chain(h):
        pair_sum(h, og, 0)
        for i in pieces(h)[1]:
            rs_copy(h, i).start()

    def rs_open(h):
        pair_sum(h, og, 1)
        rs_copy(h, 12).start()
        rs_copy(h, 17).start()
        pair_sum(h, og, 2)
        rs_copy(h, 13).start()
        rs_copy(h, 18).start()

    def rs_own(h):
        pair_sum(h, g, 1)
        pair_sum(h, g, 2)
        pair_sum(h, g, 0)
        pair_sum(h, og, 3)
        pair_sum(h, g, 3)

    def rs_early(h):
        rs_copy(h, 15).start()
        rs_copy(h, 16).start()

    def add_to(at, *terms):
        value = part[at].astype(F32)
        for term in terms:
            value += term.astype(F32)
        part[at] = value.astype(BF)

    def rs_far(h):
        for i in pieces(h)[1]:
            rs_copy(h, i).wait_recv()
            add_to((h, m_g, y2, piece(h, i)), in_a[h, piece(h, i)])
            rs_copy(h, 4 + i).start()

    def rs_cross(h, half):
        at = (first, second)[half]
        all_in(in_b.at[h, :, at], rs_recv.at[h, 8 + 2 * half])
        add_to((h, m_o, y, at), in_b[h, 0, at], in_b[h, 1, at])
        rs_copy(h, 14 + 5 * half).start()

    def rs_near(h):
        n, turns = pieces(h)
        for i in turns:
            rs_copy(h, 4 + i).wait_recv()
            add_to((h, m_g, yp if i < n else ym, piece(h, i)), in_c[h, piece(h, i)])
            rs_copy(h, 8 + i).start()

    def ret_copy(p):
        zz, hh = from_of(p)
        return remote(
            total.at[p // 8, pl.ds(p % 8 * 16, 16)], ret.at[rows_of(me)],
            ret_send.at[0], ret_recv.at[0], holder(zz, hh),
        )

    own_back = pltpu.make_async_copy(total.at[0, pl.ds(0, 16)], ret.at[rows_of(me)], own_sem.at[0])

    def rs_close(h):
        all_in(part.at[h, 0, pl.ds(0, 3)], rs_recv.at[h, 9])
        total[h] = (
            part[h, m_g, y].astype(F32) + in_d[h].astype(F32)
            + in_e[h, 0].astype(F32) + in_e[h, 1].astype(F32)
        ).astype(BF)
        for p in reversed(range(8 * h, 8 * h + 8)):
            if p == 0:
                own_back.start()
            else:
                ret_copy(p).start()

    def weight_grad(out_ref, source, a, half):
        def tile(q, _):
            acc = jnp.zeros((source.shape[1], 512), F32)
            for h in range(2):
                for gg in range(2):
                    acc += mm(source[h * 2 + gg], rows_at(a, h, gg, q), NN)
            out_ref[:, pl.ds(pl.multiple_of(q * 512, 512), 512)] = acc.astype(BF)
            return 0

        lax.fori_loop(2 * half, 2 * half + 2, tile, 0)

    def drain_rows(a):
        all_sent(sendbuf.at[a, pl.ds(0, 240)], a2a_send.at[a])
        all_sent(sendbuf2.at[a, pl.ds(0, 112)], far_send.at[a])
        for h in range(2):
            all_sent(xc.at[a, h, pl.ds(0, 2), pl.ds(0, 3)], ag_send.at[a * 2 + h])
            all_sent(xc.at[a, h, pl.ds(0, 2)], ag_send.at[a * 2 + h + 8])
        all_sent(xc.at[a, 1, 0, 0], ag_send.at[a * 2 + 5])

    def drain_sums():
        for h in range(2):
            all_sent(part.at[h, pl.ds(0, 2)], sb_send.at[h])
            all_sent(part.at[h, 0], rs_send.at[h, 0])
            all_sent(part.at[h, 0, pl.ds(0, 3)], rs_send.at[h, 1])

    a2a_wait(0, 0)
    go(0, 0, 0, 1, 2, 8)
    push_far(0)
    push_far(1)
    push(1)
    a2a_wait(1, 0)
    go(1, 0, 0, 1, 2, 8)
    relay_x(0, 0)
    relay_x(1, 0)
    relay_y(0, 0)
    relay_y(1, 0)
    relay_far(0, 0)
    relay_far(1, 0)
    a2a_wait(0, 1)
    go(0, 1, 0, 1, 2, 8)
    sum1, sum2 = sums_in(0)
    mean = sum1 / DB
    rstd = lax.rsqrt(sum2 / DB - mean * mean + 1e-05)
    norm_val = (conv_ref[...].astype(F32) - mean) * rstd
    zpre = norm_val * gain_ref[...]
    zsig = jax.nn.sigmoid(zpre)
    normed[...] = norm_val
    mixed[...] = (zpre * zsig).astype(BF)
    slope[...] = swish_slope(zpre, zsig) * gain_ref[...]
    scale[...] = jnp.broadcast_to(rstd, (128, 256))
    for copy in loads:
        copy.wait()
    sib_got(0, 0, g)
    pres = pre_acts(0, g)
    a2a_wait(1, 1)
    go(1, 1, 0, 1, 2, 8)
    sib_got(1, 0, g)
    whole(0, g, pres)
    relay_last(0, 0)
    relay_last(1, 0)
    relay_y(0, 1)
    sib_got(0, 0, og)
    pres = pre_acts(0, og)
    sib_got(1, 0, og)
    relay_y(1, 1)
    relay_x(0, 1)
    whole(0, og, pres, lambda: relay_far(0, 1), lambda: relay_x(1, 1))
    sib_got(0, 1, g)
    pres = pre_acts(1, g)
    relay_far(1, 1)
    rs_chain(0)
    rs_open(0)
    sib_got(1, 1, g)
    whole(1, g, pres)
    rs_own(0)
    rs_early(0)
    relay_last(0, 1)
    sib_got(0, 1, og)
    relay_last(1, 1)
    pres = pre_acts(1, og)
    sib_got(1, 1, og)
    whole(1, og, pres, lambda: rs_far(0), None, lambda: rs_chain(1))
    rs_open(1)
    rs_own(1)
    weight_grad(gg_ref, dg_t, 0, 0)
    rs_cross(0, 0)
    rs_cross(0, 1)
    drain_rows(0)
    weight_grad(gg_ref, dg_t, 0, 1)
    rs_far(1)
    rs_early(1)
    rs_near(0)
    rs_cross(1, 0)
    weight_grad(gu_ref, du_t, 0, 0)
    rs_cross(1, 1)
    weight_grad(gu_ref, du_t, 0, 1)
    rs_near(1)
    weight_grad(gd_ref, act_t, 1, 0)
    drain_rows(1)
    weight_grad(gd_ref, act_t, 1, 1)
    rs_close(0)
    rs_close(1)
    mix_copy = remote(mixed, mixed2, mx_sem.at[0], mx_sem.at[1], dev_2)
    mix_copy.start()
    drain_sums()

    all_in(ret.at[pl.ds(0, 240)], ret_recv.at[0])
    own_back.wait()
    moe = mm(perm[...], ret[...], TN)
    res_ref[y] = (cq[...].astype(F32) + moe).astype(BF)

    def slab(i):
        return pl.ds(i * 32, 32)

    def res_copy(yy, i, kind, dev):
        ref = res_ref.at[yy, slab(i)]
        return remote(ref, ref, res_send.at[0], res_recv.at[kind], dev)

    for i in range(4):
        res_copy(y, i, min(i, 2), dev_p).start()
        res_copy(y, 3 - i, 3 + min(i, 2), dev_m).start()
    for copy in late_loads:
        copy.wait()

    def pair_of(q):
        return pl.ds(q * 2, 2)

    def gp_copy(q, j):
        return remote(
            gp.at[oc, :, pair_of(q)], gp_sib.at[:, pair_of(q)], gs_send.at[0], gs_recv.at[j], dev_s
        )

    def proj_terms(q, j):
        feats = res_ref[q]
        term = mm(feats, mixed[...], TN)
        for i in range(8):
            for cc in range(2):
                gp[cc, i % 4, q * 2 + i // 4] = term[i * 64 + cc * 32 : i * 64 + cc * 32 + 32].astype(BF)
        gp_copy(q, j).start()
        return mm(feats, proj[pl.ds(pl.multiple_of(q * 512, 512), 512), :], NN)

    def cross_terms():
        mix_copy.wait_recv()
        term = mm(res_ref[y], mixed2[...], TN)
        for i in range(8):
            for cc in range(2):
                gp[cc, i % 4, y2 * 2 + i // 4] = term[i * 64 + cc * 32 : i * 64 + cc * 32 + 32].astype(BF)
        gp_copy(y2, 3).start()

    def gx_copy(q, j, i):
        return remote(
            gp.at[c, others_x[i], pair_of(q)], gp_x.at[i, pair_of(q)],
            gx_send.at[0], gx_recv.at[j], at_x(others_x[i]),
        )

    def over_x(q, j):
        gp_copy(q, j).wait_recv()
        gp[c, :, pair_of(q)] = (
            gp[c, :, pair_of(q)].astype(F32) + gp_sib[:, pair_of(q)].astype(F32)
        ).astype(BF)
        for i in (1, 2, 0):
            gx_copy(q, j, i).start()

    def gz_copy(to, slot):
        return remote(gp_row.at[to], gp_z.at[slot], gz_send.at[0], gz_recv.at[0], at_z(to))

    def over_z(q, j):
        pair = pair_of(q)
        all_in(gp_x.at[:, pair], gx_recv.at[j])
        gp_row[pair] = (
            (gp[c, x, pair].astype(F32) + gp_x[0, pair].astype(F32))
            + (gp_x[1, pair].astype(F32) + gp_x[2, pair].astype(F32))
        ).astype(BF)
        for i in range(2):
            if j < 3:

                @pl.when(q * 2 + i != z)
                def _():
                    gz_copy(q * 2 + i, z).start()

            else:

                @pl.when(y * 2 + i != z)
                def _():
                    remote(
                        gp_row.at[q * 2 + i], gp_z2.at[z], gz2_send.at[0], gz2_recv.at[0],
                        at_z(y * 2 + i),
                    ).start()

    d_mixed = proj_terms(y, 0)
    cross_terms()
    over_x(y, 0)
    over_x(y2, 3)
    for i in range(2):
        res_copy(ym, i, i, dev_m).wait_recv()
        res_copy(ym, i, 6, dev_p).start()
        res_copy(yp, 3 - i, 3 + i, dev_p).wait_recv()
        res_copy(yp, 3 - i, 7, dev_m).start()
    all_in(res_ref.at[ym, pl.ds(64, 64)], res_recv.at[2])
    d_mixed += proj_terms(ym, 1)
    all_in(res_ref.at[yp, pl.ds(0, 64)], res_recv.at[5])
    d_mixed += proj_terms(yp, 2)
    over_x(ym, 1)
    over_x(yp, 2)
    all_in(res_ref.at[y2, pl.ds(0, 64)], res_recv.at[6])
    all_in(res_ref.at[y2, pl.ds(64, 64)], res_recv.at[7])
    d_mixed += mm(res_ref[y2], proj[pl.ds(pl.multiple_of(y2 * 512, 512), 512), :], NN)
    d_norm = d_mixed * slope[...]
    norm_val = normed[...]
    stats2 = sums_out(
        1,
        jnp.sum(d_norm, axis=1, keepdims=True),
        jnp.sum(d_norm * norm_val, axis=1, keepdims=True),
    )
    for copy in stats2:
        copy.start()
    over_z(y, 0)
    over_z(y2, 3)

    first_sum, second_sum = sums_in(1)
    conv_grad = (
        scale[...] * (d_norm - first_sum / DB - norm_val * (second_sum / DB))
    ).astype(BF)
    halo_out[...] = conv_grad[0:32]
    halo = remote(halo_out, halo_in, halo_sem.at[0], halo_sem.at[1], dev_prev)
    halo.start()
    ext[0:128, :] = conv_grad.astype(F32)
    over_z(ym, 1)
    over_z(yp, 2)

    def correlate(start, count):
        acc = jnp.zeros((count, 256), F32)
        for k in range(WIDTH):
            acc += ext[start + k : start + k + count, :] * taps_ref[k : k + 1, :]
        return acc

    def glu_grads(start, count, unit_grad):
        span = slice(start, start + count)
        sig = jax.nn.sigmoid(gate_ref[span, :].astype(F32))
        gv_ref[span, :] = (unit_grad * sig).astype(BF)
        gt_ref[span, :] = (
            unit_grad * value_ref[span, :].astype(F32) * sig * (1.0 - sig)
        ).astype(BF)

    glu_grads(0, 64, correlate(0, 64))
    glu_grads(64, 32, correlate(64, 32))

    mine = z // 2
    fin_copy = remote(fin_out, fin_in, fin_sem.at[0], fin_sem.at[1], dev_2)

    @pl.when(mine == y)
    def _():
        all_in(gp_z2.at[pl.ds(0, 7)], gz2_recv.at[0])
        cross = gp_row[y2 * 2 + lax.rem(z, 2)].astype(F32)
        for k in range(1, 8):
            cross += gp_z2[lax.rem(z + k, 8)].astype(F32)
        fin_out[...] = cross
        fin_copy.start()

    halo.wait_recv()
    keep = jnp.where(sp < 63, 1.0, 0.0)
    ext[128:160, :] = halo_in[...].astype(F32) * keep
    glu_grads(96, 32, correlate(96, 32))

    @pl.when(mine != y2)
    def _():
        all_in(gp_z.at[pl.ds(0, 7)], gz_recv.at[0])
        rows_sum = gp_row[z].astype(F32)
        for k in range(1, 8):
            rows_sum += gp_z[lax.rem(z + k, 8)].astype(F32)
        gp_ref[...] = rows_sum
        all_sent(gp_z.at[pl.ds(0, 5)], gz_send.at[0])

    @pl.when(mine == y2)
    def _():
        fin_copy.wait_recv()
        gp_ref[...] = fin_in[...]
        all_sent(gp_z.at[pl.ds(0, 6)], gz_send.at[0])

    @pl.when(mine == y)
    def _():
        fin_copy.wait_send()
        all_sent(gp_z.at[pl.ds(0, 1)], gz2_send.at[0])

    @pl.when(mine != y)
    def _():
        all_sent(gp_z.at[pl.ds(0, 2)], gz2_send.at[0])

    mix_copy.wait_send()

    all_sent(ret.at[pl.ds(0, 240)], ret_send.at[0])
    for phase in range(2):
        all_sent(st_in.at[phase], st_send.at[phase])
    halo.wait_send()
    all_sent(res_ref.at[pl.ds(0, 3)], res_send.at[0])
    all_sent(gp.at[oc], gs_send.at[0])
    all_sent(gp_x, gx_send.at[0])


def write_kernel(*refs):
    copies = [pltpu.make_async_copy(refs[i], refs[6 + i], refs[12].at[i]) for i in range(6)]
    for copy in copies:
        copy.start()
    for copy in copies:
        copy.wait()


def local(
    moe_input,
    out_cotangent,
    routes,
    route_weight,
    w_gate,
    w_up,
    w_down,
    out_proj,
    conv_out,
    glu_value,
    glu_gate,
    taps,
    norm_gain,
):
    units, width = w_down.shape[1:]
    tokens, channels = conv_out.shape
    vmem = pl.BlockSpec(memory_space=pltpu.VMEM)
    hbm = pl.BlockSpec(memory_space=pl.ANY)
    dma = pltpu.SemaphoreType.DMA
    grad = jax.ShapeDtypeStruct((units, width), BF)
    glu = jax.ShapeDtypeStruct((tokens, channels), BF)
    shapes = (grad, grad, grad, jax.ShapeDtypeStruct((32, channels), F32), glu, glu)
    results = pl.pallas_call(
        backward_kernel,
        out_shape=[pltpu.VMEM(a.shape, a.dtype) for a in shapes],
        in_specs=[vmem] + [hbm] * 12,
        out_specs=[vmem] * 6,
        scratch_shapes=[
            pltpu.VMEM((128, 512), BF),
            pltpu.VMEM((128, 512), BF),
            pltpu.VMEM((128, 512), BF),
            pltpu.VMEM((128, 512), BF),
            pltpu.VMEM((256, 128), BF),
            pltpu.VMEM((2, 256, 512), BF),
            pltpu.VMEM((2, 256, 512), BF),
            pltpu.VMEM((2, 2, 4, 4, 128, 512), BF),
            pltpu.VMEM((units, width), BF),
            pltpu.VMEM((units, width), BF),
            pltpu.VMEM((units, width), BF),
            pltpu.VMEM((4, units, 256), BF),
            pltpu.VMEM((4, units, 256), BF),
            pltpu.VMEM((4, units, 256), BF),
            pltpu.VMEM((2, 4, 4, 128, 512), BF),
            pltpu.VMEM((2, 2, 4, 128, 512), BF),
            pltpu.VMEM((2, 128, 512), BF),
            pltpu.VMEM((2, 2, 128, 512), BF),
            pltpu.VMEM((2, 128, 512), BF),
            pltpu.VMEM((2, 128, 512), BF),
            pltpu.VMEM((2, 2, 128, 512), BF),
            pltpu.VMEM((2, 128, 512), BF),
            pltpu.VMEM((256, 512), BF),
            pltpu.VMEM((2, tokens), jnp.int32),
            pltpu.VMEM((2, tokens), F32),
            pltpu.VMEM((tokens, channels), BF),
            pltpu.VMEM((tokens, channels), BF),
            pltpu.VMEM((tokens, channels), BF),
            pltpu.VMEM((WIDTH, channels), F32),
            pltpu.VMEM((4, 128, 512), BF),
            pltpu.VMEM((width, 256), BF),
            pltpu.VMEM((128, 256), F32),
            pltpu.VMEM((128, 256), F32),
            pltpu.VMEM((128, 256), BF),
            pltpu.VMEM((128, 256), BF),
            pltpu.VMEM((128, 256), F32),
            pltpu.VMEM((2, 8, 128), F32),
            pltpu.VMEM((2, 3, 8, 128), F32),
            pltpu.VMEM((160, 256), F32),
            pltpu.VMEM((32, 256), BF),
            pltpu.VMEM((32, 256), BF),
            pltpu.VMEM((2, 4, 8, 32, 256), BF),
            pltpu.VMEM((4, 8, 32, 256), BF),
            pltpu.VMEM((3, 8, 32, 256), BF),
            pltpu.VMEM((8, 32, 256), BF),
            pltpu.VMEM((8, 32, 256), BF),
            pltpu.VMEM((8, 32, 256), BF),
            pltpu.VMEM((32, 256), F32),
            pltpu.VMEM((32, 256), F32),
            dma((14,)), dma((4,)),
            dma((2,)), dma((2, 2)), dma((2,)), dma((2,)), dma((12,)), dma((4, 10)),
            dma((2,)), dma((2, 8)), dma((2, 2)), dma((2, 11)),
            dma((1,)), dma((1,)), dma((1,)), dma((8,)),
            dma((2,)), dma((2,)), dma((2,)),
            dma((1,)), dma((4,)), dma((1,)), dma((4,)), dma((1,)), dma((1,)),
            dma((2,)), dma((2,)), dma((1,)), dma((1,)),
        ],
        compiler_params=pltpu.CompilerParams(
            collective_id=0, has_side_effects=True, vmem_limit_bytes=60 * 1024 * 1024
        ),
        name="backward",
    )(
        norm_gain[None, :], routes.T, route_weight.T,
        moe_input, out_cotangent, w_gate[0].T, w_up[0].T, w_down[0], out_proj,
        conv_out, glu_value, glu_gate, taps,
    )
    gg, gu, gd, gp, gv, gt = pl.pallas_call(
        write_kernel,
        out_shape=shapes,
        in_specs=[vmem] * 6,
        out_specs=[hbm] * 6,
        scratch_shapes=[dma((6,))],
        compiler_params=pltpu.CompilerParams(vmem_limit_bytes=1024 * 1024),
        name="write_out",
    )(*(pltpu.with_memory_space_constraint(r, pltpu.VMEM) for r in results))
    return (gg.T[None], gu.T[None], gd[None], gp, gv, gt)


def solution(mesh):
    in_specs = (
        P("sp", None),
        P("sp", None),
        P("sp", None),
        P("sp", None),
        P("sp", None, "tp"),
        P("sp", None, "tp"),
        P("sp", "tp", None),
        P(None, "tp"),
        P("sp", "tp"),
        P("sp", "tp"),
        P("sp", "tp"),
        P(None, "tp"),
        P("tp"),
    )
    out_specs = (
        P("sp", None, "tp"),
        P("sp", None, "tp"),
        P("sp", "tp", None),
        P("sp", "tp"),
        P("sp", "tp"),
        P("sp", "tp"),
    )
    return jax.shard_map(local, mesh=mesh, in_specs=in_specs, out_specs=out_specs, check_vma=False)
```
